32 devices in a mesh: grp: 2 (over y), sp: 4 (over z), tp: 4 (over x, core).
Axes of the slice: x: 2, y: 2, z: 4, core: 2. Of those that a mesh axis runs over, the one named last changes fastest.
Arguments:
- tokens: bfloat16 [1024, 2048], P(('grp', 'sp')), parts along dimension 0, may hold values from -6 to 6
- norm_gain: float32 [2048], replicated, may hold values from 0.1 to 1.9
- w_query: bfloat16 [2048, 512], P('sp', 'tp'), may hold values from -0.125 to 0.125
- w_key: bfloat16 [2048, 512], P('sp', 'tp'), may hold values from -0.125 to 0.125
- w_value: bfloat16 [2048, 512], P('sp', 'tp'), may hold values from -0.125 to 0.125
- w_glu_value: bfloat16 [2048, 1024], P('sp', 'tp'), may hold values from -0.125 to 0.125
- w_glu_gate: bfloat16 [2048, 1024], P('sp', 'tp'), may hold values from -0.125 to 0.125
- key_offset: bfloat16 [1024, 8], P(('grp', 'sp'), 'tp'), parts along dimension 0, may hold values from -13 to 0
- head_gain: float32 [8, 64], P('tp'), may hold values from 0.1 to 1.9
- conv_taps: float32 [31, 1024], P(None, 'tp'), may hold values from -2.873685 to 2.873685
- channel_gain: float32 [1024], P('tp'), may hold values from 0.1 to 1.9
- channel_bias: float32 [1024], P('tp'), may hold values from -3 to 3
- w_out_attn: bfloat16 [512, 2048], P('tp'), may hold values from -0.15625 to 0.15625
- w_out_conv: bfloat16 [1024, 2048], P('tp'), may hold values from -0.15625 to 0.15625
- out_gain: float32 [2048], replicated, may hold values from 0.1 to 1.9
Outputs:
- mixed: bfloat16 [1024, 2048], P(('grp', 'sp')), parts along dimension 0
- log_mass: float32 [8, 1024], P('tp', ('grp', 'sp')), parts along dimension 1
The draws below stay inside these ranges and needn't reach their ends.
There are 2 independent parts, one for each index of `grp`. The reference program is written for one: setup_inputs(seed, part) draws one part's arguments, and reference() takes and returns one part's arrays. A program takes and returns all parts, laid end to end along the dimension named above; an argument that names none is the same for every part. Nothing has to cross between parts.
All inputs are finite; a program needn't handle non-finite values.
Results may differ from the reference program's by a relative error of at most 0.011.
Values may be sent and summed in bfloat16 or wider, within the bound.
No kernel may reach another device: no remote copies, remote signals or barrier semaphores. Data moves between devices by JAX's collectives and lax.ppermute only.
A program may use at most 64 MiB of HBM per device.

```python
import jax
import jax.numpy as jnp
from jax import lax

D = 2048
ATTENTION_HEADS = 8
KVHEADS = 8
HD = 64
CW = 1024
KSIZE = 31
TOKENS = 512


def draw_key_offset(key, part):
    parallel_flows = jax.random.split(jax.random.fold_in(key, 11), 6)
    sequence_length_total = TOKENS
    head_order = jax.random.permutation(parallel_flows[0], ATTENTION_HEADS)
    fast_heads = head_order < ATTENTION_HEADS // 2
    random_noise_values = 0.5 * jax.random.truncated_normal(parallel_flows[1], -4.0, 4.0, (sequence_length_total, ATTENTION_HEADS), jnp.float32)
    slow_base = jnp.log(1.0 / sequence_length_total) - 0.5 - jax.random.uniform(parallel_flows[2], (ATTENTION_HEADS,), jnp.float32, 0.0, 0.5)
    fast_base = jax.random.uniform(parallel_flows[3], (ATTENTION_HEADS,), jnp.float32, -5.0, -4.0)
    head_starting_row = jnp.where(fast_heads, fast_base, slow_base)
    block_count = (sequence_length_total + 127) // 128
    height_levels = jax.random.uniform(parallel_flows[4], (block_count, ATTENTION_HEADS), jnp.float32, -0.7, 0.7)
    height_levels = jnp.repeat(height_levels, 128, axis=0)[:sequence_length_total]
    gathered_key_block = jax.random.split(parallel_flows[5], 2)
    gathered_positions = jax.random.randint(gathered_key_block[0], (4, ATTENTION_HEADS), 0, sequence_length_total)
    token_positions = jnp.arange(sequence_length_total, dtype=jnp.int32)
    broken_stick_mass = jnp.any(token_positions[:, None, None] == gathered_positions[None, :, :], axis=1)
    gathered_value_block = jax.random.uniform(gathered_key_block[1], (sequence_length_total, ATTENTION_HEADS), jnp.float32, -1.4, 0.0)
    final_output = jnp.clip(jnp.where(broken_stick_mass, gathered_value_block, head_starting_row + height_levels + random_noise_values), -13.0, 0.0)
    final_output = final_output.at[0, 0].set(-13.0)
    final_output = final_output.at[0, 1].set(0.0)
    return final_output.astype(jnp.bfloat16)


def draw_conv_taps(key, part):
    stream = jax.random.fold_in(key, 23)
    base_taps = jax.random.truncated_normal(stream, -4.0, 4.0, (KSIZE, CW), jnp.float32)
    channel_rise = jnp.exp(jnp.log(4.0) * jnp.arange(CW, dtype=jnp.float32) / CW)
    return base_taps * channel_rise / jnp.sqrt(float(KSIZE))


def block_scale(key, shape, cuts, smallest, top_value):
    gain, own = 1.0, jax.random.fold_in(key, 6)
    for axis_at, shards_of in cuts:
        steps = jnp.exp(jax.random.uniform(jax.random.fold_in(own, axis_at), (shards_of,), jnp.float32, smallest / len(cuts), top_value / len(cuts)))
        gain = gain * jnp.repeat(steps, shape[axis_at] // shards_of).reshape([-1 if axis == axis_at else 1 for axis in range(len(shape))])
    return gain


def noise(stream_key, dims, scale, reach, pieces=(), kind=jnp.bfloat16):
    values = jax.random.normal(stream_key, dims, jnp.float32) * scale
    if len(pieces) > 0:
        values = block_scale(stream_key, dims, pieces, -0.22, 0.18) * values
    return jnp.clip(values, min=-reach, max=reach).astype(kind)


def setup_inputs(seed: int = 0, part: int = 0) -> dict:
    keys = jax.random.split(jax.random.key(seed), 16)
    own_keys = jax.random.split(jax.random.fold_in(keys[15], part), 16)
    tokens = noise(own_keys[0], (TOKENS, D), 1.0, 6.0, ((0, 4),))
    norm_gain = jnp.clip(1.0 + 0.18 * jax.random.normal(keys[1], (D,), jnp.float32), 0.1, 1.9)
    w_query = noise(keys[2], (D, ATTENTION_HEADS * HD), D ** -0.5, 0.125, ((0, 4), (1, 4)))
    w_key = noise(keys[3], (D, KVHEADS * HD), D ** -0.5, 0.125, ((0, 4), (1, 4)))
    w_value = noise(keys[4], (D, KVHEADS * HD), D ** -0.5, 0.125, ((0, 4), (1, 4)))
    w_glu_value = noise(keys[5], (D, CW), D ** -0.5, 0.125, ((0, 4), (1, 4)))
    w_glu_gate = noise(keys[6], (D, CW), D ** -0.5, 0.125, ((0, 4), (1, 4)))
    key_offset = draw_key_offset(jax.random.fold_in(jax.random.fold_in(keys[15], part), 71), part)
    head_gain = jnp.clip(1.0 + 0.18 * jax.random.normal(keys[8], (ATTENTION_HEADS, HD), jnp.float32), 0.1, 1.9)
    conv_taps = draw_conv_taps(jax.random.fold_in(keys[15], 71), part)
    channel_gain = jnp.clip(1.0 + 0.18 * jax.random.normal(keys[10], (CW,), jnp.float32), 0.1, 1.9)
    channel_bias = noise(keys[11], (CW,), 0.5, 3.0, ((0, 4),), jnp.float32)
    w_out_attn = noise(keys[12], (ATTENTION_HEADS * HD, D), (ATTENTION_HEADS * HD + CW) ** -0.5, 0.15625, ((0, 4),))
    w_out_conv = noise(keys[13], (CW, D), (ATTENTION_HEADS * HD + CW) ** -0.5, 0.15625, ((0, 4),))
    out_gain = jnp.clip(1.0 + 0.18 * jax.random.normal(keys[14], (D,), jnp.float32), 0.1, 1.9)
    return dict(tokens=tokens, norm_gain=norm_gain, w_query=w_query, w_key=w_key, w_value=w_value, w_glu_value=w_glu_value, w_glu_gate=w_glu_gate, key_offset=key_offset, head_gain=head_gain, conv_taps=conv_taps, channel_gain=channel_gain, channel_bias=channel_bias, w_out_attn=w_out_attn, w_out_conv=w_out_conv, out_gain=out_gain)


norm_eps = 1e-06

def row_norm(values_in, gain_vec):
    squares = lax.optimization_barrier(jnp.mean(values_in * values_in, axis=-1, keepdims=True))
    return values_in * lax.rsqrt(squares + norm_eps) * gain_vec

def reference(tokens, norm_gain, w_query, w_key, w_value, w_glu_value, w_glu_gate, key_offset, head_gain, conv_taps, channel_gain, channel_bias, w_out_attn, w_out_conv, out_gain):
    sequence_length_total = tokens.shape[0]
    group_size = ATTENTION_HEADS // KVHEADS
    normed = row_norm(tokens.astype(jnp.float32), norm_gain).astype(jnp.bfloat16)

    def project(weight):
        return jnp.dot(normed, weight, preferred_element_type=jnp.float32).astype(jnp.bfloat16)
    query = project(w_query).astype(jnp.float32).reshape(sequence_length_total, KVHEADS, group_size, HD)
    key_rows = project(w_key).astype(jnp.float32).reshape(sequence_length_total, KVHEADS, HD)
    value_rows = project(w_value).astype(jnp.float32).reshape(sequence_length_total, KVHEADS, HD)
    glu_value = project(w_glu_value)
    glu_gate = project(w_glu_gate)
    offsets = key_offset.astype(jnp.float32).T.reshape(KVHEADS, group_size, 1, sequence_length_total)
    key_pos = jnp.arange(sequence_length_total, dtype=jnp.int32)
    q_block = min(sequence_length_total, 256)

    def attend(first_row):
        q_rows = lax.dynamic_slice_in_dim(query, first_row, q_block, 0)
        scores = jnp.einsum('qhgd,khd->hgqk', q_rows, key_rows) * HD ** (-0.5) + offsets
        query_pos = first_row + jnp.arange(q_block, dtype=jnp.int32)
        allowed = key_pos[None, :] <= query_pos[:, None]
        log_not = jnp.where(allowed, jax.nn.log_sigmoid(-scores), 0.0)
        later = lax.cumsum(log_not, axis=3, reverse=True) - log_not
        weights = jnp.where(allowed, jnp.exp(jax.nn.log_sigmoid(scores) + later), 0.0)
        log_mass = jnp.log(lax.optimization_barrier(jnp.sum(weights, axis=3)))
        rounded = lax.optimization_barrier(weights.astype(jnp.bfloat16)).astype(jnp.float32)
        head_mix = jnp.einsum('hgqk,khd->qhgd', rounded, value_rows)
        return (head_mix, log_mass)
    starts = jnp.arange(0, sequence_length_total, q_block, dtype=jnp.int32)
    head_mix, log_mass = lax.map(attend, starts)
    head_mix = head_mix.reshape(sequence_length_total, ATTENTION_HEADS, HD)
    log_mass = log_mass.transpose(1, 2, 0, 3).reshape(ATTENTION_HEADS, sequence_length_total)
    attended = row_norm(head_mix, head_gain).astype(jnp.bfloat16).reshape(sequence_length_total, ATTENTION_HEADS * HD)
    gated = (glu_value.astype(jnp.float32) * jax.nn.sigmoid(glu_gate.astype(jnp.float32))).astype(jnp.bfloat16)
    padded = jnp.pad(gated.astype(jnp.float32), ((KSIZE - 1, 0), (0, 0)))
    conv_out = jnp.zeros((sequence_length_total, gated.shape[1]), jnp.float32)
    for tap_index in range(KSIZE):
        conv_out = conv_out + conv_taps[tap_index] * padded[tap_index:tap_index + sequence_length_total]
    chan_mean = lax.optimization_barrier(jnp.mean(conv_out, axis=1, keepdims=True))
    centered = conv_out - chan_mean
    spread = lax.optimization_barrier(jnp.mean(centered * centered, axis=1, keepdims=True))
    channel_out = jax.nn.silu(centered * lax.rsqrt(spread + norm_eps) * channel_gain + channel_bias).astype(jnp.bfloat16)
    mix = jnp.dot(attended, w_out_attn, preferred_element_type=jnp.float32) + jnp.dot(channel_out, w_out_conv, preferred_element_type=jnp.float32)
    mixed = row_norm(mix, out_gain).astype(jnp.bfloat16)
    return (mixed, log_mass)
```

```python
import functools

import jax
import jax.numpy as jnp
from jax import lax
from jax.experimental import pallas as pl
from jax.experimental.pallas import tpu as pltpu
from jax.sharding import PartitionSpec as P

norm_eps = 1e-06
BF16 = jnp.bfloat16
F32 = jnp.float32


def exchange(value, axis, bit):
    count = lax.axis_size(axis)
    return lax.ppermute(value, axis, [(s, s ^ bit) for s in range(count)])


def from_behind(value, axis, steps):
    count = lax.axis_size(axis)
    initial, last = (max(0, -steps), min(count, count - steps))
    return lax.ppermute(value, axis, [(source, source + steps) for source in range(initial, last)])


def row_norm(values_in, gain_vec):
    squares = jnp.mean(values_in * values_in, axis=-1, keepdims=True)
    return values_in * lax.rsqrt(squares + norm_eps) * gain_vec


def dot_f32(a, b, dims=((1,), (0,))):
    return lax.dot_general(a, b, (dims, ((), ())), preferred_element_type=F32)


def attention_kernel(hd, q_ref, k_ref, v_ref, off_ref, gain_ref, out_ref, mass_ref, acc, mass, carry):
    me = lax.axis_index("sp")
    rows, width = q_ref.shape
    heads = width // hd
    lane = lax.broadcasted_iota(jnp.int32, (rows, width), 1) // hd
    keys = rows
    before = lax.broadcasted_iota(jnp.int32, (2 * keys, 2 * keys), 0) % keys
    column = lax.broadcasted_iota(jnp.int32, (2 * keys, 2 * keys), 1)
    suffix = jnp.where((column >= keys) | (before > column), 1.0, 0.0).astype(BF16)
    q = q_ref[...]
    scale = hd ** (-0.5)

    def block(slot, first):
        start = pl.multiple_of(slot * keys, keys)
        k = k_ref[pl.ds(start, keys), :]
        v = v_ref[pl.ds(start, keys), :]
        off = off_ref[pl.ds(pl.multiple_of(slot * 8, 8), 8), :].astype(F32)
        parts = []
        for h in range(heads):
            qh = jnp.where(lane == h, q, jnp.zeros_like(q))
            s = dot_f32(qh, k, ((1,), (1,))) * scale + off[h : h + 1, :]
            soft = jnp.maximum(s, 0.0) + jnp.log(1.0 + jnp.exp(-jnp.abs(s)))
            if first:
                allowed = lax.broadcasted_iota(jnp.int32, (rows, keys), 1) <= lax.broadcasted_iota(
                    jnp.int32, (rows, keys), 0
                )
                log_not = jnp.where(allowed, -soft, 0.0)
            else:
                log_not = -soft
            high = log_not.astype(BF16)
            low = (log_not - high.astype(F32)).astype(BF16)
            sums = dot_f32(jnp.concatenate([high, low], axis=1), suffix)
            later, total = sums[:, :keys], sums[:, keys:]
            if not first:
                later = later + carry[h]
            w = jnp.exp(s - soft + later)
            if first:
                w = jnp.where(allowed, w, 0.0)
                mass[h] = w
                carry[h] = total
            else:
                mass[h] = mass[h] + w
                carry[h] = carry[h] + total
            parts.append((w.astype(BF16), jnp.where(lane == h, v, jnp.zeros_like(v))))
        mix = dot_f32(
            jnp.concatenate([w for w, _ in parts], axis=1),
            jnp.concatenate([v for _, v in parts], axis=0),
        )
        if first:
            acc[...] = mix
        else:
            acc[...] = acc[...] + mix

    block(0, True)

    def earlier(t, _):
        block(jnp.bitwise_xor(me - t, me), False)
        return 0

    lax.fori_loop(1, me + 1, earlier, 0)
    mixed = acc[...]
    squares = mixed * mixed
    inverse = jnp.zeros_like(mixed)
    for h in range(heads):
        mean = jnp.sum(jnp.where(lane == h, squares, 0.0), axis=1, keepdims=True) / hd
        inverse = jnp.where(lane == h, lax.rsqrt(mean + norm_eps), inverse)
    out_ref[...] = (mixed * inverse * gain_ref[...]).astype(BF16)
    for h in range(heads):
        mass_ref[h : h + 1, :] = jnp.log(jnp.sum(jnp.transpose(mass[h]), axis=0, keepdims=True))


def attention(q, k, v, off, head_gain):
    rows, width = q.shape
    heads, hd = head_gain.shape
    out_shape = (jax.ShapeDtypeStruct((rows, width), BF16), jax.ShapeDtypeStruct((heads, rows), F32))
    return pl.pallas_call(
        functools.partial(attention_kernel, hd),
        out_shape=out_shape,
        in_specs=[pl.BlockSpec(memory_space=pltpu.VMEM)] * 5,
        out_specs=[pl.BlockSpec(memory_space=pltpu.VMEM)] * 2,
        scratch_shapes=[
            pltpu.VMEM((rows, width), F32),
            pltpu.VMEM((heads, rows, rows), F32),
            pltpu.VMEM((heads, rows, rows), F32),
        ],
        cost_estimate=pl.CostEstimate(flops=400_000_000, bytes_accessed=1_000_000, transcendentals=400_000),
        compiler_params=pltpu.CompilerParams(vmem_limit_bytes=16 * 1024 * 1024),
        name="stick_attention",
    )(q, k, v, off, head_gain.reshape(1, width))


def final_kernel(aw, cw, mine, core, far, wa, wc, wcore, wx, wxc, gb0, gb1, gb2, gb3, gain_ref, out_ref):
    acts = [mine[...], core[...], far[0], far[1]]
    convs = [a[:, aw:].astype(F32) for a in acts]
    count = len(convs) * cw
    mean = sum(jnp.sum(v, axis=1, keepdims=True) for v in convs) / count
    centered = [v - mean for v in convs]
    spread = sum(jnp.sum(v * v, axis=1, keepdims=True) for v in centered) / count
    inverse = lax.rsqrt(spread + norm_eps)
    total = None
    for slot, (v, gb) in enumerate(zip(centered, (gb0, gb1, gb2, gb3))):
        y = v * inverse * gb[0:1, :] + gb[1:2, :]
        y = (y * jax.nn.sigmoid(y)).astype(BF16)
        att = acts[slot][:, :aw]
        if slot == 0:
            part = dot_f32(att, wa[...]) + dot_f32(y, wc[...])
        else:
            w = (wcore, wx, wxc)[slot - 1]
            part = dot_f32(jnp.concatenate([att, y], axis=1), w[...])
        total = part if total is None else total + part
    squares = jnp.mean(total * total, axis=1, keepdims=True)
    out_ref[...] = (total * lax.rsqrt(squares + norm_eps) * gain_ref[...]).astype(BF16)


def finish(mine, core, far, wa, wc, wcore, wx, wxc, gbs, out_gain):
    rows = mine.shape[0]
    width = wa.shape[1]
    return pl.pallas_call(
        functools.partial(final_kernel, wa.shape[0], wc.shape[0]),
        out_shape=jax.ShapeDtypeStruct((rows, width), BF16),
        in_specs=[pl.BlockSpec(memory_space=pltpu.VMEM)] * 13,
        out_specs=pl.BlockSpec(memory_space=pltpu.VMEM),
        cost_estimate=pl.CostEstimate(flops=800_000_000, bytes_accessed=7_000_000, transcendentals=70_000),
        compiler_params=pltpu.CompilerParams(vmem_limit_bytes=32 * 1024 * 1024),
        name="finish_rows",
    )(mine, core, far, wa, wc, wcore, wx, wxc, *gbs, out_gain.reshape(1, width))


def depthwise(padded, conv_taps, rows):
    out = jnp.zeros((rows, padded.shape[1]), F32)
    for tap in range(conv_taps.shape[0]):
        out = out + conv_taps[tap] * padded[tap : tap + rows]
    return out


def paired(
    tokens,
    norm_gain,
    w_query,
    w_key,
    w_value,
    w_glu_value,
    w_glu_gate,
    key_offset,
    head_gain,
    conv_taps,
    channel_gain,
    channel_bias,
    w_out_attn,
    w_out_conv,
    out_gain,
):
    rows, features = tokens.shape
    half_rows, block = rows // 2, w_query.shape[0]
    half = 2 * block
    heads, hd = head_gain.shape
    aw, cw = heads * hd, conv_taps.shape[1]
    me_sp, me_tp = lax.axis_index("sp"), lax.axis_index("tp")
    side, low = me_sp // 2, me_sp % 2
    core = me_tp % 2

    normed = row_norm(tokens.astype(F32), norm_gain).astype(BF16)
    x_send = lax.dynamic_slice(normed, (core * half_rows, (1 - side) * half), (half_rows, half))
    x_got = exchange(x_send, "sp", 2)
    w_attn = jnp.concatenate([w_query, w_key, w_value], axis=1)
    w_attn_pair = exchange(w_attn, "sp", 1)
    w_glu = jnp.concatenate([w_glu_value, w_glu_gate], axis=1)
    w_glu_pair = exchange(w_glu, "sp", 1)
    w_out = jnp.concatenate([w_out_attn, w_out_conv], axis=0)
    w_out_x = exchange(w_out, "tp", 2)
    w_out_core = exchange(w_out, "tp", 1)
    gb = jnp.stack([channel_gain, channel_bias])
    gb_core = exchange(gb, "tp", 1)
    gb_x = exchange(jnp.concatenate([gb, gb_core]), "tp", 2)
    x_other = exchange(x_got, "tp", 1)
    w_out_xc = exchange(w_out_x, "tp", 1)

    x_cross = jnp.where(
        core == 0, jnp.concatenate([x_got, x_other]), jnp.concatenate([x_other, x_got])
    )
    x_mine = lax.dynamic_slice(normed, (0, side * half), (rows, half))
    x_all = jnp.concatenate([x_mine, x_cross])
    x_own = lax.dynamic_slice(x_all, (0, low * block), (2 * rows, block))
    x_pair = lax.dynamic_slice(x_all, (0, (1 - low) * block), (2 * rows, block))

    p = dot_f32(x_own, w_attn) + dot_f32(x_pair, w_attn_pair)
    pq, pk, pv = (p[:, n * aw : (n + 1) * aw] for n in range(3))
    off = jnp.pad(key_offset.T, ((0, 8 - heads), (0, 0)))
    sent = jnp.concatenate([pq[rows:], pk[rows:], pv[rows:], pk[:rows], pv[:rows]]).astype(BF16)
    got = exchange(jnp.concatenate([sent, off, off]), "sp", 2)
    g = [got[n * rows : (n + 1) * rows].astype(F32) for n in range(5)]
    q = (pq[:rows] + g[0]).astype(BF16)
    k_two = jnp.concatenate([pk[:rows] + g[1], pk[rows:] + g[3]]).astype(BF16)
    v_two = jnp.concatenate([pv[:rows] + g[2], pv[rows:] + g[4]]).astype(BF16)
    off_two = jnp.concatenate([off, got[5 * rows : 5 * rows + 8]])
    mine_two = jnp.concatenate([k_two, v_two, off_two])
    pair_two = exchange(mine_two, "sp", 1)

    def slots(first, size):
        a, b = mine_two[first : first + 2 * size], pair_two[first : first + 2 * size]
        return jnp.concatenate([a[:size], b[:size], a[size:], b[size:]])

    k_all, v_all, off_all = slots(0, rows), slots(2 * rows, rows), slots(4 * rows, 8)

    pg = dot_f32(x_own, w_glu) + dot_f32(x_pair, w_glu_pair)
    glu = pg[:rows] + exchange(pg[rows:].astype(BF16), "sp", 2).astype(F32)
    gated = (glu[:, :cw] * jax.nn.sigmoid(glu[:, cw:])).astype(BF16)
    reach = conv_taps.shape[0] - 1
    before = from_behind(gated[rows - reach :], "sp", 1)
    padded = jnp.concatenate([before, gated]).astype(F32)
    conv_out = depthwise(padded, conv_taps, rows).astype(BF16)

    attended, log_mass = attention(q, k_all, v_all, off_all, head_gain)

    act = jnp.concatenate([attended, conv_out], axis=1)
    mine = lax.dynamic_slice(act, (core * half_rows, 0), (half_rows, aw + cw))
    theirs = lax.dynamic_slice(act, ((1 - core) * half_rows, 0), (half_rows, aw + cw))
    from_core = exchange(theirs, "tp", 1)
    far = exchange(jnp.stack([mine, from_core]), "tp", 2)
    gbs = (gb, gb_core, gb_x[:2], gb_x[2:])
    done = finish(mine, from_core, far, w_out_attn, w_out_conv, w_out_core, w_out_x, w_out_xc, gbs, out_gain)
    other = exchange(done, "tp", 1)
    mixed = jnp.where(core == 0, jnp.concatenate([done, other]), jnp.concatenate([other, done]))
    return (mixed, log_mass)


def gathered(
    tokens,
    norm_gain,
    w_query,
    w_key,
    w_value,
    w_glu_value,
    w_glu_gate,
    key_offset,
    head_gain,
    conv_taps,
    channel_gain,
    channel_bias,
    w_out_attn,
    w_out_conv,
    out_gain,
):
    row_count = tokens.shape[0]
    hd = head_gain.shape[1]
    channels = conv_taps.shape[1] * lax.axis_size("tp")
    normed = row_norm(tokens.astype(jnp.float32), norm_gain).astype(jnp.bfloat16)
    weights_in = (w_query, w_key, w_value, w_glu_value, w_glu_gate)
    pieces = (
        lax.all_gather(weights_in[0], "sp", axis=0, tiled=True),
        lax.all_gather(weights_in[1], "sp", axis=0, tiled=True),
        lax.all_gather(weights_in[2], "sp", axis=0, tiled=True),
        lax.all_gather(weights_in[3], "sp", axis=0, tiled=True),
        lax.all_gather(weights_in[4], "sp", axis=0, tiled=True),
    )
    projected = tuple(
        (jnp.dot(normed, shard_piece, preferred_element_type=jnp.float32) for shard_piece in pieces)
    )
    query, key_rows, value_rows, glu_value, glu_gate = [
        summed.astype(jnp.bfloat16) for summed in projected
    ]
    kv_local = key_rows.shape[1] // hd
    group_size = query.shape[1] // key_rows.shape[1]
    heads_local = kv_local * group_size
    all_keys, all_values, all_offsets = (
        lax.all_gather(key_rows, "sp", axis=0, tiled=True),
        lax.all_gather(value_rows, "sp", axis=0, tiled=True),
        lax.all_gather(key_offset, "sp", axis=0, tiled=True),
    )
    sequence_length_total = all_keys.shape[0]
    shard_count = lax.axis_size("sp")
    per_block = 1
    while (
        per_block * 2 <= shard_count
        and shard_count % (per_block * 2) == 0
        and (per_block * 2 * row_count <= 1024)
    ):
        per_block = per_block * 2
    span_len = per_block * row_count
    query_heads = query.reshape(row_count, kv_local, group_size, hd)
    key_heads = all_keys.reshape(sequence_length_total, kv_local, hd)
    value_heads = all_values.reshape(sequence_length_total, kv_local, hd)
    my_index = lax.axis_index("sp")
    query_pos = my_index * row_count + jnp.arange(row_count, dtype=jnp.int32)
    last_block = my_index // per_block
    zeros_mix = jnp.zeros((kv_local, group_size, row_count, hd), jnp.float32)
    zeros_row = jnp.zeros((kv_local, group_size, row_count), jnp.float32)

    def sweep(turn_index, carry):
        head_mix, mass_sum, carried = carry
        first_key = (last_block - turn_index) * span_len
        key_block = lax.dynamic_slice_in_dim(key_heads, first_key, span_len, 0)
        value_block = lax.dynamic_slice_in_dim(value_heads, first_key, span_len, 0)
        offset_block = lax.dynamic_slice_in_dim(all_offsets, first_key, span_len, 0).astype(
            jnp.float32
        )
        offset_block = offset_block.T.reshape(kv_local, group_size, 1, span_len)
        scores = (
            jnp.einsum("qhgd,khd->hgqk", query_heads, key_block, preferred_element_type=jnp.float32)
            * hd ** (-0.5)
            + offset_block
        )
        key_pos = first_key + jnp.arange(span_len, dtype=jnp.int32)
        allowed = key_pos[None, :] <= query_pos[:, None]
        log_not = jnp.where(allowed, jax.nn.log_sigmoid(-scores), 0.0)
        later = lax.cumsum(log_not, axis=3, reverse=True) - log_not + carried[..., None]
        weights = jnp.where(allowed, jnp.exp(jax.nn.log_sigmoid(scores) + later), 0.0)
        head_mix = head_mix + jnp.einsum(
            "hgqk,khd->hgqd",
            weights.astype(jnp.bfloat16),
            value_block,
            preferred_element_type=jnp.float32,
        )
        return (head_mix, mass_sum + jnp.sum(weights, axis=3), carried + jnp.sum(log_not, axis=3))

    head_mix, mass_sum, leftover = lax.fori_loop(
        0, last_block + 1, sweep, (zeros_mix, zeros_row, zeros_row)
    )
    log_mass = jnp.log(mass_sum).reshape(heads_local, row_count)
    head_rows = head_mix.transpose(2, 0, 1, 3).reshape(row_count, heads_local, hd)
    attended = (
        row_norm(head_rows, head_gain).astype(jnp.bfloat16).reshape(row_count, heads_local * hd)
    )
    gated = (glu_value.astype(jnp.float32) * jax.nn.sigmoid(glu_gate.astype(jnp.float32))).astype(
        jnp.bfloat16
    )
    reach_len = conv_taps.shape[0] - 1
    before = from_behind(gated[row_count - reach_len :], "sp", 1)
    padded = jnp.concatenate([before, gated], axis=0).astype(jnp.float32)
    conv_out = jnp.zeros(gated.shape, jnp.float32)
    for tap_index in range(conv_taps.shape[0]):
        conv_out = conv_out + conv_taps[tap_index] * padded[tap_index : tap_index + row_count]
    total_sum, total_squares = lax.psum(
        (jnp.sum(conv_out, axis=1), jnp.sum(conv_out * conv_out, axis=1)), "tp"
    )
    chan_mean = (total_sum / channels)[:, None]
    spread = (total_squares / channels)[:, None] - chan_mean * chan_mean
    centered = conv_out - chan_mean
    channel_out = jax.nn.silu(
        centered * lax.rsqrt(spread + norm_eps) * channel_gain + channel_bias
    ).astype(jnp.bfloat16)
    share = lax.psum_scatter(
        jnp.dot(attended, w_out_attn, preferred_element_type=jnp.float32)
        + jnp.dot(channel_out, w_out_conv, preferred_element_type=jnp.float32),
        "tp",
        scatter_dimension=0,
        tiled=True,
    )
    mixed = lax.all_gather(row_norm(share, out_gain).astype(jnp.bfloat16), "tp", axis=0, tiled=True)
    return (mixed, log_mass)


def solution(mesh):
    in_specs = (
        P(("grp", "sp"), None),
        P(),
        P("sp", "tp"),
        P("sp", "tp"),
        P("sp", "tp"),
        P("sp", "tp"),
        P("sp", "tp"),
        P(("grp", "sp"), "tp"),
        P("tp", None),
        P(None, "tp"),
        P("tp"),
        P("tp"),
        P("tp", None),
        P("tp", None),
        P(),
    )
    out_specs = (P(("grp", "sp"), None), P("tp", ("grp", "sp")))
    small = mesh.shape["sp"] == 4 and mesh.shape["tp"] == 4
    local = paired if small else gathered
    return jax.shard_map(local, mesh=mesh, in_specs=in_specs, out_specs=out_specs, check_vma=False)
```

```python
import functools

import jax
import jax.numpy as jnp
from jax import lax
from jax.experimental import pallas as pl
from jax.experimental.pallas import tpu as pltpu
from jax.sharding import PartitionSpec as P

norm_eps = 1e-06
BF16 = jnp.bfloat16
F32 = jnp.float32


def exchange(value, axis, bit):
    count = lax.axis_size(axis)
    return lax.ppermute(value, axis, [(s, s ^ bit) for s in range(count)])


def from_behind(value, axis, steps):
    count = lax.axis_size(axis)
    initial, last = (max(0, -steps), min(count, count - steps))
    return lax.ppermute(value, axis, [(source, source + steps) for source in range(initial, last)])


def row_norm(values_in, gain_vec):
    squares = jnp.mean(values_in * values_in, axis=-1, keepdims=True)
    return values_in * lax.rsqrt(squares + norm_eps) * gain_vec


def dot_f32(a, b, dims=((1,), (0,))):
    return lax.dot_general(a, b, (dims, ((), ())), preferred_element_type=F32)


def attention_kernel(hd, q_ref, k_ref, v_ref, off_ref, gain_ref, out_ref, mass_ref, acc, mass, carry):
    me = lax.axis_index("sp")
    rows, width = q_ref.shape
    heads = width // hd
    lane = lax.broadcasted_iota(jnp.int32, (rows, width), 1) // hd
    keys = rows
    before = lax.broadcasted_iota(jnp.int32, (2 * keys, 2 * keys), 0) % keys
    column = lax.broadcasted_iota(jnp.int32, (2 * keys, 2 * keys), 1)
    suffix = jnp.where((column >= keys) | (before > column), 1.0, 0.0).astype(BF16)
    q = q_ref[...]
    scale = hd ** (-0.5)

    def block(slot, first):
        start = pl.multiple_of(slot * keys, keys)
        k = k_ref[pl.ds(start, keys), :]
        v = v_ref[pl.ds(start, keys), :]
        off = off_ref[pl.ds(pl.multiple_of(slot * 8, 8), 8), :].astype(F32)
        parts = []
        for h in range(heads):
            qh = jnp.where(lane == h, q, jnp.zeros_like(q))
            s = dot_f32(qh, k, ((1,), (1,))) * scale + off[h : h + 1, :]
            soft = jnp.maximum(s, 0.0) + jnp.log(1.0 + jnp.exp(-jnp.abs(s)))
            if first:
                allowed = lax.broadcasted_iota(jnp.int32, (rows, keys), 1) <= lax.broadcasted_iota(
                    jnp.int32, (rows, keys), 0
                )
                log_not = jnp.where(allowed, -soft, 0.0)
            else:
                log_not = -soft
            high = log_not.astype(BF16)
            low = (log_not - high.astype(F32)).astype(BF16)
            sums = dot_f32(jnp.concatenate([high, low], axis=1), suffix)
            later, total = sums[:, :keys], sums[:, keys:]
            if not first:
                later = later + carry[h]
            w = jnp.exp(s - soft + later)
            if first:
                w = jnp.where(allowed, w, 0.0)
                mass[h] = w
                carry[h] = total
            else:
                mass[h] = mass[h] + w
                carry[h] = carry[h] + total
            parts.append((w.astype(BF16), jnp.where(lane == h, v, jnp.zeros_like(v))))
        mix = dot_f32(
            jnp.concatenate([w for w, _ in parts], axis=1),
            jnp.concatenate([v for _, v in parts], axis=0),
        )
        if first:
            acc[...] = mix
        else:
            acc[...] = acc[...] + mix

    block(0, True)

    def earlier(t, _):
        block(jnp.bitwise_xor(me - t, me), False)
        return 0

    lax.fori_loop(1, me + 1, earlier, 0)
    mixed = acc[...]
    squares = mixed * mixed
    inverse = jnp.zeros_like(mixed)
    for h in range(heads):
        mean = jnp.sum(jnp.where(lane == h, squares, 0.0), axis=1, keepdims=True) / hd
        inverse = jnp.where(lane == h, lax.rsqrt(mean + norm_eps), inverse)
    out_ref[...] = (mixed * inverse * gain_ref[...]).astype(BF16)
    for h in range(heads):
        mass_ref[h : h + 1, :] = jnp.log(jnp.sum(jnp.transpose(mass[h]), axis=0, keepdims=True))


def attention(q, k, v, off, head_gain):
    rows, width = q.shape
    heads, hd = head_gain.shape
    out_shape = (jax.ShapeDtypeStruct((rows, width), BF16), jax.ShapeDtypeStruct((heads, rows), F32))
    return pl.pallas_call(
        functools.partial(attention_kernel, hd),
        out_shape=out_shape,
        in_specs=[pl.BlockSpec(memory_space=pltpu.VMEM)] * 5,
        out_specs=[pl.BlockSpec(memory_space=pltpu.VMEM)] * 2,
        scratch_shapes=[
            pltpu.VMEM((rows, width), F32),
            pltpu.VMEM((heads, rows, rows), F32),
            pltpu.VMEM((heads, rows, rows), F32),
        ],
        cost_estimate=pl.CostEstimate(flops=400_000_000, bytes_accessed=1_000_000, transcendentals=400_000),
        compiler_params=pltpu.CompilerParams(vmem_limit_bytes=16 * 1024 * 1024),
        name="stick_attention",
    )(q, k, v, off, head_gain.reshape(1, width))


def norm_kernel(rows_out, x_ref, gain_ref, send_ref, own_ref, pair_ref, normed):
    side, low = lax.axis_index("sp") // 2, lax.axis_index("sp") % 2
    core = lax.axis_index("tp") % 2
    block = own_ref.shape[1]
    half = 2 * block
    x = x_ref[...].astype(F32)
    squares = jnp.mean(x * x, axis=1, keepdims=True)
    normed[...] = (x * lax.rsqrt(squares + norm_eps) * gain_ref[...]).astype(BF16)
    first = pl.multiple_of(core * rows_out, rows_out)
    away = pl.multiple_of((1 - side) * half, half)
    send_ref[...] = normed[pl.ds(first, rows_out), pl.ds(away, half)]
    own_ref[...] = normed[:, pl.ds(pl.multiple_of(side * half + low * block, block), block)]
    pair_ref[...] = normed[:, pl.ds(pl.multiple_of(side * half + (1 - low) * block, block), block)]


def norm_parts(tokens, gain, block):
    rows, features = tokens.shape
    return pl.pallas_call(
        functools.partial(norm_kernel, rows // 2),
        out_shape=(
            jax.ShapeDtypeStruct((rows // 2, 2 * block), BF16),
            jax.ShapeDtypeStruct((rows, block), BF16),
            jax.ShapeDtypeStruct((rows, block), BF16),
        ),
        in_specs=[pl.BlockSpec(memory_space=pltpu.VMEM)] * 2,
        out_specs=[pl.BlockSpec(memory_space=pltpu.VMEM)] * 3,
        scratch_shapes=[pltpu.VMEM((rows, features), BF16)],
        cost_estimate=pl.CostEstimate(flops=2_000_000, bytes_accessed=1_000_000, transcendentals=128),
        compiler_params=pltpu.CompilerParams(vmem_limit_bytes=16 * 1024 * 1024),
        name="norm_parts",
    )(tokens, gain.reshape(1, features))


def assemble_kernel(own_ref, pair_ref, got_ref, other_ref, own_out, pair_out):
    low = lax.axis_index("sp") % 2
    core = lax.axis_index("tp") % 2
    rows, block = own_ref.shape
    half = got_ref.shape[0]
    own_out[:rows, :] = own_ref[...]
    pair_out[:rows, :] = pair_ref[...]
    own_at = pl.multiple_of(low * block, block)
    pair_at = pl.multiple_of((1 - low) * block, block)
    for part, at in ((got_ref, core), (other_ref, 1 - core)):
        first = pl.multiple_of(rows + at * half, half)
        own_out[pl.ds(first, half), :] = part[:, pl.ds(own_at, block)]
        pair_out[pl.ds(first, half), :] = part[:, pl.ds(pair_at, block)]


def assemble(own, pair, got, other):
    rows, block = own.shape
    shape = jax.ShapeDtypeStruct((2 * rows, block), BF16)
    return pl.pallas_call(
        assemble_kernel,
        out_shape=(shape, shape),
        in_specs=[pl.BlockSpec(memory_space=pltpu.VMEM)] * 4,
        out_specs=[pl.BlockSpec(memory_space=pltpu.VMEM)] * 2,
        cost_estimate=pl.CostEstimate(flops=2_000_000, bytes_accessed=1_000_000, transcendentals=0),
        compiler_params=pltpu.CompilerParams(vmem_limit_bytes=16 * 1024 * 1024),
        name="assemble",
    )(own, pair, got, other)


def final_kernel(*refs):
    att, conv, wa, wc, gb = (refs[n * 4 : (n + 1) * 4] for n in range(5))
    gain_ref, out_ref = refs[20:]
    convs = [c[...].astype(F32) for c in conv]
    count = 4 * convs[0].shape[1]
    mean = sum(jnp.sum(v, axis=1, keepdims=True) for v in convs) / count
    centered = [v - mean for v in convs]
    spread = sum(jnp.sum(v * v, axis=1, keepdims=True) for v in centered) / count
    inverse = lax.rsqrt(spread + norm_eps)
    acts = []
    for slot in range(4):
        y = centered[slot] * inverse * gb[slot][0:1, :] + gb[slot][1:2, :]
        acts.append((y * jax.nn.sigmoid(y)).astype(BF16))
    total = None
    for slot in range(4):
        part = dot_f32(att[slot][...], wa[slot][...]) + dot_f32(acts[slot], wc[slot][...])
        total = part if total is None else total + part
    squares = jnp.mean(total * total, axis=1, keepdims=True)
    out_ref[...] = (total * lax.rsqrt(squares + norm_eps) * gain_ref[...]).astype(BF16)


def finish(att, conv, wa, wc, gb, out_gain):
    rows, width = att[0].shape[0], wa[0].shape[1]
    return pl.pallas_call(
        final_kernel,
        out_shape=jax.ShapeDtypeStruct((rows, width), BF16),
        in_specs=[pl.BlockSpec(memory_space=pltpu.VMEM)] * 21,
        out_specs=pl.BlockSpec(memory_space=pltpu.VMEM),
        cost_estimate=pl.CostEstimate(flops=800_000_000, bytes_accessed=7_000_000, transcendentals=70_000),
        compiler_params=pltpu.CompilerParams(vmem_limit_bytes=32 * 1024 * 1024),
        name="finish_rows",
    )(*att, *conv, *wa, *wc, *gb, out_gain.reshape(1, width))


def depthwise(padded, conv_taps, rows):
    out = jnp.zeros((rows, padded.shape[1]), F32)
    for tap in range(conv_taps.shape[0]):
        out = out + conv_taps[tap] * padded[tap : tap + rows]
    return out


def paired(
    tokens,
    norm_gain,
    w_query,
    w_key,
    w_value,
    w_glu_value,
    w_glu_gate,
    key_offset,
    head_gain,
    conv_taps,
    channel_gain,
    channel_bias,
    w_out_attn,
    w_out_conv,
    out_gain,
):
    rows = tokens.shape[0]
    heads, _ = head_gain.shape
    x_send, mine_own, mine_pair = norm_parts(tokens, norm_gain, w_query.shape[0])
    x_got = exchange(x_send, "sp", 2)
    wk_pair = exchange(w_key, "sp", 1)
    wv_pair = exchange(w_value, "sp", 1)
    gv_pair = exchange(w_glu_value, "sp", 1)
    gg_pair = exchange(w_glu_gate, "sp", 1)
    wq_pair = exchange(w_query, "sp", 1)
    wa_x = exchange(w_out_attn, "tp", 2)
    wc_x = exchange(w_out_conv, "tp", 2)
    wa_core = exchange(w_out_attn, "tp", 1)
    wc_core = exchange(w_out_conv, "tp", 1)
    gb = jnp.stack([channel_gain, channel_bias])
    gbs = [gb] + [exchange(gb, "tp", bit) for bit in (1, 2, 3)]
    x_other = exchange(x_got, "tp", 1)
    wa_xc = exchange(wa_x, "tp", 1)
    wc_xc = exchange(wc_x, "tp", 1)

    x_own, x_pair = assemble(mine_own, mine_pair, x_got, x_other)

    def project(own, pair):
        return dot_f32(x_own, own) + dot_f32(x_pair, pair)

    off = jnp.pad(key_offset.T, ((0, 8 - heads), (0, 0)))
    pk = project(w_key, wk_pair)
    k_got = exchange(jnp.concatenate([pk[rows:], pk[:rows]]).astype(BF16), "sp", 2)
    pv = project(w_value, wv_pair)
    v_sent = jnp.concatenate([pv[rows:], pv[:rows]]).astype(BF16)
    v_got = exchange(jnp.concatenate([v_sent, off, off]), "sp", 2)
    k_two = (pk + k_got.astype(F32)).astype(BF16)
    v_two = (pv + v_got[: 2 * rows].astype(F32)).astype(BF16)
    mine_two = jnp.concatenate([k_two, v_two, off, v_got[2 * rows : 2 * rows + 8]])
    pair_two = exchange(mine_two, "sp", 1)

    def slots(first, size):
        a, b = mine_two[first : first + 2 * size], pair_two[first : first + 2 * size]
        return jnp.concatenate([a[:size], b[:size], a[size:], b[size:]])

    k_all, v_all, off_all = slots(0, rows), slots(2 * rows, rows), slots(4 * rows, 8)

    pgv = project(w_glu_value, gv_pair)
    gv = pgv[:rows] + exchange(pgv[rows:].astype(BF16), "sp", 2).astype(F32)
    pgg = project(w_glu_gate, gg_pair)
    gg = pgg[:rows] + exchange(pgg[rows:].astype(BF16), "sp", 2).astype(F32)
    pq = project(w_query, wq_pair)
    q = (pq[:rows] + exchange(pq[rows:].astype(BF16), "sp", 2).astype(F32)).astype(BF16)

    gated = (gv * jax.nn.sigmoid(gg)).astype(BF16)
    reach = conv_taps.shape[0] - 1
    before = from_behind(gated[rows - reach :], "sp", 1)

    attended, log_mass = attention(q, k_all, v_all, off_all, head_gain)
    att = [attended] + [exchange(attended, "tp", bit) for bit in (1, 2, 3)]

    padded = jnp.concatenate([before, gated]).astype(F32)
    conv_out = depthwise(padded, conv_taps, rows).astype(BF16)
    conv = [conv_out] + [exchange(conv_out, "tp", bit) for bit in (1, 2, 3)]
    wa = (w_out_attn, wa_core, wa_x, wa_xc)
    wc = (w_out_conv, wc_core, wc_x, wc_xc)
    mixed = finish(att, conv, wa, wc, gbs, out_gain)
    return (mixed, log_mass)


def gathered(
    tokens,
    norm_gain,
    w_query,
    w_key,
    w_value,
    w_glu_value,
    w_glu_gate,
    key_offset,
    head_gain,
    conv_taps,
    channel_gain,
    channel_bias,
    w_out_attn,
    w_out_conv,
    out_gain,
):
    row_count = tokens.shape[0]
    hd = head_gain.shape[1]
    channels = conv_taps.shape[1] * lax.axis_size("tp")
    normed = row_norm(tokens.astype(jnp.float32), norm_gain).astype(jnp.bfloat16)
    weights_in = (w_query, w_key, w_value, w_glu_value, w_glu_gate)
    pieces = (
        lax.all_gather(weights_in[0], "sp", axis=0, tiled=True),
        lax.all_gather(weights_in[1], "sp", axis=0, tiled=True),
        lax.all_gather(weights_in[2], "sp", axis=0, tiled=True),
        lax.all_gather(weights_in[3], "sp", axis=0, tiled=True),
        lax.all_gather(weights_in[4], "sp", axis=0, tiled=True),
    )
    projected = tuple(
        (jnp.dot(normed, shard_piece, preferred_element_type=jnp.float32) for shard_piece in pieces)
    )
    query, key_rows, value_rows, glu_value, glu_gate = [
        summed.astype(jnp.bfloat16) for summed in projected
    ]
    kv_local = key_rows.shape[1] // hd
    group_size = query.shape[1] // key_rows.shape[1]
    heads_local = kv_local * group_size
    all_keys, all_values, all_offsets = (
        lax.all_gather(key_rows, "sp", axis=0, tiled=True),
        lax.all_gather(value_rows, "sp", axis=0, tiled=True),
        lax.all_gather(key_offset, "sp", axis=0, tiled=True),
    )
    sequence_length_total = all_keys.shape[0]
    shard_count = lax.axis_size("sp")
    per_block = 1
    while (
        per_block * 2 <= shard_count
        and shard_count % (per_block * 2) == 0
        and (per_block * 2 * row_count <= 1024)
    ):
        per_block = per_block * 2
    span_len = per_block * row_count
    query_heads = query.reshape(row_count, kv_local, group_size, hd)
    key_heads = all_keys.reshape(sequence_length_total, kv_local, hd)
    value_heads = all_values.reshape(sequence_length_total, kv_local, hd)
    my_index = lax.axis_index("sp")
    query_pos = my_index * row_count + jnp.arange(row_count, dtype=jnp.int32)
    last_block = my_index // per_block
    zeros_mix = jnp.zeros((kv_local, group_size, row_count, hd), jnp.float32)
    zeros_row = jnp.zeros((kv_local, group_size, row_count), jnp.float32)

    def sweep(turn_index, carry):
        head_mix, mass_sum, carried = carry
        first_key = (last_block - turn_index) * span_len
        key_block = lax.dynamic_slice_in_dim(key_heads, first_key, span_len, 0)
        value_block = lax.dynamic_slice_in_dim(value_heads, first_key, span_len, 0)
        offset_block = lax.dynamic_slice_in_dim(all_offsets, first_key, span_len, 0).astype(
            jnp.float32
        )
        offset_block = offset_block.T.reshape(kv_local, group_size, 1, span_len)
        scores = (
            jnp.einsum("qhgd,khd->hgqk", query_heads, key_block, preferred_element_type=jnp.float32)
            * hd ** (-0.5)
            + offset_block
        )
        key_pos = first_key + jnp.arange(span_len, dtype=jnp.int32)
        allowed = key_pos[None, :] <= query_pos[:, None]
        log_not = jnp.where(allowed, jax.nn.log_sigmoid(-scores), 0.0)
        later = lax.cumsum(log_not, axis=3, reverse=True) - log_not + carried[..., None]
        weights = jnp.where(allowed, jnp.exp(jax.nn.log_sigmoid(scores) + later), 0.0)
        head_mix = head_mix + jnp.einsum(
            "hgqk,khd->hgqd",
            weights.astype(jnp.bfloat16),
            value_block,
            preferred_element_type=jnp.float32,
        )
        return (head_mix, mass_sum + jnp.sum(weights, axis=3), carried + jnp.sum(log_not, axis=3))

    head_mix, mass_sum, _ = lax.fori_loop(
        0, last_block + 1, sweep, (zeros_mix, zeros_row, zeros_row)
    )
    log_mass = jnp.log(mass_sum).reshape(heads_local, row_count)
    head_rows = head_mix.transpose(2, 0, 1, 3).reshape(row_count, heads_local, hd)
    attended = (
        row_norm(head_rows, head_gain).astype(jnp.bfloat16).reshape(row_count, heads_local * hd)
    )
    gated = (glu_value.astype(jnp.float32) * jax.nn.sigmoid(glu_gate.astype(jnp.float32))).astype(
        jnp.bfloat16
    )
    reach_len = conv_taps.shape[0] - 1
    before = from_behind(gated[row_count - reach_len :], "sp", 1)
    padded = jnp.concatenate([before, gated], axis=0).astype(jnp.float32)
    conv_out = jnp.zeros(gated.shape, jnp.float32)
    for tap_index in range(conv_taps.shape[0]):
        conv_out = conv_out + conv_taps[tap_index] * padded[tap_index : tap_index + row_count]
    total_sum, total_squares = lax.psum(
        (jnp.sum(conv_out, axis=1), jnp.sum(conv_out * conv_out, axis=1)), "tp"
    )
    chan_mean = (total_sum / channels)[:, None]
    spread = (total_squares / channels)[:, None] - chan_mean * chan_mean
    centered = conv_out - chan_mean
    channel_out = jax.nn.silu(
        centered * lax.rsqrt(spread + norm_eps) * channel_gain + channel_bias
    ).astype(jnp.bfloat16)
    share = lax.psum_scatter(
        jnp.dot(attended, w_out_attn, preferred_element_type=jnp.float32)
        + jnp.dot(channel_out, w_out_conv, preferred_element_type=jnp.float32),
        "tp",
        scatter_dimension=0,
        tiled=True,
    )
    mixed = lax.all_gather(row_norm(share, out_gain).astype(jnp.bfloat16), "tp", axis=0, tiled=True)
    return (mixed, log_mass)


def solution(mesh):
    in_specs = (
        P(("grp", "sp"), None),
        P(),
        P("sp", "tp"),
        P("sp", "tp"),
        P("sp", "tp"),
        P("sp", "tp"),
        P("sp", "tp"),
        P(("grp", "sp"), "tp"),
        P("tp", None),
        P(None, "tp"),
        P("tp"),
        P("tp"),
        P("tp", None),
        P("tp", None),
        P(),
    )
    out_specs = (P(("grp", "sp"), None), P("tp", ("grp", "sp")))
    small = mesh.shape["sp"] == 4 and mesh.shape["tp"] == 4
    local = paired if small else gathered
    return jax.shard_map(local, mesh=mesh, in_specs=in_specs, out_specs=out_specs, check_vma=False)
```

```python
import jax
import jax.numpy as jnp
from jax import lax
from jax.experimental import pallas as pl
from jax.experimental.pallas import tpu as pltpu
from jax.sharding import PartitionSpec as P

norm_eps = 1e-06
BF16 = jnp.bfloat16
F32 = jnp.float32


def exchange(value, axis, bit):
    count = lax.axis_size(axis)
    return lax.ppermute(value, axis, [(s, s ^ bit) for s in range(count)])


def from_behind(value, axis, steps):
    count = lax.axis_size(axis)
    initial, last = (max(0, -steps), min(count, count - steps))
    return lax.ppermute(value, axis, [(source, source + steps) for source in range(initial, last)])


def row_norm(values_in, gain_vec):
    squares = jnp.mean(values_in * values_in, axis=-1, keepdims=True)
    return values_in * lax.rsqrt(squares + norm_eps) * gain_vec


def dot_f32(a, b, dims=((1,), (0,))):
    return lax.dot_general(a, b, (dims, ((), ())), preferred_element_type=F32)


FULL = 60


def params(limit=16):
    return pltpu.CompilerParams(vmem_limit_bytes=limit * 1024 * 1024)


VM = pl.BlockSpec(memory_space=pltpu.VMEM)
ANY = pl.BlockSpec(memory_space=pl.ANY)
HBM = pl.BlockSpec(memory_space=pltpu.HBM)


def shape(dims, dtype=BF16):
    return jax.ShapeDtypeStruct(dims, dtype)


def cost(flops, moved):
    return pl.CostEstimate(flops=flops, bytes_accessed=moved, transcendentals=0)


def norm_kernel(x_hbm, gain_hbm, *refs):
    weights = refs[:3]
    send_ref, own_ref, pair_ref, pack_ref, x_ref, gain_ref, normed, sems = refs[3:]
    side, low = lax.axis_index("sp") // 2, lax.axis_index("sp") % 2
    core = lax.axis_index("tp") % 2
    block, width = weights[0].shape
    half = 2 * block
    half_rows = send_ref.shape[0]
    part = block // 2
    mine = pl.ds(pl.multiple_of(lax.axis_index("grp") * part, part), part)
    copies = [
        pltpu.make_async_copy(x_hbm, x_ref, sems.at[0]),
        pltpu.make_async_copy(gain_hbm, gain_ref, sems.at[1]),
    ]
    for n, w in enumerate(weights):
        at = slice(n * width, (n + 1) * width)
        copies.append(pltpu.make_async_copy(w.at[mine, :], pack_ref.at[:, at], sems.at[2 + n]))
    for copy in copies:
        copy.start()
    copies[0].wait()
    copies[1].wait()
    x = x_ref[...].astype(F32)
    squares = jnp.mean(x * x, axis=1, keepdims=True)
    normed[...] = (x * lax.rsqrt(squares + norm_eps) * gain_ref[...]).astype(BF16)
    first = pl.multiple_of(core * half_rows, half_rows)
    away = pl.multiple_of((1 - side) * half, half)
    send_ref[...] = normed[pl.ds(first, half_rows), pl.ds(away, half)]
    own_ref[...] = normed[:, pl.ds(pl.multiple_of(side * half + low * block, block), block)]
    pair_ref[...] = normed[:, pl.ds(pl.multiple_of(side * half + (1 - low) * block, block), block)]
    for copy in copies[2:]:
        copy.wait()


def norm_parts(tokens, gain, weights):
    rows, features = tokens.shape
    block, width = weights[0].shape
    return pl.pallas_call(
        norm_kernel,
        out_shape=(
            shape((rows // 2, 2 * block)),
            shape((rows, block)),
            shape((rows, block)),
            shape((block // 2, 3 * width)),
        ),
        in_specs=[HBM] * 5,
        out_specs=[VM] * 4,
        scratch_shapes=[
            pltpu.VMEM((rows, features), BF16),
            pltpu.VMEM((1, features), F32),
            pltpu.VMEM((rows, features), BF16),
            pltpu.SemaphoreType.DMA((5,)),
        ],
        cost_estimate=cost(2_000_000, 1_000_000),
        compiler_params=params(FULL),
        name="norm_parts",
    )(tokens, gain.reshape(1, features), *weights)


def pack_kernel(gv_hbm, gg_hbm, wa_hbm, gain_hbm, bias_hbm, glu_ref, out_ref, gain_ref, bias_ref, sems):
    cw, aw = gv_hbm.shape[1], wa_hbm.shape[0]
    part = glu_ref.shape[0]
    mine = pl.ds(pl.multiple_of(lax.axis_index("grp") * part, part), part)
    copies = [
        pltpu.make_async_copy(gv_hbm.at[mine, :], glu_ref.at[:, :cw], sems.at[0]),
        pltpu.make_async_copy(gg_hbm.at[mine, :], glu_ref.at[:, cw:], sems.at[1]),
        pltpu.make_async_copy(wa_hbm, out_ref.at[:aw, :], sems.at[2]),
    ]
    small = [
        pltpu.make_async_copy(gain_hbm, gain_ref, sems.at[3]),
        pltpu.make_async_copy(bias_hbm, bias_ref, sems.at[4]),
    ]
    for copy in small + copies:
        copy.start()
    for copy in small:
        copy.wait()
    extra = out_ref.shape[0] - aw
    for n, ref in enumerate((gain_ref, bias_ref)):
        rest = ref[...]
        for piece in range(3):
            part = rest.astype(BF16)
            rest = rest - part.astype(F32)
            first = (3 * n + piece) * cw
            out_ref[aw:, first : first + cw] = jnp.broadcast_to(part, (extra, cw))
    for copy in copies:
        copy.wait()


def pack(gv, gg, wa, gain, bias):
    block, cw = gv.shape
    aw, width = wa.shape
    return pl.pallas_call(
        pack_kernel,
        out_shape=(shape((block // 2, 2 * cw)), shape((aw + 16, width))),
        in_specs=[HBM] * 5,
        out_specs=[VM] * 2,
        scratch_shapes=[
            pltpu.VMEM((1, cw), F32),
            pltpu.VMEM((1, cw), F32),
            pltpu.SemaphoreType.DMA((5,)),
        ],
        cost_estimate=cost(2_000_000, 2_000_000),
        compiler_params=params(FULL),
        name="pack",
    )(gv, gg, wa, gain.reshape(1, cw), bias.reshape(1, cw))


def assemble_kernel(own_ref, pair_ref, got_ref, other_ref, own_out, pair_out):
    low = lax.axis_index("sp") % 2
    core = lax.axis_index("tp") % 2
    rows, block = own_ref.shape
    half = got_ref.shape[0]
    own_out[:rows, :] = own_ref[...]
    pair_out[:rows, :] = pair_ref[...]
    own_at = pl.multiple_of(low * block, block)
    pair_at = pl.multiple_of((1 - low) * block, block)
    for part, at in ((got_ref, core), (other_ref, 1 - core)):
        first = pl.multiple_of(rows + at * half, half)
        own_out[pl.ds(first, half), :] = part[:, pl.ds(own_at, block)]
        pair_out[pl.ds(first, half), :] = part[:, pl.ds(pair_at, block)]


def assemble(own, pair, got, other):
    rows, block = own.shape
    return pl.pallas_call(
        assemble_kernel,
        out_shape=(shape((2 * rows, block)),) * 2,
        in_specs=[VM] * 4,
        out_specs=[VM] * 2,
        cost_estimate=cost(2_000_000, 1_000_000),
        compiler_params=params(),
        name="assemble",
    )(own, pair, got, other)


def far_dot(x_pair, same, other):
    part = same.shape[0]
    group = lax.axis_index("grp")
    near = x_pair[:, pl.ds(pl.multiple_of(group * part, part), part)]
    rest = x_pair[:, pl.ds(pl.multiple_of((1 - group) * part, part), part)]
    return dot_f32(near, same[...]) + dot_f32(rest, other[...])


def qkv_kernel(x_own, x_pair, wq, wk, wv, same, other, off_ref, keep_ref, send_ref):
    rows = x_own.shape[0] // 2
    width = wk.shape[1]
    far = far_dot(x_pair, same, other)
    for n, w in enumerate((wq, wk, wv)):
        at = slice(n * width, (n + 1) * width)
        part = dot_f32(x_own[...], w[...]) + far[:, at]
        keep_ref[:, at] = part
        first = 4 * rows if n == 0 else 2 * (n - 1) * rows
        send_ref[first : first + rows, :] = part[rows:].astype(BF16)
        if n > 0:
            send_ref[first + rows : first + 2 * rows, :] = part[:rows].astype(BF16)
    send_ref[5 * rows :, :] = jnp.zeros((send_ref.shape[0] - 5 * rows, width), BF16)
    send_ref[5 * rows : 5 * rows + off_ref.shape[0], :] = off_ref[...]


def project_qkv(x_own, x_pair, own, same, other, off):
    rows, width = x_own.shape[0], own[0].shape[1]
    return pl.pallas_call(
        qkv_kernel,
        out_shape=(shape((rows, 3 * width), F32), shape((5 * rows // 2 + 16, width))),
        in_specs=[VM] * 8,
        out_specs=[VM] * 2,
        cost_estimate=cost(200_000_000, 1_000_000),
        compiler_params=params(),
        name="project_qkv",
    )(x_own, x_pair, *own, same, other, off)


def sum_kernel(keep_ref, got_ref, sent_ref, after, q_ref, out_ref):
    rows, width = q_ref.shape

    def got(n):
        return got_ref[n * rows : (n + 1) * rows, :].astype(F32)

    q_ref[...] = (keep_ref[:rows, :width] + got(4)).astype(BF16)
    for n in range(4):
        at = slice((1 + n // 2) * width, (2 + n // 2) * width)
        part = keep_ref[(n % 2) * rows : (n % 2 + 1) * rows, at]
        out_ref[n * rows : (n + 1) * rows, :] = (part + got(n)).astype(BF16)
    first = 5 * rows
    out_ref[4 * rows :, :] = jnp.concatenate([sent_ref[first : first + 8, :], got_ref[first : first + 8, :]])


def sum_qkv(keep, got, sent, after):
    rows, width = keep.shape[0] // 2, got.shape[1]
    return pl.pallas_call(
        sum_kernel,
        out_shape=(shape((rows, width)), shape((4 * rows + 16, width))),
        in_specs=[VM] * 3 + [ANY],
        out_specs=[VM] * 2,
        cost_estimate=cost(1_000_000, 1_000_000),
        compiler_params=params(),
        name="sum_qkv",
    )(keep, got, sent, after)


def glu_kernel(x_own, x_pair, gv, gg, same, other, after, keep_ref, send_ref):
    rows = x_own.shape[0] // 2
    cw = gv.shape[1]
    far = far_dot(x_pair, same, other)
    for n, w in enumerate((gv, gg)):
        at = slice(n * cw, (n + 1) * cw)
        part = dot_f32(x_own[...], w[...]) + far[:, at]
        keep_ref[:, at] = part[:rows]
        send_ref[:, at] = part[rows:].astype(BF16)


def project_glu(x_own, x_pair, own, same, other, after):
    rows, width = x_own.shape[0] // 2, same.shape[1]
    return pl.pallas_call(
        glu_kernel,
        out_shape=(shape((rows, width), F32), shape((rows, width))),
        in_specs=[VM] * 6 + [ANY],
        out_specs=[VM] * 2,
        cost_estimate=cost(270_000_000, 1_500_000),
        compiler_params=params(),
        name="project_glu",
    )(x_own, x_pair, *own, same, other, after)


def gate_kernel(keep_ref, got_ref, gated_ref, tail_ref):
    rows, cw = gated_ref.shape
    glu = keep_ref[...] + got_ref[...].astype(F32)
    value = glu[:, :cw].astype(BF16).astype(F32)
    gate = glu[:, cw:].astype(BF16).astype(F32)
    gated = (value * jax.nn.sigmoid(gate)).astype(BF16)
    gated_ref[...] = gated
    tail_ref[...] = gated[rows - tail_ref.shape[0] :]


def gate(keep, got, tail):
    rows, cw = keep.shape[0], keep.shape[1] // 2
    return pl.pallas_call(
        gate_kernel,
        out_shape=(shape((rows, cw)), shape((tail, cw))),
        in_specs=[VM] * 2,
        out_specs=[VM] * 2,
        cost_estimate=cost(2_000_000, 500_000),
        compiler_params=params(),
        name="gate",
    )(keep, got)


def conv_kernel(gated_ref, before_ref, taps_ref, att_ref, act_ref, padded):
    rows, aw = att_ref.shape
    tail = before_ref.shape[0]
    taps = taps_ref.shape[0]
    padded[:tail, :] = before_ref[...].astype(F32)
    padded[tail:, :] = gated_ref[...].astype(F32)
    total = None
    for tap in range(taps):
        first = tail - (taps - 1) + tap
        part = taps_ref[tap : tap + 1, :] * padded[first : first + rows, :]
        total = part if total is None else total + part
    act_ref[:, :aw] = att_ref[...]
    act_ref[:, aw:] = total.astype(BF16)


def conv(gated, before, taps, attended):
    rows, cw = gated.shape
    return pl.pallas_call(
        conv_kernel,
        out_shape=shape((rows, attended.shape[1] + cw)),
        in_specs=[VM] * 4,
        out_specs=VM,
        scratch_shapes=[pltpu.VMEM((rows + before.shape[0], cw), F32)],
        cost_estimate=cost(20_000_000, 500_000),
        compiler_params=params(),
        name="conv",
    )(gated, before, taps, attended)


def attention_kernel(q_ref, mine_ref, pair_ref, gain_ref, after, out_ref, mass_ref, kv, acc, mass, carry):
    me = lax.axis_index("sp")
    rows, width = q_ref.shape
    heads, hd = gain_ref.shape
    lane = lax.broadcasted_iota(jnp.int32, (rows, width), 1) // hd
    keys = rows
    for slot, (ref, n) in enumerate(((mine_ref, 0), (pair_ref, 0), (mine_ref, 1), (pair_ref, 1))):
        kv[slot, :keys, :] = ref[n * keys : (n + 1) * keys, :]
        kv[slot, keys : 2 * keys, :] = ref[(2 + n) * keys : (3 + n) * keys, :]
        off = ref[4 * keys + 8 * n : 4 * keys + 8 * n + 8, :]
        kv[slot, 2 * keys :, :] = jnp.concatenate([off, off])
    before = lax.broadcasted_iota(jnp.int32, (2 * keys, 2 * keys), 0) % keys
    column = lax.broadcasted_iota(jnp.int32, (2 * keys, 2 * keys), 1)
    suffix = jnp.where((column >= keys) | (before > column), 1.0, 0.0).astype(BF16)
    q = q_ref[...]
    scale = hd ** (-0.5)

    def block(slot, first):
        k = kv[slot, :keys, :]
        v = kv[slot, keys : 2 * keys, :]
        off = kv[slot, 2 * keys :, :].astype(F32)
        parts = []
        for h in range(heads):
            qh = jnp.where(lane == h, q, jnp.zeros_like(q))
            s = dot_f32(qh, k, ((1,), (1,))) * scale + off[h : h + 1, :]
            soft = jnp.maximum(s, 0.0) + jnp.log(1.0 + jnp.exp(-jnp.abs(s)))
            if first:
                allowed = lax.broadcasted_iota(jnp.int32, (rows, keys), 1) <= lax.broadcasted_iota(
                    jnp.int32, (rows, keys), 0
                )
                log_not = jnp.where(allowed, -soft, 0.0)
            else:
                log_not = -soft
            high = log_not.astype(BF16)
            low = (log_not - high.astype(F32)).astype(BF16)
            sums = dot_f32(jnp.concatenate([high, low], axis=1), suffix)
            later, total = sums[:, :keys], sums[:, keys:]
            if not first:
                later = later + carry[h]
            w = jnp.exp(s - soft + later)
            if first:
                w = jnp.where(allowed, w, 0.0)
                mass[h] = w
                carry[h] = total
            else:
                mass[h] = mass[h] + w
                carry[h] = carry[h] + total
            parts.append((w.astype(BF16), jnp.where(lane == h, v, jnp.zeros_like(v))))
        mix = dot_f32(
            jnp.concatenate([w for w, _ in parts], axis=1),
            jnp.concatenate([v for _, v in parts], axis=0),
        )
        if first:
            acc[...] = mix
        else:
            acc[...] = acc[...] + mix

    block(0, True)

    def earlier(t, _):
        block(jnp.bitwise_xor(me - t, me), False)
        return 0

    lax.fori_loop(1, me + 1, earlier, 0)
    mixed = acc[...]
    squares = mixed * mixed
    inverse = jnp.zeros_like(mixed)
    for h in range(heads):
        mean = jnp.sum(jnp.where(lane == h, squares, 0.0), axis=1, keepdims=True) / hd
        inverse = jnp.where(lane == h, lax.rsqrt(mean + norm_eps), inverse)
    gain = jnp.concatenate([gain_ref[h : h + 1, :] for h in range(heads)], axis=1)
    out_ref[...] = (mixed * inverse * gain).astype(BF16)
    for h in range(heads):
        mass_ref[h : h + 1, :] = jnp.log(jnp.sum(jnp.transpose(mass[h]), axis=0, keepdims=True))


def attention(q, mine, pair, head_gain, after):
    rows, width = q.shape
    heads, _ = head_gain.shape
    return pl.pallas_call(
        attention_kernel,
        out_shape=(shape((rows, width)), shape((heads, rows), F32)),
        in_specs=[VM] * 4 + [ANY],
        out_specs=[VM] * 2,
        scratch_shapes=[
            pltpu.VMEM((4, 2 * rows + 16, width), BF16),
            pltpu.VMEM((rows, width), F32),
            pltpu.VMEM((heads, rows, rows), F32),
            pltpu.VMEM((heads, rows, rows), F32),
        ],
        cost_estimate=cost(400_000_000, 1_000_000),
        compiler_params=params(),
        name="stick_attention",
    )(q, mine, pair, head_gain, after)


def final_kernel(*refs):
    act, wa, wc = (refs[n * 4 : (n + 1) * 4] for n in range(3))
    gain_ref, out_ref = refs[12:]
    cw = wc[0].shape[0]
    aw = act[0].shape[1] - cw
    convs = [c[:, aw:].astype(F32) for c in act]
    mean = sum(jnp.sum(v, axis=1, keepdims=True) for v in convs) / (4 * cw)
    centered = [v - mean for v in convs]
    spread = sum(jnp.sum(v * v, axis=1, keepdims=True) for v in centered) / (4 * cw)
    inverse = lax.rsqrt(spread + norm_eps)
    total = None
    for slot in range(4):
        pieces = [wa[slot][aw : aw + 1, n * cw : (n + 1) * cw].astype(F32) for n in range(6)]
        gain = pieces[0] + pieces[1] + pieces[2]
        bias = pieces[3] + pieces[4] + pieces[5]
        y = centered[slot] * inverse * gain + bias
        y = (y * jax.nn.sigmoid(y)).astype(BF16)
        part = dot_f32(act[slot][:, :aw], wa[slot][:aw, :]) + dot_f32(y, wc[slot][...])
        total = part if total is None else total + part
    squares = jnp.mean(total * total, axis=1, keepdims=True)
    out_ref[...] = (total * lax.rsqrt(squares + norm_eps) * gain_ref[...]).astype(BF16)


def finish(act, wa, wc, out_gain):
    rows, width = act[0].shape[0], wa[0].shape[1]
    return pl.pallas_call(
        final_kernel,
        out_shape=shape((rows, width)),
        in_specs=[VM] * 13,
        out_specs=VM,
        cost_estimate=cost(800_000_000, 7_000_000),
        compiler_params=params(32),
        name="finish_rows",
    )(*act, *wa, *wc, out_gain.reshape(1, width))


def paired(
    tokens,
    norm_gain,
    w_query,
    w_key,
    w_value,
    w_glu_value,
    w_glu_gate,
    key_offset,
    head_gain,
    conv_taps,
    channel_gain,
    channel_bias,
    w_out_attn,
    w_out_conv,
    out_gain,
):
    wc_x = exchange(w_out_conv, "tp", 2)
    own_qkv = (w_query, w_key, w_value)
    x_send, mine_own, mine_pair, w_qkv = norm_parts(tokens, norm_gain, own_qkv)
    x_got = exchange(x_send, "sp", 2)
    qkv_same = exchange(w_qkv, "sp", 1)
    w_glu, wa_mine = pack(w_glu_value, w_glu_gate, w_out_attn, channel_gain, channel_bias)
    glu_same = exchange(w_glu, "sp", 1)
    wa_x = exchange(wa_mine, "tp", 2)
    x_other = exchange(x_got, "tp", 1)
    qkv_other = exchange(qkv_same, "grp", 1)
    wc_core = exchange(w_out_conv, "tp", 1)
    wa_core = exchange(wa_mine, "tp", 1)
    glu_other = exchange(glu_same, "grp", 1)
    wc_xc = exchange(wc_x, "tp", 1)
    wa_xc = exchange(wa_x, "tp", 1)
    x_own, x_pair = assemble(mine_own, mine_pair, x_got, x_other)

    keep, sent = project_qkv(x_own, x_pair, own_qkv, qkv_same, qkv_other, key_offset.T)
    got = exchange(sent, "sp", 2)
    own_glu = (w_glu_value, w_glu_gate)
    glu_keep, glu_sent = project_glu(x_own, x_pair, own_glu, glu_same, glu_other, sent)
    glu_got = exchange(glu_sent, "sp", 2)
    q, mine_two = sum_qkv(keep, got, sent, glu_sent)
    pair_two = exchange(mine_two, "sp", 1)
    gated, tail = gate(glu_keep, glu_got, -(-conv_taps.shape[0] // 16) * 16)
    before = from_behind(tail, "sp", 1)
    attended, log_mass = attention(q, mine_two, pair_two, head_gain, tail)
    act_mine = conv(gated, before, conv_taps, attended)
    act = [act_mine] + [exchange(act_mine, "tp", bit) for bit in (1, 2, 3)]
    wa = (wa_mine, wa_core, wa_x, wa_xc)
    wc = (w_out_conv, wc_core, wc_x, wc_xc)
    mixed = finish(act, wa, wc, out_gain)
    return (mixed, log_mass)


def gathered(
    tokens,
    norm_gain,
    w_query,
    w_key,
    w_value,
    w_glu_value,
    w_glu_gate,
    key_offset,
    head_gain,
    conv_taps,
    channel_gain,
    channel_bias,
    w_out_attn,
    w_out_conv,
    out_gain,
):
    row_count = tokens.shape[0]
    hd = head_gain.shape[1]
    channels = conv_taps.shape[1] * lax.axis_size("tp")
    normed = row_norm(tokens.astype(jnp.float32), norm_gain).astype(jnp.bfloat16)
    weights_in = (w_query, w_key, w_value, w_glu_value, w_glu_gate)
    pieces = (
        lax.all_gather(weights_in[0], "sp", axis=0, tiled=True),
        lax.all_gather(weights_in[1], "sp", axis=0, tiled=True),
        lax.all_gather(weights_in[2], "sp", axis=0, tiled=True),
        lax.all_gather(weights_in[3], "sp", axis=0, tiled=True),
        lax.all_gather(weights_in[4], "sp", axis=0, tiled=True),
    )
    projected = tuple(
        (jnp.dot(normed, shard_piece, preferred_element_type=jnp.float32) for shard_piece in pieces)
    )
    query, key_rows, value_rows, glu_value, glu_gate = [
        summed.astype(jnp.bfloat16) for summed in projected
    ]
    kv_local = key_rows.shape[1] // hd
    group_size = query.shape[1] // key_rows.shape[1]
    heads_local = kv_local * group_size
    all_keys, all_values, all_offsets = (
        lax.all_gather(key_rows, "sp", axis=0, tiled=True),
        lax.all_gather(value_rows, "sp", axis=0, tiled=True),
        lax.all_gather(key_offset, "sp", axis=0, tiled=True),
    )
    sequence_length_total = all_keys.shape[0]
    shard_count = lax.axis_size("sp")
    per_block = 1
    while (
        per_block * 2 <= shard_count
        and shard_count % (per_block * 2) == 0
        and (per_block * 2 * row_count <= 1024)
    ):
        per_block = per_block * 2
    span_len = per_block * row_count
    query_heads = query.reshape(row_count, kv_local, group_size, hd)
    key_heads = all_keys.reshape(sequence_length_total, kv_local, hd)
    value_heads = all_values.reshape(sequence_length_total, kv_local, hd)
    my_index = lax.axis_index("sp")
    query_pos = my_index * row_count + jnp.arange(row_count, dtype=jnp.int32)
    last_block = my_index // per_block
    zeros_mix = jnp.zeros((kv_local, group_size, row_count, hd), jnp.float32)
    zeros_row = jnp.zeros((kv_local, group_size, row_count), jnp.float32)

    def sweep(turn_index, carry):
        head_mix, mass_sum, carried = carry
        first_key = (last_block - turn_index) * span_len
        key_block = lax.dynamic_slice_in_dim(key_heads, first_key, span_len, 0)
        value_block = lax.dynamic_slice_in_dim(value_heads, first_key, span_len, 0)
        offset_block = lax.dynamic_slice_in_dim(all_offsets, first_key, span_len, 0).astype(
            jnp.float32
        )
        offset_block = offset_block.T.reshape(kv_local, group_size, 1, span_len)
        scores = (
            jnp.einsum("qhgd,khd->hgqk", query_heads, key_block, preferred_element_type=jnp.float32)
            * hd ** (-0.5)
            + offset_block
        )
        key_pos = first_key + jnp.arange(span_len, dtype=jnp.int32)
        allowed = key_pos[None, :] <= query_pos[:, None]
        log_not = jnp.where(allowed, jax.nn.log_sigmoid(-scores), 0.0)
        later = lax.cumsum(log_not, axis=3, reverse=True) - log_not + carried[..., None]
        weights = jnp.where(allowed, jnp.exp(jax.nn.log_sigmoid(scores) + later), 0.0)
        head_mix = head_mix + jnp.einsum(
            "hgqk,khd->hgqd",
            weights.astype(jnp.bfloat16),
            value_block,
            preferred_element_type=jnp.float32,
        )
        return (head_mix, mass_sum + jnp.sum(weights, axis=3), carried + jnp.sum(log_not, axis=3))

    head_mix, mass_sum, _ = lax.fori_loop(
        0, last_block + 1, sweep, (zeros_mix, zeros_row, zeros_row)
    )
    log_mass = jnp.log(mass_sum).reshape(heads_local, row_count)
    head_rows = head_mix.transpose(2, 0, 1, 3).reshape(row_count, heads_local, hd)
    attended = (
        row_norm(head_rows, head_gain).astype(jnp.bfloat16).reshape(row_count, heads_local * hd)
    )
    gated = (glu_value.astype(jnp.float32) * jax.nn.sigmoid(glu_gate.astype(jnp.float32))).astype(
        jnp.bfloat16
    )
    reach_len = conv_taps.shape[0] - 1
    before = from_behind(gated[row_count - reach_len :], "sp", 1)
    padded = jnp.concatenate([before, gated], axis=0).astype(jnp.float32)
    conv_out = jnp.zeros(gated.shape, jnp.float32)
    for tap_index in range(conv_taps.shape[0]):
        conv_out = conv_out + conv_taps[tap_index] * padded[tap_index : tap_index + row_count]
    total_sum, total_squares = lax.psum(
        (jnp.sum(conv_out, axis=1), jnp.sum(conv_out * conv_out, axis=1)), "tp"
    )
    chan_mean = (total_sum / channels)[:, None]
    spread = (total_squares / channels)[:, None] - chan_mean * chan_mean
    centered = conv_out - chan_mean
    channel_out = jax.nn.silu(
        centered * lax.rsqrt(spread + norm_eps) * channel_gain + channel_bias
    ).astype(jnp.bfloat16)
    share = lax.psum_scatter(
        jnp.dot(attended, w_out_attn, preferred_element_type=jnp.float32)
        + jnp.dot(channel_out, w_out_conv, preferred_element_type=jnp.float32),
        "tp",
        scatter_dimension=0,
        tiled=True,
    )
    mixed = lax.all_gather(row_norm(share, out_gain).astype(jnp.bfloat16), "tp", axis=0, tiled=True)
    return (mixed, log_mass)


def solution(mesh):
    in_specs = (
        P(("grp", "sp"), None),
        P(),
        P("sp", "tp"),
        P("sp", "tp"),
        P("sp", "tp"),
        P("sp", "tp"),
        P("sp", "tp"),
        P(("grp", "sp"), "tp"),
        P("tp", None),
        P(None, "tp"),
        P("tp"),
        P("tp"),
        P("tp", None),
        P("tp", None),
        P(),
    )
    out_specs = (P(("grp", "sp"), None), P("tp", ("grp", "sp")))
    small = mesh.shape["sp"] == 4 and mesh.shape["tp"] == 4 and mesh.shape["grp"] == 2
    local = paired if small else gathered
    return jax.shard_map(local, mesh=mesh, in_specs=in_specs, out_specs=out_specs, check_vma=False)
```

```python
import jax
import jax.numpy as jnp
from jax import lax
from jax.experimental import pallas as pl
from jax.experimental.pallas import tpu as pltpu
from jax.sharding import PartitionSpec as P

norm_eps = 1e-06
BF16 = jnp.bfloat16
F32 = jnp.float32


def exchange(value, axis, bit):
    count = lax.axis_size(axis)
    return lax.ppermute(value, axis, [(s, s ^ bit) for s in range(count)])


def from_behind(value, axis, steps):
    count = lax.axis_size(axis)
    initial, last = (max(0, -steps), min(count, count - steps))
    return lax.ppermute(value, axis, [(source, source + steps) for source in range(initial, last)])


def row_norm(values_in, gain_vec):
    squares = jnp.mean(values_in * values_in, axis=-1, keepdims=True)
    return values_in * lax.rsqrt(squares + norm_eps) * gain_vec


def dot_f32(a, b, dims=((1,), (0,))):
    return lax.dot_general(a, b, (dims, ((), ())), preferred_element_type=F32)


def params(limit=16):
    return pltpu.CompilerParams(vmem_limit_bytes=limit * 1024 * 1024)


VM = pl.BlockSpec(memory_space=pltpu.VMEM)
ANY = pl.BlockSpec(memory_space=pl.ANY)
HBM = pl.BlockSpec(memory_space=pltpu.HBM)


def shape(dims, dtype=BF16):
    return jax.ShapeDtypeStruct(dims, dtype)


def cost(flops, moved):
    return pl.CostEstimate(flops=flops, bytes_accessed=moved, transcendentals=0)


def in_hbm(*values):
    return [pltpu.with_memory_space_constraint(v, pltpu.HBM) for v in values]


def pack_qkv_kernel(wq, wk, wv, pack_ref, sems):
    part = pack_ref.shape[0]
    width = wq.shape[1]
    mine = pl.ds(pl.multiple_of(lax.axis_index("grp") * part, part), part)
    copies = []
    for n, w in enumerate((wq, wk, wv)):
        at = slice(n * width, (n + 1) * width)
        copies.append(pltpu.make_async_copy(w.at[mine, :], pack_ref.at[:, at], sems.at[n]))
    for copy in copies:
        copy.start()
    for copy in copies:
        copy.wait()


def pack_qkv(weights):
    block, width = weights[0].shape
    return pl.pallas_call(
        pack_qkv_kernel,
        out_shape=shape((block // 2, 3 * width)),
        in_specs=[HBM] * 3,
        out_specs=VM,
        scratch_shapes=[pltpu.SemaphoreType.DMA((3,))],
        cost_estimate=cost(2_000_000, 400_000),
        compiler_params=params(),
        name="pack_qkv",
    )(*in_hbm(*weights))


def norm_kernel(x_hbm, gain_hbm, send_ref, own_ref, pair_ref, x_ref, gain_ref, normed, sems):
    side, low = lax.axis_index("sp") // 2, lax.axis_index("sp") % 2
    core = lax.axis_index("tp") % 2
    block = own_ref.shape[1]
    half = 2 * block
    half_rows = send_ref.shape[0]
    copies = [
        pltpu.make_async_copy(x_hbm, x_ref, sems.at[0]),
        pltpu.make_async_copy(gain_hbm, gain_ref, sems.at[1]),
    ]
    for copy in copies:
        copy.start()
    for copy in copies:
        copy.wait()
    x = x_ref[...].astype(F32)
    squares = jnp.mean(x * x, axis=1, keepdims=True)
    normed[...] = (x * lax.rsqrt(squares + norm_eps) * gain_ref[...]).astype(BF16)
    first = pl.multiple_of(core * half_rows, half_rows)
    away = pl.multiple_of((1 - side) * half, half)
    send_ref[...] = normed[pl.ds(first, half_rows), pl.ds(away, half)]
    own_ref[...] = normed[:, pl.ds(pl.multiple_of(side * half + low * block, block), block)]
    pair_ref[...] = normed[:, pl.ds(pl.multiple_of(side * half + (1 - low) * block, block), block)]


def norm_parts(tokens, gain, block):
    rows, features = tokens.shape
    return pl.pallas_call(
        norm_kernel,
        out_shape=(shape((rows // 2, 2 * block)), shape((rows, block)), shape((rows, block))),
        in_specs=[HBM] * 2,
        out_specs=[VM] * 3,
        scratch_shapes=[
            pltpu.VMEM((rows, features), BF16),
            pltpu.VMEM((1, features), F32),
            pltpu.VMEM((rows, features), BF16),
            pltpu.SemaphoreType.DMA((2,)),
        ],
        cost_estimate=cost(2_000_000, 1_000_000),
        compiler_params=params(),
        name="norm_parts",
    )(*in_hbm(tokens, gain.reshape(1, features)))


def pack_kernel(gv_hbm, gg_hbm, wa_hbm, gain_hbm, bias_hbm, glu_ref, out_ref, gain_ref, bias_ref, sems):
    cw, aw = gv_hbm.shape[1], wa_hbm.shape[0]
    copies = [
        pltpu.make_async_copy(gv_hbm, glu_ref.at[:, :cw], sems.at[0]),
        pltpu.make_async_copy(gg_hbm, glu_ref.at[:, cw:], sems.at[1]),
        pltpu.make_async_copy(wa_hbm, out_ref.at[:aw, :], sems.at[2]),
    ]
    small = [
        pltpu.make_async_copy(gain_hbm, gain_ref, sems.at[3]),
        pltpu.make_async_copy(bias_hbm, bias_ref, sems.at[4]),
    ]
    for copy in small + copies:
        copy.start()
    for copy in small:
        copy.wait()
    extra = out_ref.shape[0] - aw
    for n, ref in enumerate((gain_ref, bias_ref)):
        rest = ref[...]
        for piece in range(3):
            part = rest.astype(BF16)
            rest = rest - part.astype(F32)
            first = (3 * n + piece) * cw
            out_ref[aw:, first : first + cw] = jnp.broadcast_to(part, (extra, cw))
    for copy in copies:
        copy.wait()


def pack(gv, gg, wa, gain, bias):
    block, cw = gv.shape
    aw, width = wa.shape
    return pl.pallas_call(
        pack_kernel,
        out_shape=(shape((block, 2 * cw)), shape((aw + 16, width))),
        in_specs=[HBM] * 5,
        out_specs=[VM] * 2,
        scratch_shapes=[
            pltpu.VMEM((1, cw), F32),
            pltpu.VMEM((1, cw), F32),
            pltpu.SemaphoreType.DMA((5,)),
        ],
        cost_estimate=cost(2_000_000, 2_000_000),
        compiler_params=params(),
        name="pack",
    )(*in_hbm(gv, gg, wa, gain.reshape(1, cw), bias.reshape(1, cw)))


def assemble_kernel(own_ref, pair_ref, got_ref, other_ref, own_out, pair_out):
    low = lax.axis_index("sp") % 2
    core = lax.axis_index("tp") % 2
    rows, block = own_ref.shape
    half = got_ref.shape[0]
    own_out[:rows, :] = own_ref[...]
    pair_out[:rows, :] = pair_ref[...]
    own_at = pl.multiple_of(low * block, block)
    pair_at = pl.multiple_of((1 - low) * block, block)
    for part, at in ((got_ref, core), (other_ref, 1 - core)):
        first = pl.multiple_of(rows + at * half, half)
        own_out[pl.ds(first, half), :] = part[:, pl.ds(own_at, block)]
        pair_out[pl.ds(first, half), :] = part[:, pl.ds(pair_at, block)]


def assemble(own, pair, got, other):
    rows, block = own.shape
    return pl.pallas_call(
        assemble_kernel,
        out_shape=(shape((2 * rows, block)),) * 2,
        in_specs=[VM] * 4,
        out_specs=[VM] * 2,
        cost_estimate=cost(2_000_000, 1_000_000),
        compiler_params=params(),
        name="assemble",
    )(own, pair, got, other)


def far_dot(x_pair, same, other):
    part = same.shape[0]
    group = lax.axis_index("grp")
    near = x_pair[:, pl.ds(pl.multiple_of(group * part, part), part)]
    rest = x_pair[:, pl.ds(pl.multiple_of((1 - group) * part, part), part)]
    return dot_f32(near, same[...]) + dot_f32(rest, other[...])


def qkv_kernel(x_own, x_pair, wq, wk, wv, same, other, off_ref, keep_ref, send_ref):
    rows = x_own.shape[0] // 2
    width = wk.shape[1]
    far = far_dot(x_pair, same, other)
    for n, w in enumerate((wq, wk, wv)):
        at = slice(n * width, (n + 1) * width)
        part = dot_f32(x_own[...], w[...]) + far[:, at]
        keep_ref[:, at] = part
        first = 4 * rows if n == 0 else 2 * (n - 1) * rows
        send_ref[first : first + rows, :] = part[rows:].astype(BF16)
        if n > 0:
            send_ref[first + rows : first + 2 * rows, :] = part[:rows].astype(BF16)
    send_ref[5 * rows :, :] = jnp.zeros((send_ref.shape[0] - 5 * rows, width), BF16)
    send_ref[5 * rows : 5 * rows + off_ref.shape[0], :] = off_ref[...]


def project_qkv(x_own, x_pair, own, same, other, off):
    rows, width = x_own.shape[0], own[0].shape[1]
    return pl.pallas_call(
        qkv_kernel,
        out_shape=(shape((rows, 3 * width), F32), shape((5 * rows // 2 + 16, width))),
        in_specs=[VM] * 8,
        out_specs=[VM] * 2,
        cost_estimate=cost(200_000_000, 1_000_000),
        compiler_params=params(),
        name="project_qkv",
    )(x_own, x_pair, *own, same, other, off)


def sum_kernel(keep_ref, got_ref, sent_ref, after, q_ref, out_ref):
    rows, width = q_ref.shape

    def got(n):
        return got_ref[n * rows : (n + 1) * rows, :].astype(F32)

    q_ref[...] = (keep_ref[:rows, :width] + got(4)).astype(BF16)
    for n in range(4):
        at = slice((1 + n // 2) * width, (2 + n // 2) * width)
        part = keep_ref[(n % 2) * rows : (n % 2 + 1) * rows, at]
        out_ref[n * rows : (n + 1) * rows, :] = (part + got(n)).astype(BF16)
    first = 5 * rows
    out_ref[4 * rows :, :] = jnp.concatenate([sent_ref[first : first + 8, :], got_ref[first : first + 8, :]])


def sum_qkv(keep, got, sent, after):
    rows, width = keep.shape[0] // 2, got.shape[1]
    return pl.pallas_call(
        sum_kernel,
        out_shape=(shape((rows, width)), shape((4 * rows + 16, width))),
        in_specs=[VM] * 3 + [ANY],
        out_specs=[VM] * 2,
        cost_estimate=cost(1_000_000, 1_000_000),
        compiler_params=params(),
        name="sum_qkv",
    )(keep, got, sent, after)


def glu_kernel(x_own, x_pair, gv, gg, w_pair, after, keep_ref, send_ref):
    rows = x_own.shape[0] // 2
    cw = gv.shape[1]
    far = dot_f32(x_pair[...], w_pair[...])
    for n, w in enumerate((gv, gg)):
        at = slice(n * cw, (n + 1) * cw)
        part = dot_f32(x_own[...], w[...]) + far[:, at]
        keep_ref[:, at] = part[:rows]
        send_ref[:, at] = part[rows:].astype(BF16)


def project_glu(x_own, x_pair, own, w_pair, after):
    rows, width = x_own.shape[0] // 2, w_pair.shape[1]
    return pl.pallas_call(
        glu_kernel,
        out_shape=(shape((rows, width), F32), shape((rows, width))),
        in_specs=[VM] * 5 + [ANY],
        out_specs=[VM] * 2,
        cost_estimate=cost(270_000_000, 1_500_000),
        compiler_params=params(),
        name="project_glu",
    )(x_own, x_pair, *own, w_pair, after)


def gate_kernel(keep_ref, got_ref, gated_ref, tail_ref):
    rows, cw = gated_ref.shape
    glu = keep_ref[...] + got_ref[...].astype(F32)
    value = glu[:, :cw].astype(BF16).astype(F32)
    gate = glu[:, cw:].astype(BF16).astype(F32)
    gated = (value * jax.nn.sigmoid(gate)).astype(BF16)
    gated_ref[...] = gated
    tail_ref[...] = gated[rows - tail_ref.shape[0] :]


def gate(keep, got, tail):
    rows, cw = keep.shape[0], keep.shape[1] // 2
    return pl.pallas_call(
        gate_kernel,
        out_shape=(shape((rows, cw)), shape((tail, cw))),
        in_specs=[VM] * 2,
        out_specs=[VM] * 2,
        cost_estimate=cost(2_000_000, 500_000),
        compiler_params=params(),
        name="gate",
    )(keep, got)


def conv_kernel(gated_ref, before_ref, taps_ref, att_ref, act_ref, padded):
    rows, aw = att_ref.shape
    tail = before_ref.shape[0]
    taps = taps_ref.shape[0]
    padded[:tail, :] = before_ref[...].astype(F32)
    padded[tail:, :] = gated_ref[...].astype(F32)
    total = None
    for tap in range(taps):
        first = tail - (taps - 1) + tap
        part = taps_ref[tap : tap + 1, :] * padded[first : first + rows, :]
        total = part if total is None else total + part
    act_ref[:, :aw] = att_ref[...]
    act_ref[:, aw:] = total.astype(BF16)


def conv(gated, before, taps, attended):
    rows, cw = gated.shape
    return pl.pallas_call(
        conv_kernel,
        out_shape=shape((rows, attended.shape[1] + cw)),
        in_specs=[VM] * 4,
        out_specs=VM,
        scratch_shapes=[pltpu.VMEM((rows + before.shape[0], cw), F32)],
        cost_estimate=cost(20_000_000, 500_000),
        compiler_params=params(),
        name="conv",
    )(gated, before, taps, attended)


def attention_kernel(q_ref, mine_ref, pair_ref, gain_ref, after, out_ref, mass_ref, kv, acc, mass, carry):
    me = lax.axis_index("sp")
    rows, width = q_ref.shape
    heads, hd = gain_ref.shape
    lane = lax.broadcasted_iota(jnp.int32, (rows, width), 1) // hd
    keys = rows
    for slot, (ref, n) in enumerate(((mine_ref, 0), (pair_ref, 0), (mine_ref, 1), (pair_ref, 1))):
        kv[slot, :keys, :] = ref[n * keys : (n + 1) * keys, :]
        kv[slot, keys : 2 * keys, :] = ref[(2 + n) * keys : (3 + n) * keys, :]
        off = ref[4 * keys + 8 * n : 4 * keys + 8 * n + 8, :]
        kv[slot, 2 * keys :, :] = jnp.concatenate([off, off])
    before = lax.broadcasted_iota(jnp.int32, (2 * keys, 2 * keys), 0) % keys
    column = lax.broadcasted_iota(jnp.int32, (2 * keys, 2 * keys), 1)
    suffix = jnp.where((column >= keys) | (before > column), 1.0, 0.0).astype(BF16)
    q = q_ref[...]
    scale = hd ** (-0.5)

    def block(slot, first):
        k = kv[slot, :keys, :]
        v = kv[slot, keys : 2 * keys, :]
        off = kv[slot, 2 * keys :, :].astype(F32)
        parts = []
        for h in range(heads):
            qh = jnp.where(lane == h, q, jnp.zeros_like(q))
            s = dot_f32(qh, k, ((1,), (1,))) * scale + off[h : h + 1, :]
            soft = jnp.maximum(s, 0.0) + jnp.log(1.0 + jnp.exp(-jnp.abs(s)))
            if first:
                allowed = lax.broadcasted_iota(jnp.int32, (rows, keys), 1) <= lax.broadcasted_iota(
                    jnp.int32, (rows, keys), 0
                )
                log_not = jnp.where(allowed, -soft, 0.0)
            else:
                log_not = -soft
            high = log_not.astype(BF16)
            low = (log_not - high.astype(F32)).astype(BF16)
            sums = dot_f32(jnp.concatenate([high, low], axis=1), suffix)
            later, total = sums[:, :keys], sums[:, keys:]
            if not first:
                later = later + carry[h]
            w = jnp.exp(s - soft + later)
            if first:
                w = jnp.where(allowed, w, 0.0)
                mass[h] = w
                carry[h] = total
            else:
                mass[h] = mass[h] + w
                carry[h] = carry[h] + total
            parts.append((w.astype(BF16), jnp.where(lane == h, v, jnp.zeros_like(v))))
        mix = dot_f32(
            jnp.concatenate([w for w, _ in parts], axis=1),
            jnp.concatenate([v for _, v in parts], axis=0),
        )
        if first:
            acc[...] = mix
        else:
            acc[...] = acc[...] + mix

    block(0, True)

    def earlier(t, _):
        block(jnp.bitwise_xor(me - t, me), False)
        return 0

    lax.fori_loop(1, me + 1, earlier, 0)
    mixed = acc[...]
    squares = mixed * mixed
    inverse = jnp.zeros_like(mixed)
    for h in range(heads):
        mean = jnp.sum(jnp.where(lane == h, squares, 0.0), axis=1, keepdims=True) / hd
        inverse = jnp.where(lane == h, lax.rsqrt(mean + norm_eps), inverse)
    gain = jnp.concatenate([gain_ref[h : h + 1, :] for h in range(heads)], axis=1)
    out_ref[...] = (mixed * inverse * gain).astype(BF16)
    for h in range(heads):
        mass_ref[h : h + 1, :] = jnp.log(jnp.sum(jnp.transpose(mass[h]), axis=0, keepdims=True))


def attention(q, mine, pair, head_gain, after):
    rows, width = q.shape
    heads, _ = head_gain.shape
    return pl.pallas_call(
        attention_kernel,
        out_shape=(shape((rows, width)), shape((heads, rows), F32)),
        in_specs=[VM] * 4 + [ANY],
        out_specs=[VM] * 2,
        scratch_shapes=[
            pltpu.VMEM((4, 2 * rows + 16, width), BF16),
            pltpu.VMEM((rows, width), F32),
            pltpu.VMEM((heads, rows, rows), F32),
            pltpu.VMEM((heads, rows, rows), F32),
        ],
        cost_estimate=cost(400_000_000, 1_000_000),
        compiler_params=params(),
        name="stick_attention",
    )(q, mine, pair, head_gain, after)


def final_kernel(*refs):
    act, wa, wc = (refs[n * 4 : (n + 1) * 4] for n in range(3))
    gain_ref, out_ref = refs[12:]
    cw = wc[0].shape[0]
    aw = act[0].shape[1] - cw
    convs = [c[:, aw:].astype(F32) for c in act]
    mean = sum(jnp.sum(v, axis=1, keepdims=True) for v in convs) / (4 * cw)
    centered = [v - mean for v in convs]
    spread = sum(jnp.sum(v * v, axis=1, keepdims=True) for v in centered) / (4 * cw)
    inverse = lax.rsqrt(spread + norm_eps)
    total = None
    for slot in range(4):
        pieces = [wa[slot][aw : aw + 1, n * cw : (n + 1) * cw].astype(F32) for n in range(6)]
        gain = pieces[0] + pieces[1] + pieces[2]
        bias = pieces[3] + pieces[4] + pieces[5]
        y = centered[slot] * inverse * gain + bias
        y = (y * jax.nn.sigmoid(y)).astype(BF16)
        part = dot_f32(act[slot][:, :aw], wa[slot][:aw, :]) + dot_f32(y, wc[slot][...])
        total = part if total is None else total + part
    squares = jnp.mean(total * total, axis=1, keepdims=True)
    out_ref[...] = (total * lax.rsqrt(squares + norm_eps) * gain_ref[...]).astype(BF16)


def finish(act, wa, wc, out_gain):
    rows, width = act[0].shape[0], wa[0].shape[1]
    return pl.pallas_call(
        final_kernel,
        out_shape=shape((rows, width)),
        in_specs=[VM] * 13,
        out_specs=VM,
        cost_estimate=cost(800_000_000, 7_000_000),
        compiler_params=params(32),
        name="finish_rows",
    )(*act, *wa, *wc, out_gain.reshape(1, width))


def paired(
    tokens,
    norm_gain,
    w_query,
    w_key,
    w_value,
    w_glu_value,
    w_glu_gate,
    key_offset,
    head_gain,
    conv_taps,
    channel_gain,
    channel_bias,
    w_out_attn,
    w_out_conv,
    out_gain,
):
    own_qkv = (w_query, w_key, w_value)
    qkv_same = exchange(pack_qkv(own_qkv), "sp", 1)
    wc_x = exchange(w_out_conv, "tp", 2)
    x_send, mine_own, mine_pair = norm_parts(tokens, norm_gain, w_query.shape[0])
    x_got = exchange(x_send, "sp", 2)
    w_glu, wa_mine = pack(w_glu_value, w_glu_gate, w_out_attn, channel_gain, channel_bias)
    glu_pair = exchange(w_glu, "sp", 1)
    qkv_other = exchange(qkv_same, "grp", 1)
    x_other = exchange(x_got, "tp", 1)
    wa_x = exchange(wa_mine, "tp", 2)
    wc_core = exchange(w_out_conv, "tp", 1)
    wa_core = exchange(wa_mine, "tp", 1)
    wc_xc = exchange(wc_x, "tp", 1)
    wa_xc = exchange(wa_x, "tp", 1)
    x_own, x_pair = assemble(mine_own, mine_pair, x_got, x_other)

    keep, sent = project_qkv(x_own, x_pair, own_qkv, qkv_same, qkv_other, key_offset.T)
    got = exchange(sent, "sp", 2)
    own_glu = (w_glu_value, w_glu_gate)
    glu_keep, glu_sent = project_glu(x_own, x_pair, own_glu, glu_pair, sent)
    glu_got = exchange(glu_sent, "sp", 2)
    q, mine_two = sum_qkv(keep, got, sent, glu_sent)
    pair_two = exchange(mine_two, "sp", 1)
    gated, tail = gate(glu_keep, glu_got, -(-conv_taps.shape[0] // 16) * 16)
    before = from_behind(tail, "sp", 1)
    attended, log_mass = attention(q, mine_two, pair_two, head_gain, tail)
    act_mine = conv(gated, before, conv_taps, attended)
    act = [act_mine] + [exchange(act_mine, "tp", bit) for bit in (1, 2, 3)]
    wa = (wa_mine, wa_core, wa_x, wa_xc)
    wc = (w_out_conv, wc_core, wc_x, wc_xc)
    mixed = finish(act, wa, wc, out_gain)
    return (mixed, log_mass)


def gathered(
    tokens,
    norm_gain,
    w_query,
    w_key,
    w_value,
    w_glu_value,
    w_glu_gate,
    key_offset,
    head_gain,
    conv_taps,
    channel_gain,
    channel_bias,
    w_out_attn,
    w_out_conv,
    out_gain,
):
    row_count = tokens.shape[0]
    hd = head_gain.shape[1]
    channels = conv_taps.shape[1] * lax.axis_size("tp")
    normed = row_norm(tokens.astype(jnp.float32), norm_gain).astype(jnp.bfloat16)
    weights_in = (w_query, w_key, w_value, w_glu_value, w_glu_gate)
    pieces = (
        lax.all_gather(weights_in[0], "sp", axis=0, tiled=True),
        lax.all_gather(weights_in[1], "sp", axis=0, tiled=True),
        lax.all_gather(weights_in[2], "sp", axis=0, tiled=True),
        lax.all_gather(weights_in[3], "sp", axis=0, tiled=True),
        lax.all_gather(weights_in[4], "sp", axis=0, tiled=True),
    )
    projected = tuple(
        (jnp.dot(normed, shard_piece, preferred_element_type=jnp.float32) for shard_piece in pieces)
    )
    query, key_rows, value_rows, glu_value, glu_gate = [
        summed.astype(jnp.bfloat16) for summed in projected
    ]
    kv_local = key_rows.shape[1] // hd
    group_size = query.shape[1] // key_rows.shape[1]
    heads_local = kv_local * group_size
    all_keys, all_values, all_offsets = (
        lax.all_gather(key_rows, "sp", axis=0, tiled=True),
        lax.all_gather(value_rows, "sp", axis=0, tiled=True),
        lax.all_gather(key_offset, "sp", axis=0, tiled=True),
    )
    sequence_length_total = all_keys.shape[0]
    shard_count = lax.axis_size("sp")
    per_block = 1
    while (
        per_block * 2 <= shard_count
        and shard_count % (per_block * 2) == 0
        and (per_block * 2 * row_count <= 1024)
    ):
        per_block = per_block * 2
    span_len = per_block * row_count
    query_heads = query.reshape(row_count, kv_local, group_size, hd)
    key_heads = all_keys.reshape(sequence_length_total, kv_local, hd)
    value_heads = all_values.reshape(sequence_length_total, kv_local, hd)
    my_index = lax.axis_index("sp")
    query_pos = my_index * row_count + jnp.arange(row_count, dtype=jnp.int32)
    last_block = my_index // per_block
    zeros_mix = jnp.zeros((kv_local, group_size, row_count, hd), jnp.float32)
    zeros_row = jnp.zeros((kv_local, group_size, row_count), jnp.float32)

    def sweep(turn_index, carry):
        head_mix, mass_sum, carried = carry
        first_key = (last_block - turn_index) * span_len
        key_block = lax.dynamic_slice_in_dim(key_heads, first_key, span_len, 0)
        value_block = lax.dynamic_slice_in_dim(value_heads, first_key, span_len, 0)
        offset_block = lax.dynamic_slice_in_dim(all_offsets, first_key, span_len, 0).astype(
            jnp.float32
        )
        offset_block = offset_block.T.reshape(kv_local, group_size, 1, span_len)
        scores = (
            jnp.einsum("qhgd,khd->hgqk", query_heads, key_block, preferred_element_type=jnp.float32)
            * hd ** (-0.5)
            + offset_block
        )
        key_pos = first_key + jnp.arange(span_len, dtype=jnp.int32)
        allowed = key_pos[None, :] <= query_pos[:, None]
        log_not = jnp.where(allowed, jax.nn.log_sigmoid(-scores), 0.0)
        later = lax.cumsum(log_not, axis=3, reverse=True) - log_not + carried[..., None]
        weights = jnp.where(allowed, jnp.exp(jax.nn.log_sigmoid(scores) + later), 0.0)
        head_mix = head_mix + jnp.einsum(
            "hgqk,khd->hgqd",
            weights.astype(jnp.bfloat16),
            value_block,
            preferred_element_type=jnp.float32,
        )
        return (head_mix, mass_sum + jnp.sum(weights, axis=3), carried + jnp.sum(log_not, axis=3))

    head_mix, mass_sum, _ = lax.fori_loop(
        0, last_block + 1, sweep, (zeros_mix, zeros_row, zeros_row)
    )
    log_mass = jnp.log(mass_sum).reshape(heads_local, row_count)
    head_rows = head_mix.transpose(2, 0, 1, 3).reshape(row_count, heads_local, hd)
    attended = (
        row_norm(head_rows, head_gain).astype(jnp.bfloat16).reshape(row_count, heads_local * hd)
    )
    gated = (glu_value.astype(jnp.float32) * jax.nn.sigmoid(glu_gate.astype(jnp.float32))).astype(
        jnp.bfloat16
    )
    reach_len = conv_taps.shape[0] - 1
    before = from_behind(gated[row_count - reach_len :], "sp", 1)
    padded = jnp.concatenate([before, gated], axis=0).astype(jnp.float32)
    conv_out = jnp.zeros(gated.shape, jnp.float32)
    for tap_index in range(conv_taps.shape[0]):
        conv_out = conv_out + conv_taps[tap_index] * padded[tap_index : tap_index + row_count]
    total_sum, total_squares = lax.psum(
        (jnp.sum(conv_out, axis=1), jnp.sum(conv_out * conv_out, axis=1)), "tp"
    )
    chan_mean = (total_sum / channels)[:, None]
    spread = (total_squares / channels)[:, None] - chan_mean * chan_mean
    centered = conv_out - chan_mean
    channel_out = jax.nn.silu(
        centered * lax.rsqrt(spread + norm_eps) * channel_gain + channel_bias
    ).astype(jnp.bfloat16)
    share = lax.psum_scatter(
        jnp.dot(attended, w_out_attn, preferred_element_type=jnp.float32)
        + jnp.dot(channel_out, w_out_conv, preferred_element_type=jnp.float32),
        "tp",
        scatter_dimension=0,
        tiled=True,
    )
    mixed = lax.all_gather(row_norm(share, out_gain).astype(jnp.bfloat16), "tp", axis=0, tiled=True)
    return (mixed, log_mass)


def solution(mesh):
    in_specs = (
        P(("grp", "sp"), None),
        P(),
        P("sp", "tp"),
        P("sp", "tp"),
        P("sp", "tp"),
        P("sp", "tp"),
        P("sp", "tp"),
        P(("grp", "sp"), "tp"),
        P("tp", None),
        P(None, "tp"),
        P("tp"),
        P("tp"),
        P("tp", None),
        P("tp", None),
        P(),
    )
    out_specs = (P(("grp", "sp"), None), P("tp", ("grp", "sp")))
    small = mesh.shape["sp"] == 4 and mesh.shape["tp"] == 4 and mesh.shape["grp"] == 2
    local = paired if small else gathered
    return jax.shard_map(local, mesh=mesh, in_specs=in_specs, out_specs=out_specs, check_vma=False)
```

```python
import jax
import jax.numpy as jnp
from jax import lax
from jax.experimental import pallas as pl
from jax.experimental.pallas import tpu as pltpu
from jax.sharding import PartitionSpec as P

norm_eps = 1e-06
BF16 = jnp.bfloat16
F32 = jnp.float32


def exchange(value, axis, bit):
    count = lax.axis_size(axis)
    return lax.ppermute(value, axis, [(s, s ^ bit) for s in range(count)])


def from_behind(value, axis, steps):
    count = lax.axis_size(axis)
    initial, last = (max(0, -steps), min(count, count - steps))
    return lax.ppermute(value, axis, [(source, source + steps) for source in range(initial, last)])


def row_norm(values_in, gain_vec):
    squares = jnp.mean(values_in * values_in, axis=-1, keepdims=True)
    return values_in * lax.rsqrt(squares + norm_eps) * gain_vec


def dot_f32(a, b, dims=((1,), (0,))):
    return lax.dot_general(a, b, (dims, ((), ())), preferred_element_type=F32)


def params(limit=16):
    return pltpu.CompilerParams(vmem_limit_bytes=limit * 1024 * 1024)


VM = pl.BlockSpec(memory_space=pltpu.VMEM)
ANY = pl.BlockSpec(memory_space=pl.ANY)
HBM = pl.BlockSpec(memory_space=pltpu.HBM)


def shape(dims, dtype=BF16):
    return jax.ShapeDtypeStruct(dims, dtype)


def cost(flops, moved):
    return pl.CostEstimate(flops=flops, bytes_accessed=moved, transcendentals=0)


def in_hbm(*values):
    return [pltpu.with_memory_space_constraint(v, pltpu.HBM) for v in values]


def pack_qkv_kernel(wq, wk, wv, all_ref, send_ref, sems):
    part = send_ref.shape[0]
    width = wq.shape[1]
    mine = pl.ds(pl.multiple_of(lax.axis_index("grp") * part, part), part)
    first, rest = [], []
    for n, w in enumerate((wq, wk, wv)):
        at = slice(n * width, (n + 1) * width)
        first.append(pltpu.make_async_copy(w.at[mine, :], send_ref.at[:, at], sems.at[n]))
        rest.append(pltpu.make_async_copy(w, all_ref.at[:, at], sems.at[3 + n]))
    for copy in first + rest:
        copy.start()
    for copy in first + rest:
        copy.wait()


def pack_qkv(weights):
    block, width = weights[0].shape
    return pl.pallas_call(
        pack_qkv_kernel,
        out_shape=(shape((block, 3 * width)), shape((block // 2, 3 * width))),
        in_specs=[HBM] * 3,
        out_specs=[VM] * 2,
        scratch_shapes=[pltpu.SemaphoreType.DMA((6,))],
        cost_estimate=cost(2_000_000, 400_000),
        compiler_params=params(),
        name="pack_qkv",
    )(*in_hbm(*weights))


def norm_kernel(x_hbm, gain_hbm, send_ref, own_ref, pair_ref, x_ref, gain_ref, normed, sems):
    side, low = lax.axis_index("sp") // 2, lax.axis_index("sp") % 2
    core = lax.axis_index("tp") % 2
    block = own_ref.shape[1]
    half = 2 * block
    half_rows = send_ref.shape[0]
    copies = [
        pltpu.make_async_copy(x_hbm, x_ref, sems.at[0]),
        pltpu.make_async_copy(gain_hbm, gain_ref, sems.at[1]),
    ]
    for copy in copies:
        copy.start()
    for copy in copies:
        copy.wait()
    x = x_ref[...].astype(F32)
    squares = jnp.mean(x * x, axis=1, keepdims=True)
    normed[...] = (x * lax.rsqrt(squares + norm_eps) * gain_ref[...]).astype(BF16)
    first = pl.multiple_of(core * half_rows, half_rows)
    away = pl.multiple_of((1 - side) * half, half)
    send_ref[...] = normed[pl.ds(first, half_rows), pl.ds(away, half)]
    own_ref[...] = normed[:, pl.ds(pl.multiple_of(side * half + low * block, block), block)]
    pair_ref[...] = normed[:, pl.ds(pl.multiple_of(side * half + (1 - low) * block, block), block)]


def norm_parts(tokens, gain, block):
    rows, features = tokens.shape
    return pl.pallas_call(
        norm_kernel,
        out_shape=(shape((rows // 2, 2 * block)), shape((rows, block)), shape((rows, block))),
        in_specs=[HBM] * 2,
        out_specs=[VM] * 3,
        scratch_shapes=[
            pltpu.VMEM((rows, features), BF16),
            pltpu.VMEM((1, features), F32),
            pltpu.VMEM((rows, features), BF16),
            pltpu.SemaphoreType.DMA((2,)),
        ],
        cost_estimate=cost(2_000_000, 1_000_000),
        compiler_params=params(),
        name="norm_parts",
    )(*in_hbm(tokens, gain.reshape(1, features)))


def pack_kernel(gv_hbm, gg_hbm, wa_hbm, off_hbm, gain_hbm, bias_hbm, glu_ref, out_ref, off_ref, gain_ref, bias_ref, sems):
    cw, aw = gv_hbm.shape[1], wa_hbm.shape[0]
    copies = [
        pltpu.make_async_copy(gv_hbm, glu_ref.at[:, :cw], sems.at[0]),
        pltpu.make_async_copy(gg_hbm, glu_ref.at[:, cw:], sems.at[1]),
        pltpu.make_async_copy(wa_hbm, out_ref.at[:aw, :], sems.at[2]),
        pltpu.make_async_copy(off_hbm, off_ref, sems.at[5]),
    ]
    small = [
        pltpu.make_async_copy(gain_hbm, gain_ref, sems.at[3]),
        pltpu.make_async_copy(bias_hbm, bias_ref, sems.at[4]),
    ]
    for copy in small + copies:
        copy.start()
    for copy in small:
        copy.wait()
    extra = out_ref.shape[0] - aw
    for n, ref in enumerate((gain_ref, bias_ref)):
        rest = ref[...]
        for piece in range(3):
            part = rest.astype(BF16)
            rest = rest - part.astype(F32)
            first = (3 * n + piece) * cw
            out_ref[aw:, first : first + cw] = jnp.broadcast_to(part, (extra, cw))
    for copy in copies:
        copy.wait()


def pack(gv, gg, wa, off, gain, bias):
    block, cw = gv.shape
    aw, width = wa.shape
    return pl.pallas_call(
        pack_kernel,
        out_shape=(shape((block, 2 * cw)), shape((aw + 16, width)), shape(off.shape)),
        in_specs=[HBM] * 6,
        out_specs=[VM] * 3,
        scratch_shapes=[
            pltpu.VMEM((1, cw), F32),
            pltpu.VMEM((1, cw), F32),
            pltpu.SemaphoreType.DMA((6,)),
        ],
        cost_estimate=cost(2_000_000, 2_000_000),
        compiler_params=params(),
        name="pack",
    )(*in_hbm(gv, gg, wa, off, gain.reshape(1, cw), bias.reshape(1, cw)))


def assemble_kernel(own_ref, pair_ref, got_ref, other_ref, own_out, pair_out):
    low = lax.axis_index("sp") % 2
    core = lax.axis_index("tp") % 2
    rows, block = own_ref.shape
    half = got_ref.shape[0]
    own_out[:rows, :] = own_ref[...]
    pair_out[:rows, :] = pair_ref[...]
    own_at = pl.multiple_of(low * block, block)
    pair_at = pl.multiple_of((1 - low) * block, block)
    for part, at in ((got_ref, core), (other_ref, 1 - core)):
        first = pl.multiple_of(rows + at * half, half)
        own_out[pl.ds(first, half), :] = part[:, pl.ds(own_at, block)]
        pair_out[pl.ds(first, half), :] = part[:, pl.ds(pair_at, block)]


def assemble(own, pair, got, other):
    rows, block = own.shape
    return pl.pallas_call(
        assemble_kernel,
        out_shape=(shape((2 * rows, block)),) * 2,
        in_specs=[VM] * 4,
        out_specs=[VM] * 2,
        cost_estimate=cost(2_000_000, 1_000_000),
        compiler_params=params(),
        name="assemble",
    )(own, pair, got, other)


def far_dot(x_pair, same, other):
    part = same.shape[0]
    group = lax.axis_index("grp")
    near = x_pair[:, pl.ds(pl.multiple_of(group * part, part), part)]
    rest = x_pair[:, pl.ds(pl.multiple_of((1 - group) * part, part), part)]
    return dot_f32(near, same[...]) + dot_f32(rest, other[...])


def qkv_kernel(x_own, x_pair, own, same, other, off_ref, keep_ref, send_ref):
    rows = x_own.shape[0] // 2
    width = send_ref.shape[1]
    total = dot_f32(x_own[...], own[...]) + far_dot(x_pair, same, other)
    keep_ref[...] = total
    for n in range(3):
        part = total[:, n * width : (n + 1) * width].astype(BF16)
        first = 4 * rows if n == 0 else 2 * (n - 1) * rows
        send_ref[first : first + rows, :] = part[rows:]
        if n > 0:
            send_ref[first + rows : first + 2 * rows, :] = part[:rows]
    send_ref[5 * rows :, :] = jnp.zeros((send_ref.shape[0] - 5 * rows, width), BF16)
    send_ref[5 * rows : 5 * rows + off_ref.shape[0], :] = off_ref[...]


def project_qkv(x_own, x_pair, own, same, other, off):
    rows, width = x_own.shape[0], own.shape[1] // 3
    return pl.pallas_call(
        qkv_kernel,
        out_shape=(shape((rows, 3 * width), F32), shape((5 * rows // 2 + 16, width))),
        in_specs=[VM] * 6,
        out_specs=[VM] * 2,
        cost_estimate=cost(200_000_000, 1_000_000),
        compiler_params=params(),
        name="project_qkv",
    )(x_own, x_pair, own, same, other, off)


def sum_kernel(keep_ref, got_ref, sent_ref, after, q_ref, out_ref):
    rows, width = q_ref.shape

    def got(n):
        return got_ref[n * rows : (n + 1) * rows, :].astype(F32)

    q_ref[...] = (keep_ref[:rows, :width] + got(4)).astype(BF16)
    for n in range(4):
        at = slice((1 + n // 2) * width, (2 + n // 2) * width)
        part = keep_ref[(n % 2) * rows : (n % 2 + 1) * rows, at]
        out_ref[n * rows : (n + 1) * rows, :] = (part + got(n)).astype(BF16)
    first = 5 * rows
    out_ref[4 * rows :, :] = jnp.concatenate([sent_ref[first : first + 8, :], got_ref[first : first + 8, :]])


def sum_qkv(keep, got, sent, after):
    rows, width = keep.shape[0] // 2, got.shape[1]
    return pl.pallas_call(
        sum_kernel,
        out_shape=(shape((rows, width)), shape((4 * rows + 16, width))),
        in_specs=[VM] * 3 + [ANY],
        out_specs=[VM] * 2,
        cost_estimate=cost(1_000_000, 1_000_000),
        compiler_params=params(),
        name="sum_qkv",
    )(keep, got, sent, after)


def glu_kernel(x_own, x_pair, own, pair, after, keep_ref, send_ref):
    rows = x_own.shape[0] // 2
    total = dot_f32(x_own[...], own[...]) + dot_f32(x_pair[...], pair[...])
    keep_ref[...] = total[:rows]
    send_ref[...] = total[rows:].astype(BF16)


def project_glu(x_own, x_pair, own, pair, after):
    rows, width = x_own.shape[0] // 2, pair.shape[1]
    return pl.pallas_call(
        glu_kernel,
        out_shape=(shape((rows, width), F32), shape((rows, width))),
        in_specs=[VM] * 4 + [ANY],
        out_specs=[VM] * 2,
        cost_estimate=cost(270_000_000, 1_500_000),
        compiler_params=params(),
        name="project_glu",
    )(x_own, x_pair, own, pair, after)


def gate_kernel(keep_ref, got_ref, gated_ref, tail_ref):
    rows, cw = gated_ref.shape
    glu = keep_ref[...] + got_ref[...].astype(F32)
    value = glu[:, :cw].astype(BF16).astype(F32)
    gate = glu[:, cw:].astype(BF16).astype(F32)
    gated = (value * jax.nn.sigmoid(gate)).astype(BF16)
    gated_ref[...] = gated
    tail_ref[...] = gated[rows - tail_ref.shape[0] :]


def gate(keep, got, tail):
    rows, cw = keep.shape[0], keep.shape[1] // 2
    return pl.pallas_call(
        gate_kernel,
        out_shape=(shape((rows, cw)), shape((tail, cw))),
        in_specs=[VM] * 2,
        out_specs=[VM] * 2,
        cost_estimate=cost(2_000_000, 500_000),
        compiler_params=params(),
        name="gate",
    )(keep, got)


def conv_kernel(gated_ref, before_ref, taps_ref, att_ref, act_ref, padded):
    rows, aw = att_ref.shape
    tail = before_ref.shape[0]
    taps = taps_ref.shape[0]
    padded[:tail, :] = before_ref[...].astype(F32)
    padded[tail:, :] = gated_ref[...].astype(F32)
    total = None
    for tap in range(taps):
        first = tail - (taps - 1) + tap
        part = taps_ref[tap : tap + 1, :] * padded[first : first + rows, :]
        total = part if total is None else total + part
    act_ref[:, :aw] = att_ref[...]
    act_ref[:, aw:] = total.astype(BF16)


def conv(gated, before, taps, attended):
    rows, cw = gated.shape
    return pl.pallas_call(
        conv_kernel,
        out_shape=shape((rows, attended.shape[1] + cw)),
        in_specs=[VM] * 4,
        out_specs=VM,
        scratch_shapes=[pltpu.VMEM((rows + before.shape[0], cw), F32)],
        cost_estimate=cost(20_000_000, 500_000),
        compiler_params=params(),
        name="conv",
    )(gated, before, taps, attended)


def suffix_matrix(keys):
    before = lax.broadcasted_iota(jnp.int32, (2 * keys, 2 * keys), 0) % keys
    column = lax.broadcasted_iota(jnp.int32, (2 * keys, 2 * keys), 1)
    return jnp.where((column >= keys) | (before > column), 1.0, 0.0).astype(BF16)


def stick_block(q, k, v, off, hd, suffix, carry, diagonal):
    rows, width = q.shape
    keys = k.shape[0]
    lane = lax.broadcasted_iota(jnp.int32, (rows, width), 1) // hd
    offsets = off.astype(F32)
    weights, totals, values = [], [], []
    for h in range(width // hd):
        qh = jnp.where(lane == h, q, jnp.zeros_like(q))
        s = dot_f32(qh, k, ((1,), (1,))) * hd ** (-0.5) + offsets[h : h + 1, :]
        soft = jnp.maximum(s, 0.0) + jnp.log(1.0 + jnp.exp(-jnp.abs(s)))
        log_not = -soft
        if diagonal:
            allowed = lax.broadcasted_iota(jnp.int32, (rows, keys), 1) <= lax.broadcasted_iota(
                jnp.int32, (rows, keys), 0
            )
            log_not = jnp.where(allowed, log_not, 0.0)
        high = log_not.astype(BF16)
        low = (log_not - high.astype(F32)).astype(BF16)
        sums = dot_f32(jnp.concatenate([high, low], axis=1), suffix)
        later = sums[:, :keys]
        if carry is not None:
            later = later + carry[h]
        w = jnp.exp(s - soft + later)
        if diagonal:
            w = jnp.where(allowed, w, 0.0)
        weights.append(w)
        totals.append(sums[:, keys:])
        values.append(jnp.where(lane == h, v, jnp.zeros_like(v)))
    mix = dot_f32(
        jnp.concatenate([w.astype(BF16) for w in weights], axis=1), jnp.concatenate(values, axis=0)
    )
    return mix, weights, totals


def near_kernel(q_ref, mine_ref, gain_ref, after, mix_ref, mass_ref, carry_ref):
    rows = q_ref.shape[0]
    heads, hd = gain_ref.shape
    suffix = suffix_matrix(rows)
    for n in range(2):
        k = mine_ref[n * rows : (n + 1) * rows, :]
        v = mine_ref[(2 + n) * rows : (3 + n) * rows, :]
        off = mine_ref[4 * rows + 8 * n : 4 * rows + 8 * n + 8, :]
        mix, weights, totals = stick_block(q_ref[...], k, v, off, hd, suffix, None, n == 0)
        mix_ref[n] = mix
        for h in range(heads):
            mass_ref[n * heads + h] = weights[h]
            carry_ref[n * heads + h] = totals[h]


def near_attention(q, mine, head_gain, after):
    rows, width = q.shape
    heads = head_gain.shape[0]
    return pl.pallas_call(
        near_kernel,
        out_shape=(
            shape((2, rows, width), F32),
            shape((2 * heads, rows, rows), F32),
            shape((2 * heads, rows, rows), F32),
        ),
        in_specs=[VM] * 3 + [ANY],
        out_specs=[VM] * 3,
        cost_estimate=cost(200_000_000, 1_000_000),
        compiler_params=params(),
        name="near_attention",
    )(q, mine, head_gain, after)


def attention_kernel(q_ref, pair_ref, gain_ref, mix_ref, mass_ref, carry_ref, after, out_ref, log_ref, acc, mass, carry):
    me = lax.axis_index("sp")
    rows, width = q_ref.shape
    heads, hd = gain_ref.shape
    lane = lax.broadcasted_iota(jnp.int32, (rows, width), 1) // hd
    suffix = suffix_matrix(rows)
    acc[...] = mix_ref[0]
    for h in range(heads):
        mass[h] = mass_ref[h]
        carry[h] = carry_ref[h]

    def earlier(t, _):
        slot = jnp.bitwise_xor(me - t, me)

        @pl.when(slot == 2)
        def _():
            scale = jnp.zeros_like(acc)
            for h in range(heads):
                left = jnp.exp(carry[h])
                mass[h] = mass[h] + left * mass_ref[heads + h]
                scale = jnp.where(lane == h, left, scale)
                carry[h] = carry[h] + carry_ref[heads + h]
            acc[...] = acc[...] + scale * mix_ref[1]

        @pl.when(slot != 2)
        def _():
            n = slot // 2
            k = pair_ref[pl.ds(pl.multiple_of(n * rows, rows), rows), :]
            v = pair_ref[pl.ds(pl.multiple_of((2 + n) * rows, rows), rows), :]
            off = jnp.where(
                n == 0,
                pair_ref[4 * rows : 4 * rows + 8, :].astype(F32),
                pair_ref[4 * rows + 8 : 4 * rows + 16, :].astype(F32),
            )
            so_far = [carry[h] for h in range(heads)]
            mix, weights, totals = stick_block(q_ref[...], k, v, off, hd, suffix, so_far, False)
            acc[...] = acc[...] + mix
            for h in range(heads):
                mass[h] = mass[h] + weights[h]
                carry[h] = so_far[h] + totals[h]

        return 0

    lax.fori_loop(1, me + 1, earlier, 0)
    mixed = acc[...]
    squares = mixed * mixed
    inverse = jnp.zeros_like(mixed)
    for h in range(heads):
        mean = jnp.sum(jnp.where(lane == h, squares, 0.0), axis=1, keepdims=True) / hd
        inverse = jnp.where(lane == h, lax.rsqrt(mean + norm_eps), inverse)
    gain = jnp.concatenate([gain_ref[h : h + 1, :] for h in range(heads)], axis=1)
    out_ref[...] = (mixed * inverse * gain).astype(BF16)
    for h in range(heads):
        log_ref[h : h + 1, :] = jnp.log(jnp.sum(jnp.transpose(mass[h]), axis=0, keepdims=True))


def attention(q, pair, head_gain, near, after):
    rows, width = q.shape
    heads = head_gain.shape[0]
    return pl.pallas_call(
        attention_kernel,
        out_shape=(shape((rows, width)), shape((heads, rows), F32)),
        in_specs=[VM] * 6 + [ANY],
        out_specs=[VM] * 2,
        scratch_shapes=[
            pltpu.VMEM((rows, width), F32),
            pltpu.VMEM((heads, rows, rows), F32),
            pltpu.VMEM((heads, rows, rows), F32),
        ],
        cost_estimate=cost(400_000_000, 1_000_000),
        compiler_params=params(),
        name="stick_attention",
    )(q, pair, head_gain, *near, after)


def final_kernel(*refs):
    act, wa, wc = (refs[n * 4 : (n + 1) * 4] for n in range(3))
    gain_ref, out_ref = refs[12:]
    cw = wc[0].shape[0]
    aw = act[0].shape[1] - cw
    convs = [c[:, aw:].astype(F32) for c in act]
    mean = sum(jnp.sum(v, axis=1, keepdims=True) for v in convs) / (4 * cw)
    centered = [v - mean for v in convs]
    spread = sum(jnp.sum(v * v, axis=1, keepdims=True) for v in centered) / (4 * cw)
    inverse = lax.rsqrt(spread + norm_eps)
    total = None
    for slot in range(4):
        pieces = [wa[slot][aw : aw + 1, n * cw : (n + 1) * cw].astype(F32) for n in range(6)]
        gain = pieces[0] + pieces[1] + pieces[2]
        bias = pieces[3] + pieces[4] + pieces[5]
        y = centered[slot] * inverse * gain + bias
        y = (y * jax.nn.sigmoid(y)).astype(BF16)
        part = dot_f32(act[slot][:, :aw], wa[slot][:aw, :]) + dot_f32(y, wc[slot][...])
        total = part if total is None else total + part
    squares = jnp.mean(total * total, axis=1, keepdims=True)
    out_ref[...] = (total * lax.rsqrt(squares + norm_eps) * gain_ref[...]).astype(BF16)


def finish(act, wa, wc, out_gain):
    rows, width = act[0].shape[0], wa[0].shape[1]
    return pl.pallas_call(
        final_kernel,
        out_shape=shape((rows, width)),
        in_specs=[VM] * 13,
        out_specs=VM,
        cost_estimate=cost(800_000_000, 7_000_000),
        compiler_params=params(32),
        name="finish_rows",
    )(*act, *wa, *wc, out_gain.reshape(1, width))


def paired(
    tokens,
    norm_gain,
    w_query,
    w_key,
    w_value,
    w_glu_value,
    w_glu_gate,
    key_offset,
    head_gain,
    conv_taps,
    channel_gain,
    channel_bias,
    w_out_attn,
    w_out_conv,
    out_gain,
):
    own_qkv, half_qkv = pack_qkv((w_query, w_key, w_value))
    qkv_same = exchange(half_qkv, "sp", 1)
    wc_x = exchange(w_out_conv, "tp", 2)
    x_send, mine_own, mine_pair = norm_parts(tokens, norm_gain, w_query.shape[0])
    x_got = exchange(x_send, "sp", 2)
    own_glu, wa_mine, off = pack(
        w_glu_value, w_glu_gate, w_out_attn, key_offset.T, channel_gain, channel_bias
    )
    glu_pair = exchange(own_glu, "sp", 1)
    qkv_other = exchange(qkv_same, "grp", 1)
    x_other = exchange(x_got, "tp", 1)
    wa_x = exchange(wa_mine, "tp", 2)
    wc_core = exchange(w_out_conv, "tp", 1)
    wa_core = exchange(wa_mine, "tp", 1)
    wc_xc = exchange(wc_x, "tp", 1)
    wa_xc = exchange(wa_x, "tp", 1)
    x_own, x_pair = assemble(mine_own, mine_pair, x_got, x_other)

    keep, sent = project_qkv(x_own, x_pair, own_qkv, qkv_same, qkv_other, off)
    got = exchange(sent, "sp", 2)
    glu_keep, glu_sent = project_glu(x_own, x_pair, own_glu, glu_pair, sent)
    glu_got = exchange(glu_sent, "sp", 2)
    q, mine_two = sum_qkv(keep, got, sent, glu_sent)
    pair_two = exchange(mine_two, "sp", 1)
    near = near_attention(q, mine_two, head_gain, mine_two)
    gated, tail = gate(glu_keep, glu_got, -(-conv_taps.shape[0] // 16) * 16)
    before = from_behind(tail, "sp", 1)
    attended, log_mass = attention(q, pair_two, head_gain, near, tail)
    act_mine = conv(gated, before, conv_taps, attended)
    act = [act_mine] + [exchange(act_mine, "tp", bit) for bit in (1, 2, 3)]
    wa = (wa_mine, wa_core, wa_x, wa_xc)
    wc = (w_out_conv, wc_core, wc_x, wc_xc)
    mixed = finish(act, wa, wc, out_gain)
    return (mixed, log_mass)


def gathered(
    tokens,
    norm_gain,
    w_query,
    w_key,
    w_value,
    w_glu_value,
    w_glu_gate,
    key_offset,
    head_gain,
    conv_taps,
    channel_gain,
    channel_bias,
    w_out_attn,
    w_out_conv,
    out_gain,
):
    row_count = tokens.shape[0]
    hd = head_gain.shape[1]
    channels = conv_taps.shape[1] * lax.axis_size("tp")
    normed = row_norm(tokens.astype(jnp.float32), norm_gain).astype(jnp.bfloat16)
    weights_in = (w_query, w_key, w_value, w_glu_value, w_glu_gate)
    pieces = (
        lax.all_gather(weights_in[0], "sp", axis=0, tiled=True),
        lax.all_gather(weights_in[1], "sp", axis=0, tiled=True),
        lax.all_gather(weights_in[2], "sp", axis=0, tiled=True),
        lax.all_gather(weights_in[3], "sp", axis=0, tiled=True),
        lax.all_gather(weights_in[4], "sp", axis=0, tiled=True),
    )
    projected = tuple(
        (jnp.dot(normed, shard_piece, preferred_element_type=jnp.float32) for shard_piece in pieces)
    )
    query, key_rows, value_rows, glu_value, glu_gate = [
        summed.astype(jnp.bfloat16) for summed in projected
    ]
    kv_local = key_rows.shape[1] // hd
    group_size = query.shape[1] // key_rows.shape[1]
    heads_local = kv_local * group_size
    all_keys, all_values, all_offsets = (
        lax.all_gather(key_rows, "sp", axis=0, tiled=True),
        lax.all_gather(value_rows, "sp", axis=0, tiled=True),
        lax.all_gather(key_offset, "sp", axis=0, tiled=True),
    )
    sequence_length_total = all_keys.shape[0]
    shard_count = lax.axis_size("sp")
    per_block = 1
    while (
        per_block * 2 <= shard_count
        and shard_count % (per_block * 2) == 0
        and (per_block * 2 * row_count <= 1024)
    ):
        per_block = per_block * 2
    span_len = per_block * row_count
    query_heads = query.reshape(row_count, kv_local, group_size, hd)
    key_heads = all_keys.reshape(sequence_length_total, kv_local, hd)
    value_heads = all_values.reshape(sequence_length_total, kv_local, hd)
    my_index = lax.axis_index("sp")
    query_pos = my_index * row_count + jnp.arange(row_count, dtype=jnp.int32)
    last_block = my_index // per_block
    zeros_mix = jnp.zeros((kv_local, group_size, row_count, hd), jnp.float32)
    zeros_row = jnp.zeros((kv_local, group_size, row_count), jnp.float32)

    def sweep(turn_index, carry):
        head_mix, mass_sum, carried = carry
        first_key = (last_block - turn_index) * span_len
        key_block = lax.dynamic_slice_in_dim(key_heads, first_key, span_len, 0)
        value_block = lax.dynamic_slice_in_dim(value_heads, first_key, span_len, 0)
        offset_block = lax.dynamic_slice_in_dim(all_offsets, first_key, span_len, 0).astype(
            jnp.float32
        )
        offset_block = offset_block.T.reshape(kv_local, group_size, 1, span_len)
        scores = (
            jnp.einsum("qhgd,khd->hgqk", query_heads, key_block, preferred_element_type=jnp.float32)
            * hd ** (-0.5)
            + offset_block
        )
        key_pos = first_key + jnp.arange(span_len, dtype=jnp.int32)
        allowed = key_pos[None, :] <= query_pos[:, None]
        log_not = jnp.where(allowed, jax.nn.log_sigmoid(-scores), 0.0)
        later = lax.cumsum(log_not, axis=3, reverse=True) - log_not + carried[..., None]
        weights = jnp.where(allowed, jnp.exp(jax.nn.log_sigmoid(scores) + later), 0.0)
        head_mix = head_mix + jnp.einsum(
            "hgqk,khd->hgqd",
            weights.astype(jnp.bfloat16),
            value_block,
            preferred_element_type=jnp.float32,
        )
        return (head_mix, mass_sum + jnp.sum(weights, axis=3), carried + jnp.sum(log_not, axis=3))

    head_mix, mass_sum, _ = lax.fori_loop(
        0, last_block + 1, sweep, (zeros_mix, zeros_row, zeros_row)
    )
    log_mass = jnp.log(mass_sum).reshape(heads_local, row_count)
    head_rows = head_mix.transpose(2, 0, 1, 3).reshape(row_count, heads_local, hd)
    attended = (
        row_norm(head_rows, head_gain).astype(jnp.bfloat16).reshape(row_count, heads_local * hd)
    )
    gated = (glu_value.astype(jnp.float32) * jax.nn.sigmoid(glu_gate.astype(jnp.float32))).astype(
        jnp.bfloat16
    )
    reach_len = conv_taps.shape[0] - 1
    before = from_behind(gated[row_count - reach_len :], "sp", 1)
    padded = jnp.concatenate([before, gated], axis=0).astype(jnp.float32)
    conv_out = jnp.zeros(gated.shape, jnp.float32)
    for tap_index in range(conv_taps.shape[0]):
        conv_out = conv_out + conv_taps[tap_index] * padded[tap_index : tap_index + row_count]
    total_sum, total_squares = lax.psum(
        (jnp.sum(conv_out, axis=1), jnp.sum(conv_out * conv_out, axis=1)), "tp"
    )
    chan_mean = (total_sum / channels)[:, None]
    spread = (total_squares / channels)[:, None] - chan_mean * chan_mean
    centered = conv_out - chan_mean
    channel_out = jax.nn.silu(
        centered * lax.rsqrt(spread + norm_eps) * channel_gain + channel_bias
    ).astype(jnp.bfloat16)
    share = lax.psum_scatter(
        jnp.dot(attended, w_out_attn, preferred_element_type=jnp.float32)
        + jnp.dot(channel_out, w_out_conv, preferred_element_type=jnp.float32),
        "tp",
        scatter_dimension=0,
        tiled=True,
    )
    mixed = lax.all_gather(row_norm(share, out_gain).astype(jnp.bfloat16), "tp", axis=0, tiled=True)
    return (mixed, log_mass)


def solution(mesh):
    in_specs = (
        P(("grp", "sp"), None),
        P(),
        P("sp", "tp"),
        P("sp", "tp"),
        P("sp", "tp"),
        P("sp", "tp"),
        P("sp", "tp"),
        P(("grp", "sp"), "tp"),
        P("tp", None),
        P(None, "tp"),
        P("tp"),
        P("tp"),
        P("tp", None),
        P("tp", None),
        P(),
    )
    out_specs = (P(("grp", "sp"), None), P("tp", ("grp", "sp")))
    small = mesh.shape["sp"] == 4 and mesh.shape["tp"] == 4 and mesh.shape["grp"] == 2
    local = paired if small else gathered
    return jax.shard_map(local, mesh=mesh, in_specs=in_specs, out_specs=out_specs, check_vma=False)
```

```python
import jax
import jax.numpy as jnp
from jax import lax
from jax.experimental import pallas as pl
from jax.experimental.pallas import tpu as pltpu
from jax.sharding import PartitionSpec as P

norm_eps = 1e-06
BF16 = jnp.bfloat16
F32 = jnp.float32


def exchange(value, axis, bit):
    count = lax.axis_size(axis)
    return lax.ppermute(value, axis, [(s, s ^ bit) for s in range(count)])


def from_behind(value, axis, steps):
    count = lax.axis_size(axis)
    initial, last = (max(0, -steps), min(count, count - steps))
    return lax.ppermute(value, axis, [(source, source + steps) for source in range(initial, last)])


def row_norm(values_in, gain_vec):
    squares = jnp.mean(values_in * values_in, axis=-1, keepdims=True)
    return values_in * lax.rsqrt(squares + norm_eps) * gain_vec


def dot_f32(a, b, dims=((1,), (0,))):
    return lax.dot_general(a, b, (dims, ((), ())), preferred_element_type=F32)


def params(limit=16):
    return pltpu.CompilerParams(vmem_limit_bytes=limit * 1024 * 1024)


VM = pl.BlockSpec(memory_space=pltpu.VMEM)
ANY = pl.BlockSpec(memory_space=pl.ANY)
HBM = pl.BlockSpec(memory_space=pltpu.HBM)


def shape(dims, dtype=BF16):
    return jax.ShapeDtypeStruct(dims, dtype)


def cost(flops, moved):
    return pl.CostEstimate(flops=flops, bytes_accessed=moved, transcendentals=0)


def in_hbm(*values):
    return [pltpu.with_memory_space_constraint(v, pltpu.HBM) for v in values]


def pack_qkv_kernel(wq, wk, wv, wc, all_ref, send_ref, wc_ref, sems):
    part, width = send_ref.shape[0], wq.shape[1]
    group = lax.axis_index("grp")
    mine = pl.ds(pl.multiple_of(group * part, part), part)
    columns = wc_ref.shape[1]
    first, rest = [], []
    for n, w in enumerate((wq, wk, wv)):
        at = slice(n * width, (n + 1) * width)
        first.append(pltpu.make_async_copy(w.at[mine, :], send_ref.at[:, at], sems.at[n]))
        rest.append(pltpu.make_async_copy(w, all_ref.at[:, at], sems.at[3 + n]))
    half = wc.at[:, pl.ds(pl.multiple_of(group * columns, columns), columns)]
    rest.append(pltpu.make_async_copy(half, wc_ref, sems.at[6]))
    for copy in first + rest:
        copy.start()
    for copy in first + rest:
        copy.wait()


def pack_qkv(weights, wc):
    block, width = weights[0].shape
    return pl.pallas_call(
        pack_qkv_kernel,
        out_shape=(
            shape((block, 3 * width)),
            shape((block // 2, 3 * width)),
            shape((wc.shape[0], wc.shape[1] // 2)),
        ),
        in_specs=[HBM] * 4,
        out_specs=[VM] * 3,
        scratch_shapes=[pltpu.SemaphoreType.DMA((7,))],
        cost_estimate=cost(2_000_000, 400_000),
        compiler_params=params(),
        name="pack_qkv",
    )(*in_hbm(*weights, wc))


def norm_kernel(x_hbm, gain_hbm, send_ref, own_ref, pair_ref, x_ref, gain_ref, normed, sems):
    side, low = lax.axis_index("sp") // 2, lax.axis_index("sp") % 2
    core = lax.axis_index("tp") % 2
    block = own_ref.shape[1]
    half = 2 * block
    half_rows = send_ref.shape[0]
    copies = [
        pltpu.make_async_copy(x_hbm, x_ref, sems.at[0]),
        pltpu.make_async_copy(gain_hbm, gain_ref, sems.at[1]),
    ]
    for copy in copies:
        copy.start()
    for copy in copies:
        copy.wait()
    x = x_ref[...].astype(F32)
    squares = jnp.mean(x * x, axis=1, keepdims=True)
    normed[...] = (x * lax.rsqrt(squares + norm_eps) * gain_ref[...]).astype(BF16)
    first = pl.multiple_of(core * half_rows, half_rows)
    away = pl.multiple_of((1 - side) * half, half)
    send_ref[...] = normed[pl.ds(first, half_rows), pl.ds(away, half)]
    own_ref[...] = normed[:, pl.ds(pl.multiple_of(side * half + low * block, block), block)]
    pair_ref[...] = normed[:, pl.ds(pl.multiple_of(side * half + (1 - low) * block, block), block)]


def norm_parts(tokens, gain, block):
    rows, features = tokens.shape
    return pl.pallas_call(
        norm_kernel,
        out_shape=(shape((rows // 2, 2 * block)), shape((rows, block)), shape((rows, block))),
        in_specs=[HBM] * 2,
        out_specs=[VM] * 3,
        scratch_shapes=[
            pltpu.VMEM((rows, features), BF16),
            pltpu.VMEM((1, features), F32),
            pltpu.VMEM((rows, features), BF16),
            pltpu.SemaphoreType.DMA((2,)),
        ],
        cost_estimate=cost(2_000_000, 1_000_000),
        compiler_params=params(),
        name="norm_parts",
    )(*in_hbm(tokens, gain.reshape(1, features)))


def pack_kernel(
    gv_hbm, gg_hbm, wa_hbm, off_hbm, gain_hbm, bias_hbm, gv_ref, gv_send, gg_ref, out_ref, off_ref, gain_ref, bias_ref, sems
):
    cw, aw = gv_hbm.shape[1], wa_hbm.shape[0]
    part = gv_send.shape[0]
    mine = pl.ds(pl.multiple_of(lax.axis_index("grp") * part, part), part)
    pairs = (
        (gain_hbm, gain_ref),
        (bias_hbm, bias_ref),
        (gv_hbm.at[mine, :], gv_send),
        (gg_hbm, gg_ref),
        (wa_hbm, out_ref.at[:aw, :]),
        (off_hbm, off_ref),
        (gv_hbm, gv_ref),
    )
    copies = [pltpu.make_async_copy(a, b, sems.at[n]) for n, (a, b) in enumerate(pairs)]
    for copy in copies:
        copy.start()
    for copy in copies[:2]:
        copy.wait()
    extra = out_ref.shape[0] - aw
    for n, ref in enumerate((gain_ref, bias_ref)):
        rest = ref[...]
        for piece in range(3):
            part = rest.astype(BF16)
            rest = rest - part.astype(F32)
            first = (3 * n + piece) * cw
            out_ref[aw:, first : first + cw] = jnp.broadcast_to(part, (extra, cw))
    for copy in copies[2:]:
        copy.wait()


def pack(gv, gg, wa, off, gain, bias):
    block, cw = gv.shape
    aw, width = wa.shape
    return pl.pallas_call(
        pack_kernel,
        out_shape=(
            shape((block, cw)),
            shape((block // 2, cw)),
            shape((block, cw)),
            shape((aw + 16, width)),
            shape(off.shape),
        ),
        in_specs=[HBM] * 6,
        out_specs=[VM] * 5,
        scratch_shapes=[
            pltpu.VMEM((1, cw), F32),
            pltpu.VMEM((1, cw), F32),
            pltpu.SemaphoreType.DMA((7,)),
        ],
        cost_estimate=cost(2_000_000, 2_000_000),
        compiler_params=params(),
        name="pack",
    )(*in_hbm(gv, gg, wa, off, gain.reshape(1, cw), bias.reshape(1, cw)))


def assemble_kernel(own_ref, pair_ref, got_ref, other_ref, own_out, pair_out):
    low = lax.axis_index("sp") % 2
    core = lax.axis_index("tp") % 2
    rows, block = own_ref.shape
    half = got_ref.shape[0]
    own_out[:rows, :] = own_ref[...]
    pair_out[:rows, :] = pair_ref[...]
    own_at = pl.multiple_of(low * block, block)
    pair_at = pl.multiple_of((1 - low) * block, block)
    for part, at in ((got_ref, core), (other_ref, 1 - core)):
        first = pl.multiple_of(rows + at * half, half)
        own_out[pl.ds(first, half), :] = part[:, pl.ds(own_at, block)]
        pair_out[pl.ds(first, half), :] = part[:, pl.ds(pair_at, block)]


def assemble(own, pair, got, other):
    rows, block = own.shape
    return pl.pallas_call(
        assemble_kernel,
        out_shape=(shape((2 * rows, block)),) * 2,
        in_specs=[VM] * 4,
        out_specs=[VM] * 2,
        cost_estimate=cost(2_000_000, 1_000_000),
        compiler_params=params(),
        name="assemble",
    )(own, pair, got, other)


def far_dot(x_pair, same, other):
    part = same.shape[0]
    group = lax.axis_index("grp")
    near = x_pair[:, pl.ds(pl.multiple_of(group * part, part), part)]
    rest = x_pair[:, pl.ds(pl.multiple_of((1 - group) * part, part), part)]
    return dot_f32(near, same[...]) + dot_f32(rest, other[...])


def pick(second, a, b):
    return jnp.where(second == 1, b, a)


def qkv_kernel(x_own, x_pair, own, same, other, off_ref, keep_ref, send_ref):
    rows = x_own.shape[0] // 2
    width = send_ref.shape[1]
    hd = width // 2
    side = lax.axis_index("sp") // 2
    total = dot_f32(x_own[...], own[...]) + far_dot(x_pair, same, other)
    q, k, v = (total[:, n * width : (n + 1) * width] for n in range(3))
    heads = [slice(0, hd), slice(hd, width)]
    kvs = [jnp.concatenate([k[:, at], v[:, at]], axis=1) for at in heads]
    ordered = [jnp.concatenate([q[:rows, at], q[rows:, at]], axis=1) for at in heads]
    swapped = [jnp.concatenate([q[rows:, at], q[:rows, at]], axis=1) for at in heads]
    mine = pick(side, kvs[0], kvs[1])
    theirs = pick(side, kvs[1], kvs[0]).astype(BF16)
    for n, block in enumerate((side, 1 - side)):
        at = pl.ds(pl.multiple_of(block * rows, rows), rows)
        keep_ref[at, :] = mine[n * rows : (n + 1) * rows]
        send_ref[at, :] = theirs[n * rows : (n + 1) * rows]
    keep_ref[2 * rows :, :] = pick(side, ordered[0], swapped[1])
    send_ref[2 * rows : 3 * rows, :] = pick(side, ordered[1], swapped[0]).astype(BF16)
    offsets = off_ref[...].astype(F32)
    off = pick(side, offsets[1:2], offsets[0:1]).astype(BF16)
    send_ref[3 * rows :, :] = jnp.broadcast_to(off, (send_ref.shape[0] - 3 * rows, width))


def project_qkv(x_own, x_pair, own, same, other, off):
    rows, width = x_own.shape[0] // 2, own.shape[1] // 3
    return pl.pallas_call(
        qkv_kernel,
        out_shape=(shape((3 * rows, width), F32), shape((3 * rows + 16, width))),
        in_specs=[VM] * 6,
        out_specs=[VM] * 2,
        cost_estimate=cost(200_000_000, 1_000_000),
        compiler_params=params(),
        name="project_qkv",
    )(x_own, x_pair, own, same, other, off)


def sum_kernel(keep_ref, got_ref, off_ref, after, q_ref, kv_ref):
    rows, width = keep_ref.shape[0] // 3, keep_ref.shape[1]
    hd = width // 2
    side = lax.axis_index("sp") // 2
    kv_ref[: 2 * rows, :] = (keep_ref[: 2 * rows, :] + got_ref[: 2 * rows, :].astype(F32)).astype(BF16)
    q = keep_ref[2 * rows :, :] + got_ref[2 * rows : 3 * rows, :].astype(F32)
    none = jnp.zeros((rows, hd), F32)
    q_ref[:rows, :] = jnp.concatenate([q[:, :hd], none], axis=1).astype(BF16)
    q_ref[rows:, :] = jnp.concatenate([q[:, hd:], none], axis=1).astype(BF16)
    offsets = off_ref[...].astype(F32)
    mine = jnp.broadcast_to(pick(side, offsets[0:1], offsets[1:2]), (8, width))
    theirs = got_ref[3 * rows : 3 * rows + 8, :].astype(F32)
    both = jnp.concatenate([pick(side, mine, theirs), pick(side, theirs, mine)])
    kv_ref[2 * rows :, :] = both.astype(BF16)


def sum_qkv(keep, got, off, after):
    rows, width = keep.shape[0] // 3, got.shape[1]
    return pl.pallas_call(
        sum_kernel,
        out_shape=(shape((2 * rows, width)), shape((2 * rows + 16, width))),
        in_specs=[VM] * 3 + [ANY],
        out_specs=[VM] * 2,
        cost_estimate=cost(1_000_000, 1_000_000),
        compiler_params=params(),
        name="sum_qkv",
    )(keep, got, off, after)


def glu_kernel(x_own, x_pair, gv, gg, gv_same, gv_other, gg_pair, after, keep_ref, send_ref):
    rows = x_own.shape[0] // 2
    cw = gv.shape[1]
    for n in range(2):
        own = (gv, gg)[n]
        far = far_dot(x_pair, gv_same, gv_other) if n == 0 else dot_f32(x_pair[...], gg_pair[...])
        total = dot_f32(x_own[...], own[...]) + far
        at = slice(n * cw, (n + 1) * cw)
        keep_ref[:, at] = total[:rows]
        send_ref[:, at] = total[rows:].astype(BF16)


def project_glu(x_own, x_pair, own, pair, after):
    rows, width = x_own.shape[0] // 2, 2 * own[0].shape[1]
    return pl.pallas_call(
        glu_kernel,
        out_shape=(shape((rows, width), F32), shape((rows, width))),
        in_specs=[VM] * 7 + [ANY],
        out_specs=[VM] * 2,
        cost_estimate=cost(270_000_000, 1_000_000),
        compiler_params=params(),
        name="project_glu",
    )(x_own, x_pair, *own, *pair, after)


def gate_kernel(keep_ref, got_ref, after, gated_ref, tail_ref):
    rows, cw = gated_ref.shape
    glu = keep_ref[...] + got_ref[...].astype(F32)
    value = glu[:, :cw].astype(BF16).astype(F32)
    gated = (value * jax.nn.sigmoid(glu[:, cw:].astype(BF16).astype(F32))).astype(BF16)
    gated_ref[...] = gated
    tail_ref[...] = gated[rows - tail_ref.shape[0] :]


def gate(keep, got, tail, after):
    rows, cw = keep.shape[0], keep.shape[1] // 2
    return pl.pallas_call(
        gate_kernel,
        out_shape=(shape((rows, cw)), shape((tail, cw))),
        in_specs=[VM] * 2 + [ANY],
        out_specs=[VM] * 2,
        cost_estimate=cost(2_000_000, 500_000),
        compiler_params=params(),
        name="gate",
    )(keep, got, after)


def conv_kernel(gated_ref, before_ref, taps_ref, att_ref, got_ref, own_log, act_ref, log_ref, padded):
    rows, aw = att_ref.shape
    tail, taps, hd = before_ref.shape[0], taps_ref.shape[0], aw // 2
    side = lax.axis_index("sp") // 2
    padded[:tail, :] = before_ref[...].astype(F32)
    padded[tail:, :] = gated_ref[...].astype(F32)
    total = None
    for tap in range(taps):
        first = tail - (taps - 1) + tap
        part = taps_ref[tap : tap + 1, :] * padded[first : first + rows, :]
        total = part if total is None else total + part
    act_ref[:, aw:] = total.astype(BF16)
    half = rows // 2
    both = got_ref[:half, :].astype(F32)
    theirs = jnp.concatenate([both[:, :hd], both[:, hd:]], axis=0)
    none = jnp.zeros_like(theirs)
    placed = pick(side, jnp.concatenate([none, theirs], axis=1), jnp.concatenate([theirs, none], axis=1))
    act_ref[:, :aw] = (att_ref[...].astype(F32) + placed).astype(BF16)
    pieces = [got_ref[half + 16 * n : half + 16 * n + 1, :].astype(F32) for n in range(3)]
    far_log = pieces[0] + pieces[1] + pieces[2]
    near_log = own_log[0:1, :]
    log_ref[0:1, :] = pick(side, near_log, far_log)
    log_ref[1:2, :] = pick(side, far_log, near_log)


def conv(gated, before, taps, attended, att_got, own_log):
    rows, cw = gated.shape
    return pl.pallas_call(
        conv_kernel,
        out_shape=(shape((rows, attended.shape[1] + cw)), shape((2, rows), F32)),
        in_specs=[VM] * 6,
        out_specs=[VM] * 2,
        scratch_shapes=[pltpu.VMEM((rows + before.shape[0], cw), F32)],
        cost_estimate=cost(20_000_000, 500_000),
        compiler_params=params(),
        name="conv",
    )(gated, before, taps, attended, att_got, own_log)


def suffix_matrix(keys):
    before = lax.broadcasted_iota(jnp.int32, (2 * keys, 2 * keys), 0) % keys
    column = lax.broadcasted_iota(jnp.int32, (2 * keys, 2 * keys), 1)
    return jnp.where((column >= keys) | (before > column), 1.0, 0.0).astype(BF16)


def stick_block(q, kv, off, suffix, carry, diagonal):
    rows, keys = q.shape[0], kv.shape[0]
    s = dot_f32(q, kv, ((1,), (1,))) * (q.shape[1] // 2) ** (-0.5) + off
    soft = jnp.maximum(s, 0.0) + jnp.log(1.0 + jnp.exp(-jnp.abs(s)))
    log_not = -soft
    if diagonal:
        column = lax.broadcasted_iota(jnp.int32, (rows, keys), 1)
        allowed = column <= lax.broadcasted_iota(jnp.int32, (rows, keys), 0)
        log_not = jnp.where(allowed, log_not, 0.0)
    high = log_not.astype(BF16)
    low = (log_not - high.astype(F32)).astype(BF16)
    sums = dot_f32(jnp.concatenate([high, low], axis=1), suffix)
    later = sums[:, :keys]
    if carry is not None:
        later = later + carry
    w = jnp.exp(s - soft + later)
    if diagonal:
        w = jnp.where(allowed, w, 0.0)
    return w, sums[:, keys:]


def block_of(ref, n):
    rows = (ref.shape[0] - 16) // 2
    return ref[n * rows : (n + 1) * rows, :], ref[2 * rows + 8 * n : 2 * rows + 8 * n + 8, :].astype(F32)[0:1]


def near_kernel(q_ref, kv_ref, after, mix_ref, mass_ref, carry_ref):
    rows = q_ref.shape[0] // 2
    suffix = suffix_matrix(rows)
    for n, (query, key) in enumerate(((0, 0), (1, 1), (1, 0))):
        kv, off = block_of(kv_ref, key)
        q = q_ref[query * rows : (query + 1) * rows, :]
        w, total = stick_block(q, kv, off, suffix, None, query == key)
        mix_ref[n] = dot_f32(w.astype(BF16), kv)
        mass_ref[n] = w
        carry_ref[n] = total


def near_attention(q, kv, after):
    rows, width = q.shape[0] // 2, q.shape[1]
    out = shape((3, rows, rows), F32)
    return pl.pallas_call(
        near_kernel,
        out_shape=(shape((3, rows, width), F32), out, out),
        in_specs=[VM] * 2 + [ANY],
        out_specs=[VM] * 3,
        cost_estimate=cost(200_000_000, 1_000_000),
        compiler_params=params(),
        name="near_attention",
    )(q, kv, after)


def attention_kernel(
    q_ref, pair_ref, gain_ref, mix_ref, mass_ref, carry_ref, after, own_ref, send_ref, log_ref, acc, mass, carry
):
    side, odd = lax.axis_index("sp") // 2, lax.axis_index("sp") % 2
    rows, width = q_ref.shape[0] // 2, q_ref.shape[1]
    hd = width // 2
    suffix = suffix_matrix(rows)
    acc[:rows, :] = mix_ref[0]
    acc[rows:, :] = mix_ref[1]
    mass[:rows, :] = mass_ref[0]
    mass[rows:, :] = mass_ref[1]
    carry[...] = carry_ref[1]

    @pl.when(odd == 1)
    def _():
        kv, off = block_of(pair_ref, 1)
        w, total = stick_block(q_ref[rows:, :], kv, off, suffix, carry[...], False)
        acc[rows:, :] = acc[rows:, :] + dot_f32(w.astype(BF16), kv)
        mass[rows:, :] = mass[rows:, :] + w
        carry[...] = carry[...] + total

    share = odd.astype(F32)
    so_far = carry[...]
    kv, off = block_of(pair_ref, 0)
    both = jnp.concatenate([carry_ref[0], so_far + share * carry_ref[2]])
    w, total = stick_block(q_ref[...], kv, off, suffix, both, False)
    w = jnp.concatenate([share * w[:rows], w[rows:]])
    scale = jnp.exp(so_far + (1.0 - share) * total[rows:])
    acc[...] = acc[...] + dot_f32(w.astype(BF16), kv)
    acc[rows:, :] = acc[rows:, :] + scale * mix_ref[2]
    mass[...] = mass[...] + w
    mass[rows:, :] = mass[rows:, :] + scale * mass_ref[2]

    mixed = acc[...]
    lane = lax.broadcasted_iota(jnp.int32, (rows, width), 1)
    squares = jnp.where(lax.broadcasted_iota(jnp.int32, mixed.shape, 1) >= hd, mixed * mixed, 0.0)
    mean = jnp.sum(squares, axis=1, keepdims=True) / hd
    gain = pick(side, gain_ref[0:1, :], gain_ref[1:2, :])
    att = mixed * lax.rsqrt(mean + norm_eps) * jnp.concatenate([gain, gain], axis=1)
    own = pick(side, att[:rows], att[rows:])
    cross = pick(side, att[rows:], att[:rows])
    swapped = jnp.concatenate([own[:, hd:], own[:, :hd]], axis=1)
    own = pick(side, jnp.where(lane < hd, swapped, 0.0), jnp.where(lane >= hd, own, 0.0))
    own_ref[...] = own.astype(BF16)
    half = rows // 2
    send_ref[:half, :] = jnp.concatenate([cross[:half, hd:], cross[half:, hd:]], axis=1).astype(BF16)
    logs = [jnp.log(jnp.sum(jnp.transpose(mass[n * rows : (n + 1) * rows]), axis=0, keepdims=True)) for n in range(2)]
    log_ref[...] = jnp.broadcast_to(pick(side, logs[0], logs[1]), log_ref.shape)
    rest = pick(side, logs[1], logs[0])
    for n in range(3):
        part = rest.astype(BF16)
        rest = rest - part.astype(F32)
        send_ref[half + 16 * n : half + 16 * (n + 1), :] = jnp.broadcast_to(part, (16, width))


def attention(q, pair, head_gain, near, after):
    rows, width = q.shape[0] // 2, q.shape[1]
    return pl.pallas_call(
        attention_kernel,
        out_shape=(shape((rows, width)), shape((rows // 2 + 48, width)), shape((8, rows), F32)),
        in_specs=[VM] * 6 + [ANY],
        out_specs=[VM] * 3,
        scratch_shapes=[
            pltpu.VMEM((2 * rows, width), F32),
            pltpu.VMEM((2 * rows, rows), F32),
            pltpu.VMEM((rows, rows), F32),
        ],
        cost_estimate=cost(400_000_000, 1_000_000),
        compiler_params=params(),
        name="stick_attention",
    )(q, pair, head_gain, *near, after)


def final_kernel(*refs):
    act, wa, wc, gain_ref, out_ref = refs[:4], refs[4:8], refs[8:14], refs[14], refs[15]
    cw = wc[0].shape[0]
    aw = act[0].shape[1] - cw
    convs = [c[:, aw:].astype(F32) for c in act]
    mean = sum(jnp.sum(v, axis=1, keepdims=True) for v in convs) / (4 * cw)
    centered = [v - mean for v in convs]
    spread = sum(jnp.sum(v * v, axis=1, keepdims=True) for v in centered) / (4 * cw)
    inverse = lax.rsqrt(spread + norm_eps)
    total = None
    ys = []
    for slot in range(4):
        pieces = [wa[slot][aw : aw + 1, n * cw : (n + 1) * cw].astype(F32) for n in range(6)]
        gain = pieces[0] + pieces[1] + pieces[2]
        bias = pieces[3] + pieces[4] + pieces[5]
        y = centered[slot] * inverse * gain + bias
        y = (y * jax.nn.sigmoid(y)).astype(BF16)
        part = dot_f32(act[slot][:, :aw], wa[slot][:aw, :])
        if slot < 2:
            part = part + dot_f32(y, wc[slot][...])
        total = part if total is None else total + part
        ys.append(y)
    same = dot_f32(ys[2], wc[2][...]) + dot_f32(ys[3], wc[4][...])
    other = dot_f32(ys[2], wc[3][...]) + dot_f32(ys[3], wc[5][...])
    swap = lax.axis_index("grp") == 1
    total = total + jnp.concatenate([jnp.where(swap, other, same), jnp.where(swap, same, other)], axis=1)
    squares = jnp.mean(total * total, axis=1, keepdims=True)
    out_ref[...] = (total * lax.rsqrt(squares + norm_eps) * gain_ref[...]).astype(BF16)


def finish(act, wa, wc, out_gain):
    rows, width = act[0].shape[0], wa[0].shape[1]
    return pl.pallas_call(
        final_kernel,
        out_shape=shape((rows, width)),
        in_specs=[VM] * 15,
        out_specs=VM,
        cost_estimate=cost(800_000_000, 7_000_000),
        compiler_params=params(32),
        name="finish_rows",
    )(*act, *wa, *wc, out_gain.reshape(1, width))


def paired(
    tokens,
    norm_gain,
    w_query,
    w_key,
    w_value,
    w_glu_value,
    w_glu_gate,
    key_offset,
    head_gain,
    conv_taps,
    channel_gain,
    channel_bias,
    w_out_attn,
    w_out_conv,
    out_gain,
):
    own_qkv, half_qkv, wc_half = pack_qkv((w_query, w_key, w_value), w_out_conv)
    qkv_same = exchange(half_qkv, "sp", 1)
    wc_x = exchange(wc_half, "tp", 2)
    x_send, mine_own, mine_pair = norm_parts(tokens, norm_gain, w_query.shape[0])
    x_got = exchange(x_send, "sp", 2)
    own_gv, half_gv, own_gg, wa_mine, off = pack(
        w_glu_value, w_glu_gate, w_out_attn, key_offset.T, channel_gain, channel_bias
    )
    qkv_other = exchange(qkv_same, "grp", 1)
    gv_same = exchange(half_gv, "sp", 1)
    gg_pair = exchange(own_gg, "sp", 1)
    x_other = exchange(x_got, "tp", 1)
    wa_x = exchange(wa_mine, "tp", 2)
    wc_core = exchange(w_out_conv, "tp", 1)
    wa_core = exchange(wa_mine, "tp", 1)
    gv_other = exchange(gv_same, "grp", 1)
    wc_y = exchange(wc_x, "grp", 1)
    wc_xc = exchange(wc_x, "tp", 1)
    wa_xc = exchange(wa_x, "tp", 1)
    wc_yc = exchange(wc_y, "tp", 1)
    x_own, x_pair = assemble(mine_own, mine_pair, x_got, x_other)

    keep, sent = project_qkv(x_own, x_pair, own_qkv, qkv_same, qkv_other, off)
    got = exchange(sent, "sp", 2)
    glu_keep, glu_sent = project_glu(
        x_own, x_pair, (own_gv, own_gg), (gv_same, gv_other, gg_pair), sent
    )
    glu_got = exchange(glu_sent, "sp", 2)
    q, kv_mine = sum_qkv(keep, got, off, glu_sent)
    kv_pair = exchange(kv_mine, "sp", 1)
    near = near_attention(q, kv_mine, kv_mine)
    attended, att_sent, own_log = attention(q, kv_pair, head_gain, near, kv_mine)
    att_got = exchange(att_sent, "sp", 2)
    gated, tail = gate(glu_keep, glu_got, -(-conv_taps.shape[0] // 16) * 16, att_sent)
    before = from_behind(tail, "sp", 1)
    act_mine, log_mass = conv(gated, before, conv_taps, attended, att_got, own_log)
    act_x = exchange(act_mine, "tp", 2)
    act_core = exchange(act_mine, "tp", 1)
    act = (act_mine, act_core, act_x, exchange(act_x, "tp", 1))
    wa = (wa_mine, wa_core, wa_x, wa_xc)
    wc = (w_out_conv, wc_core, wc_x, wc_y, wc_xc, wc_yc)
    mixed = finish(act, wa, wc, out_gain)
    return (mixed, log_mass)


def gathered(
    tokens,
    norm_gain,
    w_query,
    w_key,
    w_value,
    w_glu_value,
    w_glu_gate,
    key_offset,
    head_gain,
    conv_taps,
    channel_gain,
    channel_bias,
    w_out_attn,
    w_out_conv,
    out_gain,
):
    row_count = tokens.shape[0]
    hd = head_gain.shape[1]
    channels = conv_taps.shape[1] * lax.axis_size("tp")
    normed = row_norm(tokens.astype(jnp.float32), norm_gain).astype(jnp.bfloat16)
    weights_in = (w_query, w_key, w_value, w_glu_value, w_glu_gate)
    pieces = (
        lax.all_gather(weights_in[0], "sp", axis=0, tiled=True),
        lax.all_gather(weights_in[1], "sp", axis=0, tiled=True),
        lax.all_gather(weights_in[2], "sp", axis=0, tiled=True),
        lax.all_gather(weights_in[3], "sp", axis=0, tiled=True),
        lax.all_gather(weights_in[4], "sp", axis=0, tiled=True),
    )
    projected = tuple(
        (jnp.dot(normed, shard_piece, preferred_element_type=jnp.float32) for shard_piece in pieces)
    )
    query, key_rows, value_rows, glu_value, glu_gate = [
        summed.astype(jnp.bfloat16) for summed in projected
    ]
    kv_local = key_rows.shape[1] // hd
    group_size = query.shape[1] // key_rows.shape[1]
    heads_local = kv_local * group_size
    all_keys, all_values, all_offsets = (
        lax.all_gather(key_rows, "sp", axis=0, tiled=True),
        lax.all_gather(value_rows, "sp", axis=0, tiled=True),
        lax.all_gather(key_offset, "sp", axis=0, tiled=True),
    )
    sequence_length_total = all_keys.shape[0]
    shard_count = lax.axis_size("sp")
    per_block = 1
    while (
        per_block * 2 <= shard_count
        and shard_count % (per_block * 2) == 0
        and (per_block * 2 * row_count <= 1024)
    ):
        per_block = per_block * 2
    span_len = per_block * row_count
    query_heads = query.reshape(row_count, kv_local, group_size, hd)
    key_heads = all_keys.reshape(sequence_length_total, kv_local, hd)
    value_heads = all_values.reshape(sequence_length_total, kv_local, hd)
    my_index = lax.axis_index("sp")
    query_pos = my_index * row_count + jnp.arange(row_count, dtype=jnp.int32)
    last_block = my_index // per_block
    zeros_mix = jnp.zeros((kv_local, group_size, row_count, hd), jnp.float32)
    zeros_row = jnp.zeros((kv_local, group_size, row_count), jnp.float32)

    def sweep(turn_index, carry):
        head_mix, mass_sum, carried = carry
        first_key = (last_block - turn_index) * span_len
        key_block = lax.dynamic_slice_in_dim(key_heads, first_key, span_len, 0)
        value_block = lax.dynamic_slice_in_dim(value_heads, first_key, span_len, 0)
        offset_block = lax.dynamic_slice_in_dim(all_offsets, first_key, span_len, 0).astype(
            jnp.float32
        )
        offset_block = offset_block.T.reshape(kv_local, group_size, 1, span_len)
        scores = (
            jnp.einsum("qhgd,khd->hgqk", query_heads, key_block, preferred_element_type=jnp.float32)
            * hd ** (-0.5)
            + offset_block
        )
        key_pos = first_key + jnp.arange(span_len, dtype=jnp.int32)
        allowed = key_pos[None, :] <= query_pos[:, None]
        log_not = jnp.where(allowed, jax.nn.log_sigmoid(-scores), 0.0)
        later = lax.cumsum(log_not, axis=3, reverse=True) - log_not + carried[..., None]
        weights = jnp.where(allowed, jnp.exp(jax.nn.log_sigmoid(scores) + later), 0.0)
        head_mix = head_mix + jnp.einsum(
            "hgqk,khd->hgqd",
            weights.astype(jnp.bfloat16),
            value_block,
            preferred_element_type=jnp.float32,
        )
        return (head_mix, mass_sum + jnp.sum(weights, axis=3), carried + jnp.sum(log_not, axis=3))

    head_mix, mass_sum, _ = lax.fori_loop(
        0, last_block + 1, sweep, (zeros_mix, zeros_row, zeros_row)
    )
    log_mass = jnp.log(mass_sum).reshape(heads_local, row_count)
    head_rows = head_mix.transpose(2, 0, 1, 3).reshape(row_count, heads_local, hd)
    attended = (
        row_norm(head_rows, head_gain).astype(jnp.bfloat16).reshape(row_count, heads_local * hd)
    )
    gated = (glu_value.astype(jnp.float32) * jax.nn.sigmoid(glu_gate.astype(jnp.float32))).astype(
        jnp.bfloat16
    )
    reach_len = conv_taps.shape[0] - 1
    before = from_behind(gated[row_count - reach_len :], "sp", 1)
    padded = jnp.concatenate([before, gated], axis=0).astype(jnp.float32)
    conv_out = jnp.zeros(gated.shape, jnp.float32)
    for tap_index in range(conv_taps.shape[0]):
        conv_out = conv_out + conv_taps[tap_index] * padded[tap_index : tap_index + row_count]
    total_sum, total_squares = lax.psum(
        (jnp.sum(conv_out, axis=1), jnp.sum(conv_out * conv_out, axis=1)), "tp"
    )
    chan_mean = (total_sum / channels)[:, None]
    spread = (total_squares / channels)[:, None] - chan_mean * chan_mean
    centered = conv_out - chan_mean
    channel_out = jax.nn.silu(
        centered * lax.rsqrt(spread + norm_eps) * channel_gain + channel_bias
    ).astype(jnp.bfloat16)
    share = lax.psum_scatter(
        jnp.dot(attended, w_out_attn, preferred_element_type=jnp.float32)
        + jnp.dot(channel_out, w_out_conv, preferred_element_type=jnp.float32),
        "tp",
        scatter_dimension=0,
        tiled=True,
    )
    mixed = lax.all_gather(row_norm(share, out_gain).astype(jnp.bfloat16), "tp", axis=0, tiled=True)
    return (mixed, log_mass)


def solution(mesh):
    in_specs = (
        P(("grp", "sp"), None),
        P(),
        P("sp", "tp"),
        P("sp", "tp"),
        P("sp", "tp"),
        P("sp", "tp"),
        P("sp", "tp"),
        P(("grp", "sp"), "tp"),
        P("tp", None),
        P(None, "tp"),
        P("tp"),
        P("tp"),
        P("tp", None),
        P("tp", None),
        P(),
    )
    out_specs = (P(("grp", "sp"), None), P("tp", ("grp", "sp")))
    small = mesh.shape["sp"] == 4 and mesh.shape["tp"] == 4 and mesh.shape["grp"] == 2
    local = paired if small else gathered
    return jax.shard_map(local, mesh=mesh, in_specs=in_specs, out_specs=out_specs, check_vma=False)
```

```python
import jax
import jax.numpy as jnp
from jax import lax
from jax.experimental import pallas as pl
from jax.experimental.pallas import tpu as pltpu
from jax.sharding import PartitionSpec as P

norm_eps = 1e-06
BF16 = jnp.bfloat16
F32 = jnp.float32


def exchange(value, axis, bit):
    count = lax.axis_size(axis)
    return lax.ppermute(value, axis, [(s, s ^ bit) for s in range(count)])


def from_behind(value, axis, steps):
    count = lax.axis_size(axis)
    initial, last = (max(0, -steps), min(count, count - steps))
    return lax.ppermute(value, axis, [(source, source + steps) for source in range(initial, last)])


def row_norm(values_in, gain_vec):
    squares = jnp.mean(values_in * values_in, axis=-1, keepdims=True)
    return values_in * lax.rsqrt(squares + norm_eps) * gain_vec


def dot_f32(a, b, dims=((1,), (0,))):
    return lax.dot_general(a, b, (dims, ((), ())), preferred_element_type=F32)


def params(limit=16):
    return pltpu.CompilerParams(vmem_limit_bytes=limit * 1024 * 1024)


VM = pl.BlockSpec(memory_space=pltpu.VMEM)
ANY = pl.BlockSpec(memory_space=pl.ANY)
HBM = pl.BlockSpec(memory_space=pltpu.HBM)


def shape(dims, dtype=BF16):
    return jax.ShapeDtypeStruct(dims, dtype)


def cost(flops, moved):
    return pl.CostEstimate(flops=flops, bytes_accessed=moved, transcendentals=0)


def in_hbm(*values):
    return [pltpu.with_memory_space_constraint(v, pltpu.HBM) for v in values]


def pack_qkv_kernel(wq, wk, wv, wc, all_ref, send_ref, wc_ref, sems):
    part, width = send_ref.shape[0], wq.shape[1]
    group = lax.axis_index("grp")
    mine = pl.ds(pl.multiple_of(group * part, part), part)
    columns = wc_ref.shape[1]
    first, rest = [], []
    for n, w in enumerate((wq, wk, wv)):
        at = slice(n * width, (n + 1) * width)
        first.append(pltpu.make_async_copy(w.at[mine, :], send_ref.at[:, at], sems.at[n]))
        rest.append(pltpu.make_async_copy(w, all_ref.at[:, at], sems.at[3 + n]))
    half = wc.at[:, pl.ds(pl.multiple_of(group * columns, columns), columns)]
    rest.append(pltpu.make_async_copy(half, wc_ref, sems.at[6]))
    for copy in first + rest:
        copy.start()
    for copy in first + rest:
        copy.wait()


def pack_qkv(weights, wc):
    block, width = weights[0].shape
    return pl.pallas_call(
        pack_qkv_kernel,
        out_shape=(
            shape((block, 3 * width)),
            shape((block // 2, 3 * width)),
            shape((wc.shape[0], wc.shape[1] // 2)),
        ),
        in_specs=[HBM] * 4,
        out_specs=[VM] * 3,
        scratch_shapes=[pltpu.SemaphoreType.DMA((7,))],
        cost_estimate=cost(2_000_000, 400_000),
        compiler_params=params(),
        name="pack_qkv",
    )(*in_hbm(*weights, wc))


def norm_kernel(x_hbm, gain_hbm, send_ref, own_ref, pair_ref, x_ref, gain_ref, normed, sems):
    side, low = lax.axis_index("sp") // 2, lax.axis_index("sp") % 2
    core = lax.axis_index("tp") % 2
    block = own_ref.shape[1]
    half = 2 * block
    half_rows = send_ref.shape[0]
    copies = [
        pltpu.make_async_copy(x_hbm, x_ref, sems.at[0]),
        pltpu.make_async_copy(gain_hbm, gain_ref, sems.at[1]),
    ]
    for copy in copies:
        copy.start()
    for copy in copies:
        copy.wait()
    x = x_ref[...].astype(F32)
    squares = jnp.mean(x * x, axis=1, keepdims=True)
    normed[...] = (x * lax.rsqrt(squares + norm_eps) * gain_ref[...]).astype(BF16)
    first = pl.multiple_of(core * half_rows, half_rows)
    away = pl.multiple_of((1 - side) * half, half)
    send_ref[...] = normed[pl.ds(first, half_rows), pl.ds(away, half)]
    own_ref[...] = normed[:, pl.ds(pl.multiple_of(side * half + low * block, block), block)]
    pair_ref[...] = normed[:, pl.ds(pl.multiple_of(side * half + (1 - low) * block, block), block)]


def norm_parts(tokens, gain, block):
    rows, features = tokens.shape
    return pl.pallas_call(
        norm_kernel,
        out_shape=(shape((rows // 2, 2 * block)), shape((rows, block)), shape((rows, block))),
        in_specs=[HBM] * 2,
        out_specs=[VM] * 3,
        scratch_shapes=[
            pltpu.VMEM((rows, features), BF16),
            pltpu.VMEM((1, features), F32),
            pltpu.VMEM((rows, features), BF16),
            pltpu.SemaphoreType.DMA((2,)),
        ],
        cost_estimate=cost(2_000_000, 1_000_000),
        compiler_params=params(),
        name="norm_parts",
    )(*in_hbm(tokens, gain.reshape(1, features)))


def pack_kernel(
    gv_hbm, gg_hbm, wa_hbm, off_hbm, head_hbm, gain_hbm, bias_hbm, *refs
):
    gv_ref, gv_send, gg_ref, out_ref, off_ref, head_ref, gain_ref, bias_ref, sems = refs
    cw, aw = gv_hbm.shape[1], wa_hbm.shape[0]
    part = gv_send.shape[0]
    mine = pl.ds(pl.multiple_of(lax.axis_index("grp") * part, part), part)
    pairs = (
        (gain_hbm, gain_ref),
        (bias_hbm, bias_ref),
        (gv_hbm.at[mine, :], gv_send),
        (gg_hbm, gg_ref),
        (wa_hbm, out_ref.at[:aw, :]),
        (off_hbm, off_ref),
        (head_hbm, head_ref),
        (gv_hbm, gv_ref),
    )
    copies = [pltpu.make_async_copy(a, b, sems.at[n]) for n, (a, b) in enumerate(pairs)]
    for copy in copies:
        copy.start()
    for copy in copies[:2]:
        copy.wait()
    extra = out_ref.shape[0] - aw
    for n, ref in enumerate((gain_ref, bias_ref)):
        rest = ref[...]
        for piece in range(3):
            part = rest.astype(BF16)
            rest = rest - part.astype(F32)
            first = (3 * n + piece) * cw
            out_ref[aw:, first : first + cw] = jnp.broadcast_to(part, (extra, cw))
    for copy in copies[2:]:
        copy.wait()


def pack(gv, gg, wa, off, head_gain, gain, bias):
    block, cw = gv.shape
    aw, width = wa.shape
    return pl.pallas_call(
        pack_kernel,
        out_shape=(
            shape((block, cw)),
            shape((block // 2, cw)),
            shape((block, cw)),
            shape((aw + 16, width)),
            shape(off.shape),
            shape(head_gain.shape, F32),
        ),
        in_specs=[HBM] * 7,
        out_specs=[VM] * 6,
        scratch_shapes=[
            pltpu.VMEM((1, cw), F32),
            pltpu.VMEM((1, cw), F32),
            pltpu.SemaphoreType.DMA((8,)),
        ],
        cost_estimate=cost(2_000_000, 2_000_000),
        compiler_params=params(),
        name="pack",
    )(*in_hbm(gv, gg, wa, off, head_gain, gain.reshape(1, cw), bias.reshape(1, cw)))


def assemble_kernel(own_ref, pair_ref, got_ref, other_ref, own_out, pair_out):
    low = lax.axis_index("sp") % 2
    core = lax.axis_index("tp") % 2
    rows, block = own_ref.shape
    half = got_ref.shape[0]
    own_out[:rows, :] = own_ref[...]
    pair_out[:rows, :] = pair_ref[...]
    own_at = pl.multiple_of(low * block, block)
    pair_at = pl.multiple_of((1 - low) * block, block)
    for part, at in ((got_ref, core), (other_ref, 1 - core)):
        first = pl.multiple_of(rows + at * half, half)
        own_out[pl.ds(first, half), :] = part[:, pl.ds(own_at, block)]
        pair_out[pl.ds(first, half), :] = part[:, pl.ds(pair_at, block)]


def assemble(own, pair, got, other):
    rows, block = own.shape
    return pl.pallas_call(
        assemble_kernel,
        out_shape=(shape((2 * rows, block)),) * 2,
        in_specs=[VM] * 4,
        out_specs=[VM] * 2,
        cost_estimate=cost(2_000_000, 1_000_000),
        compiler_params=params(),
        name="assemble",
    )(own, pair, got, other)


def far_dot(x_pair, same, other):
    part = same.shape[0]
    group = lax.axis_index("grp")
    near = x_pair[:, pl.ds(pl.multiple_of(group * part, part), part)]
    rest = x_pair[:, pl.ds(pl.multiple_of((1 - group) * part, part), part)]
    return dot_f32(near, same[...]) + dot_f32(rest, other[...])


def qkv_kernel(x_own, x_pair, own, same, other, off_ref, keep_ref, send_ref):
    rows = x_own.shape[0] // 2
    width = send_ref.shape[1]
    total = dot_f32(x_own[...], own[...]) + far_dot(x_pair, same, other)
    keep_ref[...] = total
    for n in range(3):
        part = total[:, n * width : (n + 1) * width].astype(BF16)
        first = 4 * rows if n == 0 else 2 * (n - 1) * rows
        send_ref[first : first + rows, :] = part[rows:]
        if n > 0:
            send_ref[first + rows : first + 2 * rows, :] = part[:rows]
    send_ref[5 * rows :, :] = jnp.zeros((send_ref.shape[0] - 5 * rows, width), BF16)
    send_ref[5 * rows : 5 * rows + off_ref.shape[0], :] = off_ref[...]


def project_qkv(x_own, x_pair, own, same, other, off):
    rows, width = x_own.shape[0], own.shape[1] // 3
    return pl.pallas_call(
        qkv_kernel,
        out_shape=(shape((rows, 3 * width), F32), shape((5 * rows // 2 + 16, width))),
        in_specs=[VM] * 6,
        out_specs=[VM] * 2,
        cost_estimate=cost(200_000_000, 1_000_000),
        compiler_params=params(),
        name="project_qkv",
    )(x_own, x_pair, own, same, other, off)


def sum_kernel(keep_ref, got_ref, sent_ref, after, q_ref, out_ref):
    rows, width = q_ref.shape

    def got(n):
        return got_ref[n * rows : (n + 1) * rows, :].astype(F32)

    q_ref[...] = (keep_ref[:rows, :width] + got(4)).astype(BF16)
    for n in range(4):
        at = slice((1 + n // 2) * width, (2 + n // 2) * width)
        part = keep_ref[(n % 2) * rows : (n % 2 + 1) * rows, at]
        out_ref[n * rows : (n + 1) * rows, :] = (part + got(n)).astype(BF16)
    first = 5 * rows
    out_ref[4 * rows :, :] = jnp.concatenate([sent_ref[first : first + 8, :], got_ref[first : first + 8, :]])


def sum_qkv(keep, got, sent, after):
    rows, width = keep.shape[0] // 2, got.shape[1]
    return pl.pallas_call(
        sum_kernel,
        out_shape=(shape((rows, width)), shape((4 * rows + 16, width))),
        in_specs=[VM] * 3 + [ANY],
        out_specs=[VM] * 2,
        cost_estimate=cost(1_000_000, 1_000_000),
        compiler_params=params(),
        name="sum_qkv",
    )(keep, got, sent, after)


def glu_kernel(x_own, x_pair, gv, gg, gv_same, gv_other, gg_pair, after, keep_ref, send_ref):
    rows = x_own.shape[0] // 2
    cw = gv.shape[1]
    for n in range(2):
        own = (gv, gg)[n]
        far = far_dot(x_pair, gv_same, gv_other) if n == 0 else dot_f32(x_pair[...], gg_pair[...])
        total = dot_f32(x_own[...], own[...]) + far
        at = slice(n * cw, (n + 1) * cw)
        keep_ref[:, at] = total[:rows]
        send_ref[:, at] = total[rows:].astype(BF16)


def project_glu(x_own, x_pair, own, pair, after):
    rows, width = x_own.shape[0] // 2, 2 * own[0].shape[1]
    return pl.pallas_call(
        glu_kernel,
        out_shape=(shape((rows, width), F32), shape((rows, width))),
        in_specs=[VM] * 7 + [ANY],
        out_specs=[VM] * 2,
        cost_estimate=cost(270_000_000, 1_000_000),
        compiler_params=params(),
        name="project_glu",
    )(x_own, x_pair, *own, *pair, after)


def gate_kernel(keep_ref, got_ref, gated_ref, tail_ref):
    rows, cw = gated_ref.shape
    glu = keep_ref[...] + got_ref[...].astype(F32)
    value = glu[:, :cw].astype(BF16).astype(F32)
    gate = glu[:, cw:].astype(BF16).astype(F32)
    gated = (value * jax.nn.sigmoid(gate)).astype(BF16)
    gated_ref[...] = gated
    tail_ref[...] = gated[rows - tail_ref.shape[0] :]


def gate(keep, got, tail):
    rows, cw = keep.shape[0], keep.shape[1] // 2
    return pl.pallas_call(
        gate_kernel,
        out_shape=(shape((rows, cw)), shape((tail, cw))),
        in_specs=[VM] * 2,
        out_specs=[VM] * 2,
        cost_estimate=cost(2_000_000, 500_000),
        compiler_params=params(),
        name="gate",
    )(keep, got)


def conv_kernel(gated_ref, before_ref, taps_ref, att_ref, act_ref, padded):
    rows, aw = att_ref.shape
    tail = before_ref.shape[0]
    taps = taps_ref.shape[0]
    padded[:tail, :] = before_ref[...].astype(F32)
    padded[tail:, :] = gated_ref[...].astype(F32)
    total = None
    for tap in range(taps):
        first = tail - (taps - 1) + tap
        part = taps_ref[tap : tap + 1, :] * padded[first : first + rows, :]
        total = part if total is None else total + part
    act_ref[:, :aw] = att_ref[...]
    act_ref[:, aw:] = total.astype(BF16)


def conv(gated, before, taps, attended):
    rows, cw = gated.shape
    return pl.pallas_call(
        conv_kernel,
        out_shape=shape((rows, attended.shape[1] + cw)),
        in_specs=[VM] * 4,
        out_specs=VM,
        scratch_shapes=[pltpu.VMEM((rows + before.shape[0], cw), F32)],
        cost_estimate=cost(20_000_000, 500_000),
        compiler_params=params(),
        name="conv",
    )(gated, before, taps, attended)


def suffix_matrix(keys):
    before = lax.broadcasted_iota(jnp.int32, (2 * keys, 2 * keys), 0) % keys
    column = lax.broadcasted_iota(jnp.int32, (2 * keys, 2 * keys), 1)
    return jnp.where((column >= keys) | (before > column), 1.0, 0.0).astype(BF16)


def stick_block(q, k, v, off, hd, suffix, carry, diagonal):
    rows, width = q.shape
    keys = k.shape[0]
    lane = lax.broadcasted_iota(jnp.int32, (rows, width), 1) // hd
    offsets = off.astype(F32)
    weights, totals, values = [], [], []
    for h in range(width // hd):
        qh = jnp.where(lane == h, q, jnp.zeros_like(q))
        s = dot_f32(qh, k, ((1,), (1,))) * hd ** (-0.5) + offsets[h : h + 1, :]
        soft = jnp.maximum(s, 0.0) + jnp.log(1.0 + jnp.exp(-jnp.abs(s)))
        log_not = -soft
        if diagonal:
            allowed = lax.broadcasted_iota(jnp.int32, (rows, keys), 1) <= lax.broadcasted_iota(
                jnp.int32, (rows, keys), 0
            )
            log_not = jnp.where(allowed, log_not, 0.0)
        high = log_not.astype(BF16)
        low = (log_not - high.astype(F32)).astype(BF16)
        sums = dot_f32(jnp.concatenate([high, low], axis=1), suffix)
        later = sums[:, :keys]
        if carry is not None:
            later = later + carry[h]
        w = jnp.exp(s - soft + later)
        if diagonal:
            w = jnp.where(allowed, w, 0.0)
        weights.append(w)
        totals.append(sums[:, keys:])
        values.append(jnp.where(lane == h, v, jnp.zeros_like(v)))
    mix = dot_f32(
        jnp.concatenate([w.astype(BF16) for w in weights], axis=1), jnp.concatenate(values, axis=0)
    )
    return mix, weights, totals


def near_kernel(q_ref, mine_ref, gain_ref, after, mix_ref, mass_ref, carry_ref):
    rows = q_ref.shape[0]
    heads, hd = gain_ref.shape
    suffix = suffix_matrix(rows)
    for n in range(2):
        k = mine_ref[n * rows : (n + 1) * rows, :]
        v = mine_ref[(2 + n) * rows : (3 + n) * rows, :]
        off = mine_ref[4 * rows + 8 * n : 4 * rows + 8 * n + 8, :]
        mix, weights, totals = stick_block(q_ref[...], k, v, off, hd, suffix, None, n == 0)
        mix_ref[n] = mix
        for h in range(heads):
            mass_ref[n * heads + h] = weights[h]
            carry_ref[n * heads + h] = totals[h]


def near_attention(q, mine, head_gain, after):
    rows, width = q.shape
    heads = head_gain.shape[0]
    return pl.pallas_call(
        near_kernel,
        out_shape=(
            shape((2, rows, width), F32),
            shape((2 * heads, rows, rows), F32),
            shape((2 * heads, rows, rows), F32),
        ),
        in_specs=[VM] * 3 + [ANY],
        out_specs=[VM] * 3,
        cost_estimate=cost(200_000_000, 1_000_000),
        compiler_params=params(),
        name="near_attention",
    )(q, mine, head_gain, after)


def attention_kernel(q_ref, pair_ref, gain_ref, mix_ref, mass_ref, carry_ref, after, out_ref, log_ref, acc, mass, carry):
    me = lax.axis_index("sp")
    rows, width = q_ref.shape
    heads, hd = gain_ref.shape
    lane = lax.broadcasted_iota(jnp.int32, (rows, width), 1) // hd
    suffix = suffix_matrix(rows)
    acc[...] = mix_ref[0]
    for h in range(heads):
        mass[h] = mass_ref[h]
        carry[h] = carry_ref[h]

    def earlier(t, _):
        slot = jnp.bitwise_xor(me - t, me)

        @pl.when(slot == 2)
        def _():
            scale = jnp.zeros_like(acc)
            for h in range(heads):
                left = jnp.exp(carry[h])
                mass[h] = mass[h] + left * mass_ref[heads + h]
                scale = jnp.where(lane == h, left, scale)
                carry[h] = carry[h] + carry_ref[heads + h]
            acc[...] = acc[...] + scale * mix_ref[1]

        @pl.when(slot != 2)
        def _():
            n = slot // 2
            k = pair_ref[pl.ds(pl.multiple_of(n * rows, rows), rows), :]
            v = pair_ref[pl.ds(pl.multiple_of((2 + n) * rows, rows), rows), :]
            off = jnp.where(
                n == 0,
                pair_ref[4 * rows : 4 * rows + 8, :].astype(F32),
                pair_ref[4 * rows + 8 : 4 * rows + 16, :].astype(F32),
            )
            so_far = [carry[h] for h in range(heads)]
            mix, weights, totals = stick_block(q_ref[...], k, v, off, hd, suffix, so_far, False)
            acc[...] = acc[...] + mix
            for h in range(heads):
                mass[h] = mass[h] + weights[h]
                carry[h] = so_far[h] + totals[h]

        return 0

    lax.fori_loop(1, me + 1, earlier, 0)
    mixed = acc[...]
    squares = mixed * mixed
    inverse = jnp.zeros_like(mixed)
    for h in range(heads):
        mean = jnp.sum(jnp.where(lane == h, squares, 0.0), axis=1, keepdims=True) / hd
        inverse = jnp.where(lane == h, lax.rsqrt(mean + norm_eps), inverse)
    gain = jnp.concatenate([gain_ref[h : h + 1, :] for h in range(heads)], axis=1)
    out_ref[...] = (mixed * inverse * gain).astype(BF16)
    for h in range(heads):
        log_ref[h : h + 1, :] = jnp.log(jnp.sum(jnp.transpose(mass[h]), axis=0, keepdims=True))


def attention(q, pair, head_gain, near, after):
    rows, width = q.shape
    heads = head_gain.shape[0]
    return pl.pallas_call(
        attention_kernel,
        out_shape=(shape((rows, width)), shape((heads, rows), F32)),
        in_specs=[VM] * 6 + [ANY],
        out_specs=[VM] * 2,
        scratch_shapes=[
            pltpu.VMEM((rows, width), F32),
            pltpu.VMEM((heads, rows, rows), F32),
            pltpu.VMEM((heads, rows, rows), F32),
        ],
        cost_estimate=cost(400_000_000, 1_000_000),
        compiler_params=params(),
        name="stick_attention",
    )(q, pair, head_gain, *near, after)


def final_kernel(*refs):
    act, wa, wc, gain_ref, out_ref = refs[:4], refs[4:8], refs[8:14], refs[14], refs[15]
    cw = wc[0].shape[0]
    aw = act[0].shape[1] - cw
    convs = [c[:, aw:].astype(F32) for c in act]
    mean = sum(jnp.sum(v, axis=1, keepdims=True) for v in convs) / (4 * cw)
    centered = [v - mean for v in convs]
    spread = sum(jnp.sum(v * v, axis=1, keepdims=True) for v in centered) / (4 * cw)
    inverse = lax.rsqrt(spread + norm_eps)
    total = None
    ys = []
    for slot in range(4):
        pieces = [wa[slot][aw : aw + 1, n * cw : (n + 1) * cw].astype(F32) for n in range(6)]
        gain = pieces[0] + pieces[1] + pieces[2]
        bias = pieces[3] + pieces[4] + pieces[5]
        y = centered[slot] * inverse * gain + bias
        y = (y * jax.nn.sigmoid(y)).astype(BF16)
        part = dot_f32(act[slot][:, :aw], wa[slot][:aw, :])
        if slot < 2:
            part = part + dot_f32(y, wc[slot][...])
        total = part if total is None else total + part
        ys.append(y)
    same = dot_f32(ys[2], wc[2][...]) + dot_f32(ys[3], wc[4][...])
    other = dot_f32(ys[2], wc[3][...]) + dot_f32(ys[3], wc[5][...])
    swap = lax.axis_index("grp") == 1
    total = total + jnp.concatenate([jnp.where(swap, other, same), jnp.where(swap, same, other)], axis=1)
    squares = jnp.mean(total * total, axis=1, keepdims=True)
    out_ref[...] = (total * lax.rsqrt(squares + norm_eps) * gain_ref[...]).astype(BF16)


def finish(act, wa, wc, out_gain):
    rows, width = act[0].shape[0], wa[0].shape[1]
    return pl.pallas_call(
        final_kernel,
        out_shape=shape((rows, width)),
        in_specs=[VM] * 15,
        out_specs=VM,
        cost_estimate=cost(800_000_000, 7_000_000),
        compiler_params=params(32),
        name="finish_rows",
    )(*act, *wa, *wc, out_gain.reshape(1, width))


def paired(
    tokens,
    norm_gain,
    w_query,
    w_key,
    w_value,
    w_glu_value,
    w_glu_gate,
    key_offset,
    head_gain,
    conv_taps,
    channel_gain,
    channel_bias,
    w_out_attn,
    w_out_conv,
    out_gain,
):
    own_qkv, half_qkv, wc_half = pack_qkv((w_query, w_key, w_value), w_out_conv)
    qkv_same = exchange(half_qkv, "sp", 1)
    wc_x = exchange(wc_half, "tp", 2)
    wc_y = exchange(wc_x, "grp", 1)
    wc_yc = exchange(wc_y, "tp", 1)
    x_send, mine_own, mine_pair = norm_parts(tokens, norm_gain, w_query.shape[0])
    x_got = exchange(x_send, "sp", 2)
    own_gv, half_gv, own_gg, wa_mine, off, head_rows = pack(
        w_glu_value, w_glu_gate, w_out_attn, key_offset.T, head_gain, channel_gain, channel_bias
    )
    qkv_same, half_gv = lax.optimization_barrier((qkv_same, half_gv))
    gv_same = exchange(half_gv, "sp", 1)
    gg_pair = exchange(own_gg, "sp", 1)
    gv_other = exchange(gv_same, "grp", 1)
    qkv_other = exchange(qkv_same, "grp", 1)
    x_other = exchange(x_got, "tp", 1)
    wa_x = exchange(wa_mine, "tp", 2)
    wc_core = exchange(w_out_conv, "tp", 1)
    wa_core = exchange(wa_mine, "tp", 1)
    wc_xc = exchange(wc_x, "tp", 1)
    wa_xc = exchange(wa_x, "tp", 1)
    x_own, x_pair = assemble(mine_own, mine_pair, x_got, x_other)

    keep, sent = project_qkv(x_own, x_pair, own_qkv, qkv_same, qkv_other, off)
    got = exchange(sent, "sp", 2)
    glu_keep, glu_sent = project_glu(
        x_own, x_pair, (own_gv, own_gg), (gv_same, gv_other, gg_pair), sent
    )
    glu_got = exchange(glu_sent, "sp", 2)
    q, mine_two = sum_qkv(keep, got, sent, glu_sent)
    pair_two = exchange(mine_two, "sp", 1)
    near = near_attention(q, mine_two, head_rows, mine_two)
    gated, tail = gate(glu_keep, glu_got, -(-conv_taps.shape[0] // 16) * 16)
    before = from_behind(tail, "sp", 1)
    attended, log_mass = attention(q, pair_two, head_rows, near, tail)
    act_mine = conv(gated, before, conv_taps, attended)
    act_x = exchange(act_mine, "tp", 2)
    act_core = exchange(act_mine, "tp", 1)
    act = (act_mine, act_core, act_x, exchange(act_x, "tp", 1))
    wa = (wa_mine, wa_core, wa_x, wa_xc)
    wc = (w_out_conv, wc_core, wc_x, wc_y, wc_xc, wc_yc)
    mixed = finish(act, wa, wc, out_gain)
    return (mixed, log_mass)


def gathered(
    tokens,
    norm_gain,
    w_query,
    w_key,
    w_value,
    w_glu_value,
    w_glu_gate,
    key_offset,
    head_gain,
    conv_taps,
    channel_gain,
    channel_bias,
    w_out_attn,
    w_out_conv,
    out_gain,
):
    row_count = tokens.shape[0]
    hd = head_gain.shape[1]
    channels = conv_taps.shape[1] * lax.axis_size("tp")
    normed = row_norm(tokens.astype(jnp.float32), norm_gain).astype(jnp.bfloat16)
    weights_in = (w_query, w_key, w_value, w_glu_value, w_glu_gate)
    pieces = (
        lax.all_gather(weights_in[0], "sp", axis=0, tiled=True),
        lax.all_gather(weights_in[1], "sp", axis=0, tiled=True),
        lax.all_gather(weights_in[2], "sp", axis=0, tiled=True),
        lax.all_gather(weights_in[3], "sp", axis=0, tiled=True),
        lax.all_gather(weights_in[4], "sp", axis=0, tiled=True),
    )
    projected = tuple(
        (jnp.dot(normed, shard_piece, preferred_element_type=jnp.float32) for shard_piece in pieces)
    )
    query, key_rows, value_rows, glu_value, glu_gate = [
        summed.astype(jnp.bfloat16) for summed in projected
    ]
    kv_local = key_rows.shape[1] // hd
    group_size = query.shape[1] // key_rows.shape[1]
    heads_local = kv_local * group_size
    all_keys, all_values, all_offsets = (
        lax.all_gather(key_rows, "sp", axis=0, tiled=True),
        lax.all_gather(value_rows, "sp", axis=0, tiled=True),
        lax.all_gather(key_offset, "sp", axis=0, tiled=True),
    )
    sequence_length_total = all_keys.shape[0]
    shard_count = lax.axis_size("sp")
    per_block = 1
    while (
        per_block * 2 <= shard_count
        and shard_count % (per_block * 2) == 0
        and (per_block * 2 * row_count <= 1024)
    ):
        per_block = per_block * 2
    span_len = per_block * row_count
    query_heads = query.reshape(row_count, kv_local, group_size, hd)
    key_heads = all_keys.reshape(sequence_length_total, kv_local, hd)
    value_heads = all_values.reshape(sequence_length_total, kv_local, hd)
    my_index = lax.axis_index("sp")
    query_pos = my_index * row_count + jnp.arange(row_count, dtype=jnp.int32)
    last_block = my_index // per_block
    zeros_mix = jnp.zeros((kv_local, group_size, row_count, hd), jnp.float32)
    zeros_row = jnp.zeros((kv_local, group_size, row_count), jnp.float32)

    def sweep(turn_index, carry):
        head_mix, mass_sum, carried = carry
        first_key = (last_block - turn_index) * span_len
        key_block = lax.dynamic_slice_in_dim(key_heads, first_key, span_len, 0)
        value_block = lax.dynamic_slice_in_dim(value_heads, first_key, span_len, 0)
        offset_block = lax.dynamic_slice_in_dim(all_offsets, first_key, span_len, 0).astype(
            jnp.float32
        )
        offset_block = offset_block.T.reshape(kv_local, group_size, 1, span_len)
        scores = (
            jnp.einsum("qhgd,khd->hgqk", query_heads, key_block, preferred_element_type=jnp.float32)
            * hd ** (-0.5)
            + offset_block
        )
        key_pos = first_key + jnp.arange(span_len, dtype=jnp.int32)
        allowed = key_pos[None, :] <= query_pos[:, None]
        log_not = jnp.where(allowed, jax.nn.log_sigmoid(-scores), 0.0)
        later = lax.cumsum(log_not, axis=3, reverse=True) - log_not + carried[..., None]
        weights = jnp.where(allowed, jnp.exp(jax.nn.log_sigmoid(scores) + later), 0.0)
        head_mix = head_mix + jnp.einsum(
            "hgqk,khd->hgqd",
            weights.astype(jnp.bfloat16),
            value_block,
            preferred_element_type=jnp.float32,
        )
        return (head_mix, mass_sum + jnp.sum(weights, axis=3), carried + jnp.sum(log_not, axis=3))

    head_mix, mass_sum, _ = lax.fori_loop(
        0, last_block + 1, sweep, (zeros_mix, zeros_row, zeros_row)
    )
    log_mass = jnp.log(mass_sum).reshape(heads_local, row_count)
    head_rows = head_mix.transpose(2, 0, 1, 3).reshape(row_count, heads_local, hd)
    attended = (
        row_norm(head_rows, head_gain).astype(jnp.bfloat16).reshape(row_count, heads_local * hd)
    )
    gated = (glu_value.astype(jnp.float32) * jax.nn.sigmoid(glu_gate.astype(jnp.float32))).astype(
        jnp.bfloat16
    )
    reach_len = conv_taps.shape[0] - 1
    before = from_behind(gated[row_count - reach_len :], "sp", 1)
    padded = jnp.concatenate([before, gated], axis=0).astype(jnp.float32)
    conv_out = jnp.zeros(gated.shape, jnp.float32)
    for tap_index in range(conv_taps.shape[0]):
        conv_out = conv_out + conv_taps[tap_index] * padded[tap_index : tap_index + row_count]
    total_sum, total_squares = lax.psum(
        (jnp.sum(conv_out, axis=1), jnp.sum(conv_out * conv_out, axis=1)), "tp"
    )
    chan_mean = (total_sum / channels)[:, None]
    spread = (total_squares / channels)[:, None] - chan_mean * chan_mean
    centered = conv_out - chan_mean
    channel_out = jax.nn.silu(
        centered * lax.rsqrt(spread + norm_eps) * channel_gain + channel_bias
    ).astype(jnp.bfloat16)
    share = lax.psum_scatter(
        jnp.dot(attended, w_out_attn, preferred_element_type=jnp.float32)
        + jnp.dot(channel_out, w_out_conv, preferred_element_type=jnp.float32),
        "tp",
        scatter_dimension=0,
        tiled=True,
    )
    mixed = lax.all_gather(row_norm(share, out_gain).astype(jnp.bfloat16), "tp", axis=0, tiled=True)
    return (mixed, log_mass)


def solution(mesh):
    in_specs = (
        P(("grp", "sp"), None),
        P(),
        P("sp", "tp"),
        P("sp", "tp"),
        P("sp", "tp"),
        P("sp", "tp"),
        P("sp", "tp"),
        P(("grp", "sp"), "tp"),
        P("tp", None),
        P(None, "tp"),
        P("tp"),
        P("tp"),
        P("tp", None),
        P("tp", None),
        P(),
    )
    out_specs = (P(("grp", "sp"), None), P("tp", ("grp", "sp")))
    small = mesh.shape["sp"] == 4 and mesh.shape["tp"] == 4 and mesh.shape["grp"] == 2
    local = paired if small else gathered
    return jax.shard_map(local, mesh=mesh, in_specs=in_specs, out_specs=out_specs, check_vma=False)
```

```python
import jax
import jax.numpy as jnp
from jax import lax
from jax.experimental import pallas as pl
from jax.experimental.pallas import tpu as pltpu
from jax.sharding import PartitionSpec as P

norm_eps = 1e-06
BF16 = jnp.bfloat16
F32 = jnp.float32


def exchange(value, axis, bit):
    count = lax.axis_size(axis)
    return lax.ppermute(value, axis, [(s, s ^ bit) for s in range(count)])


def from_behind(value, axis, steps):
    count = lax.axis_size(axis)
    initial, last = (max(0, -steps), min(count, count - steps))
    return lax.ppermute(value, axis, [(source, source + steps) for source in range(initial, last)])


def row_norm(values_in, gain_vec):
    squares = jnp.mean(values_in * values_in, axis=-1, keepdims=True)
    return values_in * lax.rsqrt(squares + norm_eps) * gain_vec


def dot_f32(a, b, dims=((1,), (0,))):
    return lax.dot_general(a, b, (dims, ((), ())), preferred_element_type=F32)


def params(limit=16):
    return pltpu.CompilerParams(vmem_limit_bytes=limit * 1024 * 1024)


VM = pl.BlockSpec(memory_space=pltpu.VMEM)
ANY = pl.BlockSpec(memory_space=pl.ANY)
HBM = pl.BlockSpec(memory_space=pltpu.HBM)


def shape(dims, dtype=BF16):
    return jax.ShapeDtypeStruct(dims, dtype)


def cost(flops, moved):
    return pl.CostEstimate(flops=flops, bytes_accessed=moved, transcendentals=0)


def in_hbm(*values):
    return [pltpu.with_memory_space_constraint(v, pltpu.HBM) for v in values]


def pack_qkv_kernel(wq, wk, wv, wc, all_ref, send_ref, wc_ref, sems):
    part, width = send_ref.shape[0], wq.shape[1]
    group = lax.axis_index("grp")
    mine = pl.ds(pl.multiple_of(group * part, part), part)
    columns = wc_ref.shape[1]
    first, rest = [], []
    for n, w in enumerate((wq, wk, wv)):
        at = slice(n * width, (n + 1) * width)
        first.append(pltpu.make_async_copy(w.at[mine, :], send_ref.at[:, at], sems.at[n]))
        rest.append(pltpu.make_async_copy(w, all_ref.at[:, at], sems.at[3 + n]))
    half = wc.at[:, pl.ds(pl.multiple_of(group * columns, columns), columns)]
    rest.append(pltpu.make_async_copy(half, wc_ref, sems.at[6]))
    for copy in first + rest:
        copy.start()
    for copy in first + rest:
        copy.wait()


def pack_qkv(weights, wc):
    block, width = weights[0].shape
    return pl.pallas_call(
        pack_qkv_kernel,
        out_shape=(
            shape((block, 3 * width)),
            shape((block // 2, 3 * width)),
            shape((wc.shape[0], wc.shape[1] // 2)),
        ),
        in_specs=[HBM] * 4,
        out_specs=[VM] * 3,
        scratch_shapes=[pltpu.SemaphoreType.DMA((7,))],
        cost_estimate=cost(2_000_000, 400_000),
        compiler_params=params(),
        name="pack_qkv",
    )(*in_hbm(*weights, wc))


def norm_kernel(x_hbm, gain_hbm, send_ref, own_ref, pair_ref, x_ref, gain_ref, normed, sems):
    side, low = lax.axis_index("sp") // 2, lax.axis_index("sp") % 2
    core = lax.axis_index("tp") % 2
    block = own_ref.shape[1]
    half = 2 * block
    half_rows = send_ref.shape[0]
    copies = [
        pltpu.make_async_copy(x_hbm, x_ref, sems.at[0]),
        pltpu.make_async_copy(gain_hbm, gain_ref, sems.at[1]),
    ]
    for copy in copies:
        copy.start()
    for copy in copies:
        copy.wait()
    x = x_ref[...].astype(F32)
    squares = jnp.mean(x * x, axis=1, keepdims=True)
    normed[...] = (x * lax.rsqrt(squares + norm_eps) * gain_ref[...]).astype(BF16)
    first = pl.multiple_of(core * half_rows, half_rows)
    away = pl.multiple_of((1 - side) * half, half)
    send_ref[...] = normed[pl.ds(first, half_rows), pl.ds(away, half)]
    own_ref[...] = normed[:, pl.ds(pl.multiple_of(side * half + low * block, block), block)]
    pair_ref[...] = normed[:, pl.ds(pl.multiple_of(side * half + (1 - low) * block, block), block)]


def norm_parts(tokens, gain, block):
    rows, features = tokens.shape
    return pl.pallas_call(
        norm_kernel,
        out_shape=(shape((rows // 2, 2 * block)), shape((rows, block)), shape((rows, block))),
        in_specs=[HBM] * 2,
        out_specs=[VM] * 3,
        scratch_shapes=[
            pltpu.VMEM((rows, features), BF16),
            pltpu.VMEM((1, features), F32),
            pltpu.VMEM((rows, features), BF16),
            pltpu.SemaphoreType.DMA((2,)),
        ],
        cost_estimate=cost(2_000_000, 1_000_000),
        compiler_params=params(),
        name="norm_parts",
    )(*in_hbm(tokens, gain.reshape(1, features)))


def pack_kernel(
    gv_hbm, gg_hbm, wa_hbm, off_hbm, head_hbm, gain_hbm, bias_hbm, *refs
):
    gv_ref, gv_send, gg_ref, out_ref, off_ref, head_ref, gain_ref, bias_ref, sems = refs
    cw, aw = gv_hbm.shape[1], wa_hbm.shape[0]
    part = gv_send.shape[0]
    mine = pl.ds(pl.multiple_of(lax.axis_index("grp") * part, part), part)
    pairs = (
        (gain_hbm, gain_ref),
        (bias_hbm, bias_ref),
        (gv_hbm.at[mine, :], gv_send),
        (gg_hbm, gg_ref),
        (wa_hbm, out_ref.at[:aw, :]),
        (off_hbm, off_ref),
        (head_hbm, head_ref),
        (gv_hbm, gv_ref),
    )
    copies = [pltpu.make_async_copy(a, b, sems.at[n]) for n, (a, b) in enumerate(pairs)]
    for copy in copies:
        copy.start()
    for copy in copies[:2]:
        copy.wait()
    extra = out_ref.shape[0] - aw
    for n, ref in enumerate((gain_ref, bias_ref)):
        rest = ref[...]
        for piece in range(3):
            part = rest.astype(BF16)
            rest = rest - part.astype(F32)
            first = (3 * n + piece) * cw
            out_ref[aw:, first : first + cw] = jnp.broadcast_to(part, (extra, cw))
    for copy in copies[2:]:
        copy.wait()


def pack(gv, gg, wa, off, head_gain, gain, bias):
    block, cw = gv.shape
    aw, width = wa.shape
    return pl.pallas_call(
        pack_kernel,
        out_shape=(
            shape((block, cw)),
            shape((block // 2, cw)),
            shape((block, cw)),
            shape((aw + 16, width)),
            shape(off.shape),
            shape(head_gain.shape, F32),
        ),
        in_specs=[HBM] * 7,
        out_specs=[VM] * 6,
        scratch_shapes=[
            pltpu.VMEM((1, cw), F32),
            pltpu.VMEM((1, cw), F32),
            pltpu.SemaphoreType.DMA((8,)),
        ],
        cost_estimate=cost(2_000_000, 2_000_000),
        compiler_params=params(),
        name="pack",
    )(*in_hbm(gv, gg, wa, off, head_gain, gain.reshape(1, cw), bias.reshape(1, cw)))


def assemble_kernel(own_ref, pair_ref, got_ref, other_ref, own_out, pair_out):
    low = lax.axis_index("sp") % 2
    core = lax.axis_index("tp") % 2
    rows, block = own_ref.shape
    half = got_ref.shape[0]
    own_out[:rows, :] = own_ref[...]
    pair_out[:rows, :] = pair_ref[...]
    own_at = pl.multiple_of(low * block, block)
    pair_at = pl.multiple_of((1 - low) * block, block)
    for part, at in ((got_ref, core), (other_ref, 1 - core)):
        first = pl.multiple_of(rows + at * half, half)
        own_out[pl.ds(first, half), :] = part[:, pl.ds(own_at, block)]
        pair_out[pl.ds(first, half), :] = part[:, pl.ds(pair_at, block)]


def assemble(own, pair, got, other):
    rows, block = own.shape
    return pl.pallas_call(
        assemble_kernel,
        out_shape=(shape((2 * rows, block)),) * 2,
        in_specs=[VM] * 4,
        out_specs=[VM] * 2,
        cost_estimate=cost(2_000_000, 1_000_000),
        compiler_params=params(),
        name="assemble",
    )(own, pair, got, other)


def far_dot(x_pair, same, other):
    part = same.shape[0]
    group = lax.axis_index("grp")
    near = x_pair[:, pl.ds(pl.multiple_of(group * part, part), part)]
    rest = x_pair[:, pl.ds(pl.multiple_of((1 - group) * part, part), part)]
    return dot_f32(near, same[...]) + dot_f32(rest, other[...])


def qkv_kernel(x_own, x_pair, own, same, other, off_ref, keep_ref, send_ref):
    rows = x_own.shape[0] // 2
    width = send_ref.shape[1]
    total = dot_f32(x_own[...], own[...]) + far_dot(x_pair, same, other)
    keep_ref[...] = total
    for n in range(3):
        part = total[:, n * width : (n + 1) * width].astype(BF16)
        first = 4 * rows if n == 0 else 2 * (n - 1) * rows
        send_ref[first : first + rows, :] = part[rows:]
        if n > 0:
            send_ref[first + rows : first + 2 * rows, :] = part[:rows]
    send_ref[5 * rows :, :] = jnp.zeros((send_ref.shape[0] - 5 * rows, width), BF16)
    send_ref[5 * rows : 5 * rows + off_ref.shape[0], :] = off_ref[...]


def project_qkv(x_own, x_pair, own, same, other, off):
    rows, width = x_own.shape[0], own.shape[1] // 3
    return pl.pallas_call(
        qkv_kernel,
        out_shape=(shape((rows, 3 * width), F32), shape((5 * rows // 2 + 16, width))),
        in_specs=[VM] * 6,
        out_specs=[VM] * 2,
        cost_estimate=cost(200_000_000, 1_000_000),
        compiler_params=params(),
        name="project_qkv",
    )(x_own, x_pair, own, same, other, off)


def sum_kernel(keep_ref, got_ref, sent_ref, after, q_ref, out_ref):
    rows, width = q_ref.shape

    def got(n):
        return got_ref[n * rows : (n + 1) * rows, :].astype(F32)

    q_ref[...] = (keep_ref[:rows, :width] + got(4)).astype(BF16)
    for n in range(4):
        at = slice((1 + n // 2) * width, (2 + n // 2) * width)
        part = keep_ref[(n % 2) * rows : (n % 2 + 1) * rows, at]
        out_ref[n * rows : (n + 1) * rows, :] = (part + got(n)).astype(BF16)
    first = 5 * rows
    out_ref[4 * rows :, :] = jnp.concatenate([sent_ref[first : first + 8, :], got_ref[first : first + 8, :]])


def sum_qkv(keep, got, sent, after):
    rows, width = keep.shape[0] // 2, got.shape[1]
    return pl.pallas_call(
        sum_kernel,
        out_shape=(shape((rows, width)), shape((4 * rows + 16, width))),
        in_specs=[VM] * 3 + [ANY],
        out_specs=[VM] * 2,
        cost_estimate=cost(1_000_000, 1_000_000),
        compiler_params=params(),
        name="sum_qkv",
    )(keep, got, sent, after)


def glu_kernel(x_own, x_pair, gv, gg, gv_same, gv_other, gg_pair, after, keep_ref, send_ref):
    rows = x_own.shape[0] // 2
    cw = gv.shape[1]
    for n in range(2):
        own = (gv, gg)[n]
        far = far_dot(x_pair, gv_same, gv_other) if n == 0 else dot_f32(x_pair[...], gg_pair[...])
        total = dot_f32(x_own[...], own[...]) + far
        at = slice(n * cw, (n + 1) * cw)
        keep_ref[:, at] = total[:rows]
        send_ref[:, at] = total[rows:].astype(BF16)


def project_glu(x_own, x_pair, own, pair, after):
    rows, width = x_own.shape[0] // 2, 2 * own[0].shape[1]
    return pl.pallas_call(
        glu_kernel,
        out_shape=(shape((rows, width), F32), shape((rows, width))),
        in_specs=[VM] * 7 + [ANY],
        out_specs=[VM] * 2,
        cost_estimate=cost(270_000_000, 1_000_000),
        compiler_params=params(),
        name="project_glu",
    )(x_own, x_pair, *own, *pair, after)


def gate_kernel(keep_ref, got_ref, gated_ref, tail_ref):
    rows, cw = gated_ref.shape
    glu = keep_ref[...] + got_ref[...].astype(F32)
    value = glu[:, :cw].astype(BF16).astype(F32)
    gate = glu[:, cw:].astype(BF16).astype(F32)
    gated = (value * jax.nn.sigmoid(gate)).astype(BF16)
    gated_ref[...] = gated
    tail_ref[...] = gated[rows - tail_ref.shape[0] :]


def gate(keep, got, tail):
    rows, cw = keep.shape[0], keep.shape[1] // 2
    return pl.pallas_call(
        gate_kernel,
        out_shape=(shape((rows, cw)), shape((tail, cw))),
        in_specs=[VM] * 2,
        out_specs=[VM] * 2,
        cost_estimate=cost(2_000_000, 500_000),
        compiler_params=params(),
        name="gate",
    )(keep, got)


def conv_kernel(gated_ref, before_ref, taps_ref, att_ref, act_ref, padded):
    rows, aw = att_ref.shape
    tail = before_ref.shape[0]
    taps = taps_ref.shape[0]
    padded[:tail, :] = before_ref[...].astype(F32)
    padded[tail:, :] = gated_ref[...].astype(F32)
    total = None
    for tap in range(taps):
        first = tail - (taps - 1) + tap
        part = taps_ref[tap : tap + 1, :] * padded[first : first + rows, :]
        total = part if total is None else total + part
    act_ref[:, :aw] = att_ref[...]
    act_ref[:, aw:] = total.astype(BF16)


def conv(gated, before, taps, attended):
    rows, cw = gated.shape
    return pl.pallas_call(
        conv_kernel,
        out_shape=shape((rows, attended.shape[1] + cw)),
        in_specs=[VM] * 4,
        out_specs=VM,
        scratch_shapes=[pltpu.VMEM((rows + before.shape[0], cw), F32)],
        cost_estimate=cost(20_000_000, 500_000),
        compiler_params=params(),
        name="conv",
    )(gated, before, taps, attended)


def suffix_matrix(keys):
    before = lax.broadcasted_iota(jnp.int32, (2 * keys, 2 * keys), 0) % keys
    column = lax.broadcasted_iota(jnp.int32, (2 * keys, 2 * keys), 1)
    return jnp.where((column >= keys) | (before > column), 1.0, 0.0).astype(BF16)


def stick_block(q, k, v, off, hd, suffix, carry, diagonal):
    rows, width = q.shape
    keys = k.shape[0]
    lane = lax.broadcasted_iota(jnp.int32, (rows, width), 1) // hd
    offsets = off.astype(F32)
    weights, totals, values = [], [], []
    for h in range(width // hd):
        qh = jnp.where(lane == h, q, jnp.zeros_like(q))
        s = dot_f32(qh, k, ((1,), (1,))) * hd ** (-0.5) + offsets[h : h + 1, :]
        soft = jnp.maximum(s, 0.0) + jnp.log(1.0 + jnp.exp(-jnp.abs(s)))
        log_not = -soft
        if diagonal:
            allowed = lax.broadcasted_iota(jnp.int32, (rows, keys), 1) <= lax.broadcasted_iota(
                jnp.int32, (rows, keys), 0
            )
            log_not = jnp.where(allowed, log_not, 0.0)
        high = log_not.astype(BF16)
        low = (log_not - high.astype(F32)).astype(BF16)
        sums = dot_f32(jnp.concatenate([high, low], axis=1), suffix)
        later = sums[:, :keys]
        if carry is not None:
            later = later + carry[h]
        w = jnp.exp(s - soft + later)
        if diagonal:
            w = jnp.where(allowed, w, 0.0)
        weights.append(w)
        totals.append(sums[:, keys:])
        values.append(jnp.where(lane == h, v, jnp.zeros_like(v)))
    mix = dot_f32(
        jnp.concatenate([w.astype(BF16) for w in weights], axis=1), jnp.concatenate(values, axis=0)
    )
    return mix, weights, totals


def near_kernel(q_ref, mine_ref, gain_ref, after, mix_ref, mass_ref, carry_ref):
    rows = q_ref.shape[0]
    heads, hd = gain_ref.shape
    suffix = suffix_matrix(rows)
    for n in range(2):
        k = mine_ref[n * rows : (n + 1) * rows, :]
        v = mine_ref[(2 + n) * rows : (3 + n) * rows, :]
        off = mine_ref[4 * rows + 8 * n : 4 * rows + 8 * n + 8, :]
        mix, weights, totals = stick_block(q_ref[...], k, v, off, hd, suffix, None, n == 0)
        mix_ref[n] = mix
        for h in range(heads):
            mass_ref[n * heads + h] = weights[h]
            carry_ref[n * heads + h] = totals[h]


def near_attention(q, mine, head_gain, after):
    rows, width = q.shape
    heads = head_gain.shape[0]
    return pl.pallas_call(
        near_kernel,
        out_shape=(
            shape((2, rows, width), F32),
            shape((2 * heads, rows, rows), F32),
            shape((2 * heads, rows, rows), F32),
        ),
        in_specs=[VM] * 3 + [ANY],
        out_specs=[VM] * 3,
        cost_estimate=cost(200_000_000, 1_000_000),
        compiler_params=params(),
        name="near_attention",
    )(q, mine, head_gain, after)


def attention_kernel(q_ref, pair_ref, gain_ref, mix_ref, mass_ref, carry_ref, after, out_ref, log_ref, acc, mass, carry):
    me = lax.axis_index("sp")
    rows, width = q_ref.shape
    heads, hd = gain_ref.shape
    lane = lax.broadcasted_iota(jnp.int32, (rows, width), 1) // hd
    suffix = suffix_matrix(rows)
    acc[...] = mix_ref[0]
    for h in range(heads):
        mass[h] = mass_ref[h]
        carry[h] = carry_ref[h]

    def earlier(t, _):
        slot = jnp.bitwise_xor(me - t, me)

        @pl.when(slot == 2)
        def _():
            scale = jnp.zeros_like(acc)
            for h in range(heads):
                left = jnp.exp(carry[h])
                mass[h] = mass[h] + left * mass_ref[heads + h]
                scale = jnp.where(lane == h, left, scale)
                carry[h] = carry[h] + carry_ref[heads + h]
            acc[...] = acc[...] + scale * mix_ref[1]

        @pl.when(slot != 2)
        def _():
            n = slot // 2
            k = pair_ref[pl.ds(pl.multiple_of(n * rows, rows), rows), :]
            v = pair_ref[pl.ds(pl.multiple_of((2 + n) * rows, rows), rows), :]
            off = jnp.where(
                n == 0,
                pair_ref[4 * rows : 4 * rows + 8, :].astype(F32),
                pair_ref[4 * rows + 8 : 4 * rows + 16, :].astype(F32),
            )
            so_far = [carry[h] for h in range(heads)]
            mix, weights, totals = stick_block(q_ref[...], k, v, off, hd, suffix, so_far, False)
            acc[...] = acc[...] + mix
            for h in range(heads):
                mass[h] = mass[h] + weights[h]
                carry[h] = so_far[h] + totals[h]

        return 0

    lax.fori_loop(1, me + 1, earlier, 0)
    mixed = acc[...]
    squares = mixed * mixed
    inverse = jnp.zeros_like(mixed)
    for h in range(heads):
        mean = jnp.sum(jnp.where(lane == h, squares, 0.0), axis=1, keepdims=True) / hd
        inverse = jnp.where(lane == h, lax.rsqrt(mean + norm_eps), inverse)
    gain = jnp.concatenate([gain_ref[h : h + 1, :] for h in range(heads)], axis=1)
    out_ref[...] = (mixed * inverse * gain).astype(BF16)
    for h in range(heads):
        log_ref[h : h + 1, :] = jnp.log(jnp.sum(jnp.transpose(mass[h]), axis=0, keepdims=True))


def attention(q, pair, head_gain, near, after):
    rows, width = q.shape
    heads = head_gain.shape[0]
    return pl.pallas_call(
        attention_kernel,
        out_shape=(shape((rows, width)), shape((heads, rows), F32)),
        in_specs=[VM] * 6 + [ANY],
        out_specs=[VM] * 2,
        scratch_shapes=[
            pltpu.VMEM((rows, width), F32),
            pltpu.VMEM((heads, rows, rows), F32),
            pltpu.VMEM((heads, rows, rows), F32),
        ],
        cost_estimate=cost(400_000_000, 1_000_000),
        compiler_params=params(),
        name="stick_attention",
    )(q, pair, head_gain, *near, after)


def final_kernel(*refs):
    act, wa, wc, gain_ref, out_ref, mix = refs[:4], refs[4:8], refs[8:14], refs[14], refs[15], refs[16]
    cw = wc[0].shape[0]
    aw = act[0].shape[1] - cw
    convs = [c[:, aw:].astype(F32) for c in act]
    mean = sum(jnp.sum(v, axis=1, keepdims=True) for v in convs) / (4 * cw)
    centered = [v - mean for v in convs]
    spread = sum(jnp.sum(v * v, axis=1, keepdims=True) for v in centered) / (4 * cw)
    inverse = lax.rsqrt(spread + norm_eps)
    ys = []
    for slot in range(4):
        pieces = [wa[slot][aw : aw + 1, n * cw : (n + 1) * cw].astype(F32) for n in range(6)]
        gain = pieces[0] + pieces[1] + pieces[2]
        bias = pieces[3] + pieces[4] + pieces[5]
        y = centered[slot] * inverse * gain + bias
        ys.append((y * jax.nn.sigmoid(y)).astype(BF16))
    swap = lax.axis_index("grp") == 1
    rows, width = mix.shape
    half = width // 2
    squares = jnp.zeros((rows, 1), F32)
    for first in range(0, width, CHUNK):
        at = slice(first, first + CHUNK)
        part = None
        for slot in range(4):
            if slot < 2:
                w = wc[slot][:, at]
            else:
                pair = wc[2 * slot - 2], wc[2 * slot - 1]
                near, far = pair if first < half else pair[::-1]
                inner = slice(first % half, first % half + CHUNK)
                w = jnp.where(swap, far[:, inner], near[:, inner])
            one = dot_f32(ys[slot], w)
            part = one if part is None else part + one
        for slot in (0, 2):
            w = jnp.concatenate([wa[slot][:aw, at], wa[slot + 1][:aw, at]], axis=0)
            part = part + dot_f32(jnp.concatenate([act[slot][:, :aw], act[slot + 1][:, :aw]], axis=1), w)
        mix[:, at] = part
        squares = squares + jnp.sum(part * part, axis=1, keepdims=True)
    out_ref[...] = (mix[...] * lax.rsqrt(squares / width + norm_eps) * gain_ref[...]).astype(BF16)


CHUNK = 256


def finish(act, wa, wc, out_gain):
    rows, width = act[0].shape[0], wa[0].shape[1]
    return pl.pallas_call(
        final_kernel,
        out_shape=shape((rows, width)),
        in_specs=[VM] * 15,
        out_specs=VM,
        scratch_shapes=[pltpu.VMEM((rows, width), F32)],
        cost_estimate=cost(800_000_000, 7_000_000),
        compiler_params=params(32),
        name="finish_rows",
    )(*act, *wa, *wc, out_gain.reshape(1, width))


def paired(
    tokens,
    norm_gain,
    w_query,
    w_key,
    w_value,
    w_glu_value,
    w_glu_gate,
    key_offset,
    head_gain,
    conv_taps,
    channel_gain,
    channel_bias,
    w_out_attn,
    w_out_conv,
    out_gain,
):
    own_qkv, half_qkv, wc_half = pack_qkv((w_query, w_key, w_value), w_out_conv)
    qkv_same = exchange(half_qkv, "sp", 1)
    wc_x = exchange(wc_half, "tp", 2)
    wc_y = exchange(wc_x, "grp", 1)
    wc_yc = exchange(wc_y, "tp", 1)
    x_send, mine_own, mine_pair = norm_parts(tokens, norm_gain, w_query.shape[0])
    x_got = exchange(x_send, "sp", 2)
    own_gv, half_gv, own_gg, wa_mine, off, head_rows = pack(
        w_glu_value, w_glu_gate, w_out_attn, key_offset.T, head_gain, channel_gain, channel_bias
    )
    qkv_same, half_gv = lax.optimization_barrier((qkv_same, half_gv))
    gv_same = exchange(half_gv, "sp", 1)
    gg_pair = exchange(own_gg, "sp", 1)
    gv_other = exchange(gv_same, "grp", 1)
    qkv_other = exchange(qkv_same, "grp", 1)
    x_other = exchange(x_got, "tp", 1)
    wa_x = exchange(wa_mine, "tp", 2)
    wc_core = exchange(w_out_conv, "tp", 1)
    wa_core = exchange(wa_mine, "tp", 1)
    wc_xc = exchange(wc_x, "tp", 1)
    wa_xc = exchange(wa_x, "tp", 1)
    x_own, x_pair = assemble(mine_own, mine_pair, x_got, x_other)

    keep, sent = project_qkv(x_own, x_pair, own_qkv, qkv_same, qkv_other, off)
    got = exchange(sent, "sp", 2)
    glu_keep, glu_sent = project_glu(
        x_own, x_pair, (own_gv, own_gg), (gv_same, gv_other, gg_pair), sent
    )
    glu_got = exchange(glu_sent, "sp", 2)
    q, mine_two = sum_qkv(keep, got, sent, glu_sent)
    pair_two = exchange(mine_two, "sp", 1)
    near = near_attention(q, mine_two, head_rows, mine_two)
    gated, tail = gate(glu_keep, glu_got, -(-conv_taps.shape[0] // 16) * 16)
    before = from_behind(tail, "sp", 1)
    attended, log_mass = attention(q, pair_two, head_rows, near, tail)
    act_mine = conv(gated, before, conv_taps, attended)
    act_x = exchange(act_mine, "tp", 2)
    act_core = exchange(act_mine, "tp", 1)
    act = (act_mine, act_core, act_x, exchange(act_x, "tp", 1))
    wa = (wa_mine, wa_core, wa_x, wa_xc)
    wc = (w_out_conv, wc_core, wc_x, wc_y, wc_xc, wc_yc)
    mixed = finish(act, wa, wc, out_gain)
    return (mixed, log_mass)


def gathered(
    tokens,
    norm_gain,
    w_query,
    w_key,
    w_value,
    w_glu_value,
    w_glu_gate,
    key_offset,
    head_gain,
    conv_taps,
    channel_gain,
    channel_bias,
    w_out_attn,
    w_out_conv,
    out_gain,
):
    row_count = tokens.shape[0]
    hd = head_gain.shape[1]
    channels = conv_taps.shape[1] * lax.axis_size("tp")
    normed = row_norm(tokens.astype(jnp.float32), norm_gain).astype(jnp.bfloat16)
    weights_in = (w_query, w_key, w_value, w_glu_value, w_glu_gate)
    pieces = (
        lax.all_gather(weights_in[0], "sp", axis=0, tiled=True),
        lax.all_gather(weights_in[1], "sp", axis=0, tiled=True),
        lax.all_gather(weights_in[2], "sp", axis=0, tiled=True),
        lax.all_gather(weights_in[3], "sp", axis=0, tiled=True),
        lax.all_gather(weights_in[4], "sp", axis=0, tiled=True),
    )
    projected = tuple(
        (jnp.dot(normed, shard_piece, preferred_element_type=jnp.float32) for shard_piece in pieces)
    )
    query, key_rows, value_rows, glu_value, glu_gate = [
        summed.astype(jnp.bfloat16) for summed in projected
    ]
    kv_local = key_rows.shape[1] // hd
    group_size = query.shape[1] // key_rows.shape[1]
    heads_local = kv_local * group_size
    all_keys, all_values, all_offsets = (
        lax.all_gather(key_rows, "sp", axis=0, tiled=True),
        lax.all_gather(value_rows, "sp", axis=0, tiled=True),
        lax.all_gather(key_offset, "sp", axis=0, tiled=True),
    )
    sequence_length_total = all_keys.shape[0]
    shard_count = lax.axis_size("sp")
    per_block = 1
    while (
        per_block * 2 <= shard_count
        and shard_count % (per_block * 2) == 0
        and (per_block * 2 * row_count <= 1024)
    ):
        per_block = per_block * 2
    span_len = per_block * row_count
    query_heads = query.reshape(row_count, kv_local, group_size, hd)
    key_heads = all_keys.reshape(sequence_length_total, kv_local, hd)
    value_heads = all_values.reshape(sequence_length_total, kv_local, hd)
    my_index = lax.axis_index("sp")
    query_pos = my_index * row_count + jnp.arange(row_count, dtype=jnp.int32)
    last_block = my_index // per_block
    zeros_mix = jnp.zeros((kv_local, group_size, row_count, hd), jnp.float32)
    zeros_row = jnp.zeros((kv_local, group_size, row_count), jnp.float32)

    def sweep(turn_index, carry):
        head_mix, mass_sum, carried = carry
        first_key = (last_block - turn_index) * span_len
        key_block = lax.dynamic_slice_in_dim(key_heads, first_key, span_len, 0)
        value_block = lax.dynamic_slice_in_dim(value_heads, first_key, span_len, 0)
        offset_block = lax.dynamic_slice_in_dim(all_offsets, first_key, span_len, 0).astype(
            jnp.float32
        )
        offset_block = offset_block.T.reshape(kv_local, group_size, 1, span_len)
        scores = (
            jnp.einsum("qhgd,khd->hgqk", query_heads, key_block, preferred_element_type=jnp.float32)
            * hd ** (-0.5)
            + offset_block
        )
        key_pos = first_key + jnp.arange(span_len, dtype=jnp.int32)
        allowed = key_pos[None, :] <= query_pos[:, None]
        log_not = jnp.where(allowed, jax.nn.log_sigmoid(-scores), 0.0)
        later = lax.cumsum(log_not, axis=3, reverse=True) - log_not + carried[..., None]
        weights = jnp.where(allowed, jnp.exp(jax.nn.log_sigmoid(scores) + later), 0.0)
        head_mix = head_mix + jnp.einsum(
            "hgqk,khd->hgqd",
            weights.astype(jnp.bfloat16),
            value_block,
            preferred_element_type=jnp.float32,
        )
        return (head_mix, mass_sum + jnp.sum(weights, axis=3), carried + jnp.sum(log_not, axis=3))

    head_mix, mass_sum, _ = lax.fori_loop(
        0, last_block + 1, sweep, (zeros_mix, zeros_row, zeros_row)
    )
    log_mass = jnp.log(mass_sum).reshape(heads_local, row_count)
    head_rows = head_mix.transpose(2, 0, 1, 3).reshape(row_count, heads_local, hd)
    attended = (
        row_norm(head_rows, head_gain).astype(jnp.bfloat16).reshape(row_count, heads_local * hd)
    )
    gated = (glu_value.astype(jnp.float32) * jax.nn.sigmoid(glu_gate.astype(jnp.float32))).astype(
        jnp.bfloat16
    )
    reach_len = conv_taps.shape[0] - 1
    before = from_behind(gated[row_count - reach_len :], "sp", 1)
    padded = jnp.concatenate([before, gated], axis=0).astype(jnp.float32)
    conv_out = jnp.zeros(gated.shape, jnp.float32)
    for tap_index in range(conv_taps.shape[0]):
        conv_out = conv_out + conv_taps[tap_index] * padded[tap_index : tap_index + row_count]
    total_sum, total_squares = lax.psum(
        (jnp.sum(conv_out, axis=1), jnp.sum(conv_out * conv_out, axis=1)), "tp"
    )
    chan_mean = (total_sum / channels)[:, None]
    spread = (total_squares / channels)[:, None] - chan_mean * chan_mean
    centered = conv_out - chan_mean
    channel_out = jax.nn.silu(
        centered * lax.rsqrt(spread + norm_eps) * channel_gain + channel_bias
    ).astype(jnp.bfloat16)
    share = lax.psum_scatter(
        jnp.dot(attended, w_out_attn, preferred_element_type=jnp.float32)
        + jnp.dot(channel_out, w_out_conv, preferred_element_type=jnp.float32),
        "tp",
        scatter_dimension=0,
        tiled=True,
    )
    mixed = lax.all_gather(row_norm(share, out_gain).astype(jnp.bfloat16), "tp", axis=0, tiled=True)
    return (mixed, log_mass)


def solution(mesh):
    in_specs = (
        P(("grp", "sp"), None),
        P(),
        P("sp", "tp"),
        P("sp", "tp"),
        P("sp", "tp"),
        P("sp", "tp"),
        P("sp", "tp"),
        P(("grp", "sp"), "tp"),
        P("tp", None),
        P(None, "tp"),
        P("tp"),
        P("tp"),
        P("tp", None),
        P("tp", None),
        P(),
    )
    out_specs = (P(("grp", "sp"), None), P("tp", ("grp", "sp")))
    small = mesh.shape["sp"] == 4 and mesh.shape["tp"] == 4 and mesh.shape["grp"] == 2
    local = paired if small else gathered
    return jax.shard_map(local, mesh=mesh, in_specs=in_specs, out_specs=out_specs, check_vma=False)
```

```python
import jax
import jax.numpy as jnp
from jax import lax
from jax.experimental import pallas as pl
from jax.experimental.pallas import tpu as pltpu
from jax.sharding import PartitionSpec as P

norm_eps = 1e-06
BF16 = jnp.bfloat16
F32 = jnp.float32


def exchange(value, axis, bit):
    count = lax.axis_size(axis)
    return lax.ppermute(value, axis, [(s, s ^ bit) for s in range(count)])


def from_cross_behind(value, axis):
    count = lax.axis_size(axis)
    pairs = [(source, (source ^ 2) + 1) for source in range(count)]
    return lax.ppermute(value, axis, [(a, b) for a, b in pairs if b < count])


def from_behind(value, axis, steps):
    count = lax.axis_size(axis)
    initial, last = (max(0, -steps), min(count, count - steps))
    return lax.ppermute(value, axis, [(source, source + steps) for source in range(initial, last)])


def row_norm(values_in, gain_vec):
    squares = jnp.mean(values_in * values_in, axis=-1, keepdims=True)
    return values_in * lax.rsqrt(squares + norm_eps) * gain_vec


def dot_f32(a, b, dims=((1,), (0,))):
    return lax.dot_general(a, b, (dims, ((), ())), preferred_element_type=F32)


def params(limit=16):
    return pltpu.CompilerParams(vmem_limit_bytes=limit * 1024 * 1024)


VM = pl.BlockSpec(memory_space=pltpu.VMEM)
ANY = pl.BlockSpec(memory_space=pl.ANY)
HBM = pl.BlockSpec(memory_space=pltpu.HBM)


def shape(dims, dtype=BF16):
    return jax.ShapeDtypeStruct(dims, dtype)


def cost(flops, moved):
    return pl.CostEstimate(flops=flops, bytes_accessed=moved, transcendentals=0)


def in_hbm(*values):
    return [pltpu.with_memory_space_constraint(v, pltpu.HBM) for v in values]


def pack_qkv_kernel(wq, wk, wv, all_ref, send_ref, sems):
    part, width = send_ref.shape[0], wq.shape[1]
    mine = pl.ds(pl.multiple_of(lax.axis_index("grp") * part, part), part)
    first, rest = [], []
    for n, w in enumerate((wq, wk, wv)):
        at = slice(n * width, (n + 1) * width)
        first.append(pltpu.make_async_copy(w.at[mine, :], send_ref.at[:, at], sems.at[n]))
        rest.append(pltpu.make_async_copy(w, all_ref.at[:, at], sems.at[3 + n]))
    for copy in first + rest:
        copy.start()
    for copy in first + rest:
        copy.wait()


def pack_qkv(weights):
    block, width = weights[0].shape
    return pl.pallas_call(
        pack_qkv_kernel,
        out_shape=(shape((block, 3 * width)), shape((block // 2, 3 * width))),
        in_specs=[HBM] * 3,
        out_specs=[VM] * 2,
        scratch_shapes=[pltpu.SemaphoreType.DMA((6,))],
        cost_estimate=cost(2_000_000, 400_000),
        compiler_params=params(),
        name="pack_qkv",
    )(*in_hbm(*weights))


def norm_kernel(x_hbm, gain_hbm, wc_hbm, send_ref, own_ref, pair_ref, wc_ref, x_ref, gain_ref, normed, sems):
    side, low = lax.axis_index("sp") // 2, lax.axis_index("sp") % 2
    core = lax.axis_index("tp") % 2
    block = own_ref.shape[1]
    half = 2 * block
    half_rows = send_ref.shape[0]
    columns = wc_ref.shape[1]
    mine = pl.ds(pl.multiple_of(lax.axis_index("grp") * columns, columns), columns)
    copies = [
        pltpu.make_async_copy(x_hbm, x_ref, sems.at[0]),
        pltpu.make_async_copy(gain_hbm, gain_ref, sems.at[1]),
        pltpu.make_async_copy(wc_hbm.at[:, mine], wc_ref, sems.at[2]),
    ]
    for copy in copies:
        copy.start()
    for copy in copies[:2]:
        copy.wait()
    x = x_ref[...].astype(F32)
    squares = jnp.mean(x * x, axis=1, keepdims=True)
    normed[...] = (x * lax.rsqrt(squares + norm_eps) * gain_ref[...]).astype(BF16)
    first = pl.multiple_of(core * half_rows, half_rows)
    away = pl.multiple_of((1 - side) * half, half)
    send_ref[...] = normed[pl.ds(first, half_rows), pl.ds(away, half)]
    own_ref[...] = normed[:, pl.ds(pl.multiple_of(side * half + low * block, block), block)]
    pair_ref[...] = normed[:, pl.ds(pl.multiple_of(side * half + (1 - low) * block, block), block)]
    copies[2].wait()


def norm_parts(tokens, gain, block, wc):
    rows, features = tokens.shape
    return pl.pallas_call(
        norm_kernel,
        out_shape=(
            shape((rows // 2, 2 * block)),
            shape((rows, block)),
            shape((rows, block)),
            shape((wc.shape[0], wc.shape[1] // 2)),
        ),
        in_specs=[HBM] * 3,
        out_specs=[VM] * 4,
        scratch_shapes=[
            pltpu.VMEM((rows, features), BF16),
            pltpu.VMEM((1, features), F32),
            pltpu.VMEM((rows, features), BF16),
            pltpu.SemaphoreType.DMA((3,)),
        ],
        cost_estimate=cost(2_000_000, 1_000_000),
        compiler_params=params(),
        name="norm_parts",
    )(*in_hbm(tokens, gain.reshape(1, features), wc))


def pack_kernel(
    gv_hbm, gg_hbm, wa_hbm, off_hbm, head_hbm, gain_hbm, bias_hbm, *refs
):
    gv_ref, gv_send, gg_ref, out_ref, off_ref, head_ref, gain_ref, bias_ref, sems = refs
    cw, aw = gv_hbm.shape[1], wa_hbm.shape[0]
    part = gv_send.shape[0]
    mine = pl.ds(pl.multiple_of(lax.axis_index("grp") * part, part), part)
    pairs = (
        (gain_hbm, gain_ref),
        (bias_hbm, bias_ref),
        (gv_hbm.at[mine, :], gv_send),
        (gg_hbm, gg_ref),
        (wa_hbm, out_ref.at[:aw, :]),
        (off_hbm, off_ref),
        (head_hbm, head_ref),
        (gv_hbm, gv_ref),
    )
    copies = [pltpu.make_async_copy(a, b, sems.at[n]) for n, (a, b) in enumerate(pairs)]
    for copy in copies:
        copy.start()
    for copy in copies[:2]:
        copy.wait()
    extra = out_ref.shape[0] - aw
    for n, ref in enumerate((gain_ref, bias_ref)):
        rest = ref[...]
        for piece in range(3):
            part = rest.astype(BF16)
            rest = rest - part.astype(F32)
            first = (3 * n + piece) * cw
            out_ref[aw:, first : first + cw] = jnp.broadcast_to(part, (extra, cw))
    for copy in copies[2:]:
        copy.wait()


def pack(gv, gg, wa, off, head_gain, gain, bias):
    block, cw = gv.shape
    aw, width = wa.shape
    return pl.pallas_call(
        pack_kernel,
        out_shape=(
            shape((block, cw)),
            shape((block // 2, cw)),
            shape((block, cw)),
            shape((aw + 16, width)),
            shape(off.shape),
            shape(head_gain.shape, F32),
        ),
        in_specs=[HBM] * 7,
        out_specs=[VM] * 6,
        scratch_shapes=[
            pltpu.VMEM((1, cw), F32),
            pltpu.VMEM((1, cw), F32),
            pltpu.SemaphoreType.DMA((8,)),
        ],
        cost_estimate=cost(2_000_000, 2_000_000),
        compiler_params=params(),
        name="pack",
    )(*in_hbm(gv, gg, wa, off, head_gain, gain.reshape(1, cw), bias.reshape(1, cw)))


def assemble_kernel(own_ref, pair_ref, got_ref, other_ref, own_out, pair_out):
    low = lax.axis_index("sp") % 2
    core = lax.axis_index("tp") % 2
    rows, block = own_ref.shape
    half = got_ref.shape[0]
    own_out[:rows, :] = own_ref[...]
    pair_out[:rows, :] = pair_ref[...]
    own_at = pl.multiple_of(low * block, block)
    pair_at = pl.multiple_of((1 - low) * block, block)
    for part, at in ((got_ref, core), (other_ref, 1 - core)):
        first = pl.multiple_of(rows + at * half, half)
        own_out[pl.ds(first, half), :] = part[:, pl.ds(own_at, block)]
        pair_out[pl.ds(first, half), :] = part[:, pl.ds(pair_at, block)]


def assemble(own, pair, got, other):
    rows, block = own.shape
    return pl.pallas_call(
        assemble_kernel,
        out_shape=(shape((2 * rows, block)),) * 2,
        in_specs=[VM] * 4,
        out_specs=[VM] * 2,
        cost_estimate=cost(2_000_000, 1_000_000),
        compiler_params=params(),
        name="assemble",
    )(own, pair, got, other)


def far_dot(x_pair, same, other):
    part = same.shape[0]
    group = lax.axis_index("grp")
    near = x_pair[:, pl.ds(pl.multiple_of(group * part, part), part)]
    rest = x_pair[:, pl.ds(pl.multiple_of((1 - group) * part, part), part)]
    return dot_f32(near, same[...]) + dot_f32(rest, other[...])


def qkv_kernel(x_own, x_pair, own, same, other, off_ref, keep_ref, send_ref):
    rows = x_own.shape[0] // 2
    width = send_ref.shape[1]
    total = dot_f32(x_own[...], own[...]) + far_dot(x_pair, same, other)
    keep_ref[...] = total
    for n in range(3):
        part = total[:, n * width : (n + 1) * width].astype(BF16)
        first = 4 * rows if n == 0 else 2 * (n - 1) * rows
        send_ref[first : first + rows, :] = part[rows:]
        if n > 0:
            send_ref[first + rows : first + 2 * rows, :] = part[:rows]
    send_ref[5 * rows :, :] = jnp.zeros((send_ref.shape[0] - 5 * rows, width), BF16)
    send_ref[5 * rows : 5 * rows + off_ref.shape[0], :] = off_ref[...]


def project_qkv(x_own, x_pair, own, same, other, off):
    rows, width = x_own.shape[0], own.shape[1] // 3
    return pl.pallas_call(
        qkv_kernel,
        out_shape=(shape((rows, 3 * width), F32), shape((5 * rows // 2 + 16, width))),
        in_specs=[VM] * 6,
        out_specs=[VM] * 2,
        cost_estimate=cost(200_000_000, 1_000_000),
        compiler_params=params(),
        name="project_qkv",
    )(x_own, x_pair, own, same, other, off)


def sum_kernel(keep_ref, got_ref, sent_ref, after, q_ref, out_ref):
    rows, width = q_ref.shape

    def got(n):
        return got_ref[n * rows : (n + 1) * rows, :].astype(F32)

    q_ref[...] = (keep_ref[:rows, :width] + got(4)).astype(BF16)
    for n in range(4):
        at = slice((1 + n // 2) * width, (2 + n // 2) * width)
        part = keep_ref[(n % 2) * rows : (n % 2 + 1) * rows, at]
        out_ref[n * rows : (n + 1) * rows, :] = (part + got(n)).astype(BF16)
    first = 5 * rows
    out_ref[4 * rows :, :] = jnp.concatenate([sent_ref[first : first + 8, :], got_ref[first : first + 8, :]])


def sum_qkv(keep, got, sent, after):
    rows, width = keep.shape[0] // 2, got.shape[1]
    return pl.pallas_call(
        sum_kernel,
        out_shape=(shape((rows, width)), shape((4 * rows + 16, width))),
        in_specs=[VM] * 3 + [ANY],
        out_specs=[VM] * 2,
        cost_estimate=cost(1_000_000, 1_000_000),
        compiler_params=params(),
        name="sum_qkv",
    )(keep, got, sent, after)


def glu_kernel(x_own, x_pair, gv, gg, gv_same, gv_other, gg_pair, after, keep_ref, send_ref, own_tail, far_tail):
    rows = x_own.shape[0] // 2
    tail, cw = own_tail.shape[0], gv.shape[1]
    for n in range(2):
        own = (gv, gg)[n]
        far = far_dot(x_pair, gv_same, gv_other) if n == 0 else dot_f32(x_pair[...], gg_pair[...])
        total = dot_f32(x_own[...], own[...]) + far
        at = slice(n * cw, (n + 1) * cw)
        keep_ref[:, at] = total[:rows]
        send_ref[:, at] = total[rows:].astype(BF16)
        own_tail[:, at] = total[rows - tail : rows].astype(BF16)
        far_tail[:, at] = total[2 * rows - tail :].astype(BF16)


def project_glu(x_own, x_pair, own, pair, tail, after):
    rows, width = x_own.shape[0] // 2, 2 * own[0].shape[1]
    return pl.pallas_call(
        glu_kernel,
        out_shape=(
            shape((rows, width), F32),
            shape((rows, width)),
            shape((tail, width)),
            shape((tail, width)),
        ),
        in_specs=[VM] * 7 + [ANY],
        out_specs=[VM] * 4,
        cost_estimate=cost(270_000_000, 1_000_000),
        compiler_params=params(),
        name="project_glu",
    )(x_own, x_pair, *own, *pair, after)


def conv_kernel(keep_ref, got_ref, near_ref, far_ref, taps_ref, att_ref, act_ref, padded):
    rows, aw = att_ref.shape
    tail, cw = near_ref.shape[0], taps_ref.shape[1]
    taps = taps_ref.shape[0]

    def gated(glu):
        value = glu[:, :cw].astype(BF16).astype(F32)
        gate = glu[:, cw:].astype(BF16).astype(F32)
        return (value * jax.nn.sigmoid(gate)).astype(BF16).astype(F32)

    padded[:tail, :] = gated(near_ref[...].astype(F32) + far_ref[...].astype(F32))
    padded[tail:, :] = gated(keep_ref[...] + got_ref[...].astype(F32))
    total = None
    for tap in range(taps):
        first = tail - (taps - 1) + tap
        part = taps_ref[tap : tap + 1, :] * padded[first : first + rows, :]
        total = part if total is None else total + part
    act_ref[:, :aw] = att_ref[...]
    act_ref[:, aw:] = total.astype(BF16)


def conv(keep, got, near, far, taps, attended):
    rows, cw = keep.shape[0], taps.shape[1]
    return pl.pallas_call(
        conv_kernel,
        out_shape=shape((rows, attended.shape[1] + cw)),
        in_specs=[VM] * 6,
        out_specs=VM,
        scratch_shapes=[pltpu.VMEM((rows + near.shape[0], cw), F32)],
        cost_estimate=cost(20_000_000, 500_000),
        compiler_params=params(),
        name="conv",
    )(keep, got, near, far, taps, attended)


def suffix_matrix(keys):
    before = lax.broadcasted_iota(jnp.int32, (2 * keys, 2 * keys), 0) % keys
    column = lax.broadcasted_iota(jnp.int32, (2 * keys, 2 * keys), 1)
    return jnp.where((column >= keys) | (before > column), 1.0, 0.0).astype(BF16)


def stick_block(q, k, v, off, hd, suffix, carry, diagonal):
    rows, width = q.shape
    keys = k.shape[0]
    lane = lax.broadcasted_iota(jnp.int32, (rows, width), 1) // hd
    offsets = off.astype(F32)
    weights, totals, values = [], [], []
    for h in range(width // hd):
        qh = jnp.where(lane == h, q, jnp.zeros_like(q))
        s = dot_f32(qh, k, ((1,), (1,))) * hd ** (-0.5) + offsets[h : h + 1, :]
        soft = jnp.maximum(s, 0.0) + jnp.log(1.0 + jnp.exp(-jnp.abs(s)))
        log_not = -soft
        if diagonal:
            allowed = lax.broadcasted_iota(jnp.int32, (rows, keys), 1) <= lax.broadcasted_iota(
                jnp.int32, (rows, keys), 0
            )
            log_not = jnp.where(allowed, log_not, 0.0)
        high = log_not.astype(BF16)
        low = (log_not - high.astype(F32)).astype(BF16)
        sums = dot_f32(jnp.concatenate([high, low], axis=1), suffix)
        later = sums[:, :keys]
        if carry is not None:
            later = later + carry[h]
        w = jnp.exp(s - soft + later)
        if diagonal:
            w = jnp.where(allowed, w, 0.0)
        weights.append(w)
        totals.append(sums[:, keys:])
        values.append(jnp.where(lane == h, v, jnp.zeros_like(v)))
    mix = dot_f32(
        jnp.concatenate([w.astype(BF16) for w in weights], axis=1), jnp.concatenate(values, axis=0)
    )
    return mix, weights, totals


def near_kernel(q_ref, mine_ref, gain_ref, after, mix_ref, mass_ref, carry_ref):
    rows = q_ref.shape[0]
    heads, hd = gain_ref.shape
    suffix = suffix_matrix(rows)
    for n in range(2):
        k = mine_ref[n * rows : (n + 1) * rows, :]
        v = mine_ref[(2 + n) * rows : (3 + n) * rows, :]
        off = mine_ref[4 * rows + 8 * n : 4 * rows + 8 * n + 8, :]
        mix, weights, totals = stick_block(q_ref[...], k, v, off, hd, suffix, None, n == 0)
        mix_ref[n] = mix
        for h in range(heads):
            mass_ref[n * heads + h] = weights[h]
            carry_ref[n * heads + h] = totals[h]


def near_attention(q, mine, head_gain, after):
    rows, width = q.shape
    heads = head_gain.shape[0]
    return pl.pallas_call(
        near_kernel,
        out_shape=(
            shape((2, rows, width), F32),
            shape((2 * heads, rows, rows), F32),
            shape((2 * heads, rows, rows), F32),
        ),
        in_specs=[VM] * 3 + [ANY],
        out_specs=[VM] * 3,
        cost_estimate=cost(200_000_000, 1_000_000),
        compiler_params=params(),
        name="near_attention",
    )(q, mine, head_gain, after)


def attention_kernel(q_ref, pair_ref, gain_ref, mix_ref, mass_ref, carry_ref, after, out_ref, log_ref, acc, mass, carry):
    me = lax.axis_index("sp")
    rows, width = q_ref.shape
    heads, hd = gain_ref.shape
    lane = lax.broadcasted_iota(jnp.int32, (rows, width), 1) // hd
    suffix = suffix_matrix(rows)
    acc[...] = mix_ref[0]
    for h in range(heads):
        mass[h] = mass_ref[h]
        carry[h] = carry_ref[h]

    def earlier(t, _):
        slot = jnp.bitwise_xor(me - t, me)

        @pl.when(slot == 2)
        def _():
            scale = jnp.zeros_like(acc)
            for h in range(heads):
                left = jnp.exp(carry[h])
                mass[h] = mass[h] + left * mass_ref[heads + h]
                scale = jnp.where(lane == h, left, scale)
                carry[h] = carry[h] + carry_ref[heads + h]
            acc[...] = acc[...] + scale * mix_ref[1]

        @pl.when(slot != 2)
        def _():
            n = slot // 2
            k = pair_ref[pl.ds(pl.multiple_of(n * rows, rows), rows), :]
            v = pair_ref[pl.ds(pl.multiple_of((2 + n) * rows, rows), rows), :]
            off = jnp.where(
                n == 0,
                pair_ref[4 * rows : 4 * rows + 8, :].astype(F32),
                pair_ref[4 * rows + 8 : 4 * rows + 16, :].astype(F32),
            )
            so_far = [carry[h] for h in range(heads)]
            mix, weights, totals = stick_block(q_ref[...], k, v, off, hd, suffix, so_far, False)
            acc[...] = acc[...] + mix
            for h in range(heads):
                mass[h] = mass[h] + weights[h]
                carry[h] = so_far[h] + totals[h]

        return 0

    lax.fori_loop(1, me + 1, earlier, 0)
    mixed = acc[...]
    squares = mixed * mixed
    inverse = jnp.zeros_like(mixed)
    for h in range(heads):
        mean = jnp.sum(jnp.where(lane == h, squares, 0.0), axis=1, keepdims=True) / hd
        inverse = jnp.where(lane == h, lax.rsqrt(mean + norm_eps), inverse)
    gain = jnp.concatenate([gain_ref[h : h + 1, :] for h in range(heads)], axis=1)
    out_ref[...] = (mixed * inverse * gain).astype(BF16)
    for h in range(heads):
        log_ref[h : h + 1, :] = jnp.log(jnp.sum(jnp.transpose(mass[h]), axis=0, keepdims=True))


def attention(q, pair, head_gain, near, after):
    rows, width = q.shape
    heads = head_gain.shape[0]
    return pl.pallas_call(
        attention_kernel,
        out_shape=(shape((rows, width)), shape((heads, rows), F32)),
        in_specs=[VM] * 6 + [ANY],
        out_specs=[VM] * 2,
        scratch_shapes=[
            pltpu.VMEM((rows, width), F32),
            pltpu.VMEM((heads, rows, rows), F32),
            pltpu.VMEM((heads, rows, rows), F32),
        ],
        cost_estimate=cost(400_000_000, 1_000_000),
        compiler_params=params(),
        name="stick_attention",
    )(q, pair, head_gain, *near, after)


def heads_part(act, wa, aw, at):
    w = jnp.concatenate([ref[:aw, at] for ref in wa], axis=0)
    return dot_f32(jnp.concatenate([ref[:, :aw] for ref in act], axis=1), w)


def begin_kernel(act0, act1, wa0, wa1, out_ref):
    aw = wa0.shape[0] - 16
    for first in range(0, out_ref.shape[1], CHUNK):
        at = slice(first, first + CHUNK)
        out_ref[:, at] = heads_part((act0, act1), (wa0, wa1), aw, at)


def begin(act0, act1, wa0, wa1):
    rows, width = act0.shape[0], wa0.shape[1]
    return pl.pallas_call(
        begin_kernel,
        out_shape=shape((rows, width), F32),
        in_specs=[VM] * 4,
        out_specs=VM,
        cost_estimate=cost(130_000_000, 2_000_000),
        compiler_params=params(),
        name="begin_rows",
    )(act0, act1, wa0, wa1)


def final_kernel(*refs):
    act, wa, wc, begun, gain_ref, out_ref, mix = refs[:4], refs[4:8], refs[8:14], *refs[14:]
    cw = wc[0].shape[0]
    aw = act[0].shape[1] - cw
    convs = [c[:, aw:].astype(F32) for c in act]
    mean = sum(jnp.sum(v, axis=1, keepdims=True) for v in convs) / (4 * cw)
    centered = [v - mean for v in convs]
    spread = sum(jnp.sum(v * v, axis=1, keepdims=True) for v in centered) / (4 * cw)
    inverse = lax.rsqrt(spread + norm_eps)
    ys = []
    for slot in range(4):
        pieces = [wa[slot][aw : aw + 1, n * cw : (n + 1) * cw].astype(F32) for n in range(6)]
        gain = pieces[0] + pieces[1] + pieces[2]
        bias = pieces[3] + pieces[4] + pieces[5]
        y = centered[slot] * inverse * gain + bias
        ys.append((y * jax.nn.sigmoid(y)).astype(BF16))
    swap = lax.axis_index("grp") == 1
    rows, width = mix.shape
    half = width // 2
    squares = jnp.zeros((rows, 1), F32)
    for first in range(0, width, CHUNK):
        at = slice(first, first + CHUNK)
        part = begun[:, at]
        for slot in range(4):
            if slot < 2:
                w = wc[slot][:, at]
            else:
                pair = wc[2 * slot - 2], wc[2 * slot - 1]
                near, far = pair if first < half else pair[::-1]
                inner = slice(first % half, first % half + CHUNK)
                w = jnp.where(swap, far[:, inner], near[:, inner])
            one = dot_f32(ys[slot], w)
            part = part + one
        part = part + heads_part(act[2:], wa[2:], aw, at)
        mix[:, at] = part
        squares = squares + jnp.sum(part * part, axis=1, keepdims=True)
    out_ref[...] = (mix[...] * lax.rsqrt(squares / width + norm_eps) * gain_ref[...]).astype(BF16)


CHUNK = 256


def finish(act, wa, wc, begun, out_gain):
    rows, width = act[0].shape[0], wa[0].shape[1]
    return pl.pallas_call(
        final_kernel,
        out_shape=shape((rows, width)),
        in_specs=[VM] * 16,
        out_specs=VM,
        scratch_shapes=[pltpu.VMEM((rows, width), F32)],
        cost_estimate=cost(800_000_000, 7_000_000),
        compiler_params=params(32),
        name="finish_rows",
    )(*act, *wa, *wc, begun, out_gain.reshape(1, width))


def paired(
    tokens,
    norm_gain,
    w_query,
    w_key,
    w_value,
    w_glu_value,
    w_glu_gate,
    key_offset,
    head_gain,
    conv_taps,
    channel_gain,
    channel_bias,
    w_out_attn,
    w_out_conv,
    out_gain,
):
    own_qkv, half_qkv = pack_qkv((w_query, w_key, w_value))
    qkv_same = exchange(half_qkv, "sp", 1)
    x_send, mine_own, mine_pair, wc_half = norm_parts(tokens, norm_gain, w_query.shape[0], w_out_conv)
    wc_x = exchange(wc_half, "tp", 2)
    wc_y = exchange(wc_x, "grp", 1)
    wc_yc = exchange(wc_y, "tp", 1)
    x_got = exchange(x_send, "sp", 2)
    own_gv, half_gv, own_gg, wa_mine, off, head_rows = pack(
        w_glu_value, w_glu_gate, w_out_attn, key_offset.T, head_gain, channel_gain, channel_bias
    )
    qkv_same, half_gv = lax.optimization_barrier((qkv_same, half_gv))
    gv_same = exchange(half_gv, "sp", 1)
    gg_pair = exchange(own_gg, "sp", 1)
    gv_other = exchange(gv_same, "grp", 1)
    qkv_other = exchange(qkv_same, "grp", 1)
    x_other = exchange(x_got, "tp", 1)
    wa_x = exchange(wa_mine, "tp", 2)
    wc_core = exchange(w_out_conv, "tp", 1)
    wa_core = exchange(wa_mine, "tp", 1)
    wc_xc = exchange(wc_x, "tp", 1)
    wa_xc = exchange(wa_x, "tp", 1)
    x_own, x_pair = assemble(mine_own, mine_pair, x_got, x_other)

    keep, sent = project_qkv(x_own, x_pair, own_qkv, qkv_same, qkv_other, off)
    got = exchange(sent, "sp", 2)
    tail_rows = -(-conv_taps.shape[0] // 16) * 16
    glu_keep, glu_sent, own_tail, cross_tail = project_glu(
        x_own, x_pair, (own_gv, own_gg), (gv_same, gv_other, gg_pair), tail_rows, sent
    )
    glu_got = exchange(glu_sent, "sp", 2)
    tail_near = from_behind(own_tail, "sp", 1)
    tail_far = from_cross_behind(cross_tail, "sp")
    q, mine_two = sum_qkv(keep, got, sent, glu_sent)
    pair_two = exchange(mine_two, "sp", 1)
    near = near_attention(q, mine_two, head_rows, mine_two)
    attended, log_mass = attention(q, pair_two, head_rows, near, mine_two)
    act_mine = conv(glu_keep, glu_got, tail_near, tail_far, conv_taps, attended)
    act_x = exchange(act_mine, "tp", 2)
    act_core = exchange(act_mine, "tp", 1)
    act = (act_mine, act_core, act_x, exchange(act_x, "tp", 1))
    wa = (wa_mine, wa_core, wa_x, wa_xc)
    wc = (w_out_conv, wc_core, wc_x, wc_y, wc_xc, wc_yc)
    begun = begin(act_mine, act_core, wa_mine, wa_core)
    mixed = finish(act, wa, wc, begun, out_gain)
    return (mixed, log_mass)


def gathered(
    tokens,
    norm_gain,
    w_query,
    w_key,
    w_value,
    w_glu_value,
    w_glu_gate,
    key_offset,
    head_gain,
    conv_taps,
    channel_gain,
    channel_bias,
    w_out_attn,
    w_out_conv,
    out_gain,
):
    row_count = tokens.shape[0]
    hd = head_gain.shape[1]
    channels = conv_taps.shape[1] * lax.axis_size("tp")
    normed = row_norm(tokens.astype(jnp.float32), norm_gain).astype(jnp.bfloat16)
    weights_in = (w_query, w_key, w_value, w_glu_value, w_glu_gate)
    pieces = (
        lax.all_gather(weights_in[0], "sp", axis=0, tiled=True),
        lax.all_gather(weights_in[1], "sp", axis=0, tiled=True),
        lax.all_gather(weights_in[2], "sp", axis=0, tiled=True),
        lax.all_gather(weights_in[3], "sp", axis=0, tiled=True),
        lax.all_gather(weights_in[4], "sp", axis=0, tiled=True),
    )
    projected = tuple(
        (jnp.dot(normed, shard_piece, preferred_element_type=jnp.float32) for shard_piece in pieces)
    )
    query, key_rows, value_rows, glu_value, glu_gate = [
        summed.astype(jnp.bfloat16) for summed in projected
    ]
    kv_local = key_rows.shape[1] // hd
    group_size = query.shape[1] // key_rows.shape[1]
    heads_local = kv_local * group_size
    all_keys, all_values, all_offsets = (
        lax.all_gather(key_rows, "sp", axis=0, tiled=True),
        lax.all_gather(value_rows, "sp", axis=0, tiled=True),
        lax.all_gather(key_offset, "sp", axis=0, tiled=True),
    )
    sequence_length_total = all_keys.shape[0]
    shard_count = lax.axis_size("sp")
    per_block = 1
    while (
        per_block * 2 <= shard_count
        and shard_count % (per_block * 2) == 0
        and (per_block * 2 * row_count <= 1024)
    ):
        per_block = per_block * 2
    span_len = per_block * row_count
    query_heads = query.reshape(row_count, kv_local, group_size, hd)
    key_heads = all_keys.reshape(sequence_length_total, kv_local, hd)
    value_heads = all_values.reshape(sequence_length_total, kv_local, hd)
    my_index = lax.axis_index("sp")
    query_pos = my_index * row_count + jnp.arange(row_count, dtype=jnp.int32)
    last_block = my_index // per_block
    zeros_mix = jnp.zeros((kv_local, group_size, row_count, hd), jnp.float32)
    zeros_row = jnp.zeros((kv_local, group_size, row_count), jnp.float32)

    def sweep(turn_index, carry):
        head_mix, mass_sum, carried = carry
        first_key = (last_block - turn_index) * span_len
        key_block = lax.dynamic_slice_in_dim(key_heads, first_key, span_len, 0)
        value_block = lax.dynamic_slice_in_dim(value_heads, first_key, span_len, 0)
        offset_block = lax.dynamic_slice_in_dim(all_offsets, first_key, span_len, 0).astype(
            jnp.float32
        )
        offset_block = offset_block.T.reshape(kv_local, group_size, 1, span_len)
        scores = (
            jnp.einsum("qhgd,khd->hgqk", query_heads, key_block, preferred_element_type=jnp.float32)
            * hd ** (-0.5)
            + offset_block
        )
        key_pos = first_key + jnp.arange(span_len, dtype=jnp.int32)
        allowed = key_pos[None, :] <= query_pos[:, None]
        log_not = jnp.where(allowed, jax.nn.log_sigmoid(-scores), 0.0)
        later = lax.cumsum(log_not, axis=3, reverse=True) - log_not + carried[..., None]
        weights = jnp.where(allowed, jnp.exp(jax.nn.log_sigmoid(scores) + later), 0.0)
        head_mix = head_mix + jnp.einsum(
            "hgqk,khd->hgqd",
            weights.astype(jnp.bfloat16),
            value_block,
            preferred_element_type=jnp.float32,
        )
        return (head_mix, mass_sum + jnp.sum(weights, axis=3), carried + jnp.sum(log_not, axis=3))

    head_mix, mass_sum, _ = lax.fori_loop(
        0, last_block + 1, sweep, (zeros_mix, zeros_row, zeros_row)
    )
    log_mass = jnp.log(mass_sum).reshape(heads_local, row_count)
    head_rows = head_mix.transpose(2, 0, 1, 3).reshape(row_count, heads_local, hd)
    attended = (
        row_norm(head_rows, head_gain).astype(jnp.bfloat16).reshape(row_count, heads_local * hd)
    )
    gated = (glu_value.astype(jnp.float32) * jax.nn.sigmoid(glu_gate.astype(jnp.float32))).astype(
        jnp.bfloat16
    )
    reach_len = conv_taps.shape[0] - 1
    before = from_behind(gated[row_count - reach_len :], "sp", 1)
    padded = jnp.concatenate([before, gated], axis=0).astype(jnp.float32)
    conv_out = jnp.zeros(gated.shape, jnp.float32)
    for tap_index in range(conv_taps.shape[0]):
        conv_out = conv_out + conv_taps[tap_index] * padded[tap_index : tap_index + row_count]
    total_sum, total_squares = lax.psum(
        (jnp.sum(conv_out, axis=1), jnp.sum(conv_out * conv_out, axis=1)), "tp"
    )
    chan_mean = (total_sum / channels)[:, None]
    spread = (total_squares / channels)[:, None] - chan_mean * chan_mean
    centered = conv_out - chan_mean
    channel_out = jax.nn.silu(
        centered * lax.rsqrt(spread + norm_eps) * channel_gain + channel_bias
    ).astype(jnp.bfloat16)
    share = lax.psum_scatter(
        jnp.dot(attended, w_out_attn, preferred_element_type=jnp.float32)
        + jnp.dot(channel_out, w_out_conv, preferred_element_type=jnp.float32),
        "tp",
        scatter_dimension=0,
        tiled=True,
    )
    mixed = lax.all_gather(row_norm(share, out_gain).astype(jnp.bfloat16), "tp", axis=0, tiled=True)
    return (mixed, log_mass)


def solution(mesh):
    in_specs = (
        P(("grp", "sp"), None),
        P(),
        P("sp", "tp"),
        P("sp", "tp"),
        P("sp", "tp"),
        P("sp", "tp"),
        P("sp", "tp"),
        P(("grp", "sp"), "tp"),
        P("tp", None),
        P(None, "tp"),
        P("tp"),
        P("tp"),
        P("tp", None),
        P("tp", None),
        P(),
    )
    out_specs = (P(("grp", "sp"), None), P("tp", ("grp", "sp")))
    small = mesh.shape["sp"] == 4 and mesh.shape["tp"] == 4 and mesh.shape["grp"] == 2
    local = paired if small else gathered
    return jax.shard_map(local, mesh=mesh, in_specs=in_specs, out_specs=out_specs, check_vma=False)
```

```python
import jax
import jax.numpy as jnp
from jax import lax
from jax.experimental import pallas as pl
from jax.experimental.pallas import tpu as pltpu
from jax.sharding import PartitionSpec as P

norm_eps = 1e-06
BF16 = jnp.bfloat16
F32 = jnp.float32


def exchange(value, axis, bit):
    count = lax.axis_size(axis)
    return lax.ppermute(value, axis, [(s, s ^ bit) for s in range(count)])


def from_cross_behind(value, axis):
    count = lax.axis_size(axis)
    pairs = [(source, (source ^ 2) + 1) for source in range(count)]
    return lax.ppermute(value, axis, [(a, b) for a, b in pairs if b < count])


def from_behind(value, axis, steps):
    count = lax.axis_size(axis)
    initial, last = (max(0, -steps), min(count, count - steps))
    return lax.ppermute(value, axis, [(source, source + steps) for source in range(initial, last)])


def row_norm(values_in, gain_vec):
    squares = jnp.mean(values_in * values_in, axis=-1, keepdims=True)
    return values_in * lax.rsqrt(squares + norm_eps) * gain_vec


def dot_f32(a, b, dims=((1,), (0,))):
    return lax.dot_general(a, b, (dims, ((), ())), preferred_element_type=F32)


def params(limit=16):
    return pltpu.CompilerParams(vmem_limit_bytes=limit * 1024 * 1024)


VM = pl.BlockSpec(memory_space=pltpu.VMEM)
ANY = pl.BlockSpec(memory_space=pl.ANY)
HBM = pl.BlockSpec(memory_space=pltpu.HBM)


def shape(dims, dtype=BF16):
    return jax.ShapeDtypeStruct(dims, dtype)


def cost(flops, moved):
    return pl.CostEstimate(flops=flops, bytes_accessed=moved, transcendentals=0)


def in_hbm(*values):
    return [pltpu.with_memory_space_constraint(v, pltpu.HBM) for v in values]


def pack_qkv_kernel(wq, wk, wv, all_ref, send_ref, sems):
    part, width = send_ref.shape[0], wq.shape[1]
    mine = pl.ds(pl.multiple_of(lax.axis_index("grp") * part, part), part)
    first, rest = [], []
    for n, w in enumerate((wq, wk, wv)):
        at = slice(n * width, (n + 1) * width)
        first.append(pltpu.make_async_copy(w.at[mine, :], send_ref.at[:, at], sems.at[n]))
        rest.append(pltpu.make_async_copy(w, all_ref.at[:, at], sems.at[3 + n]))
    for copy in first + rest:
        copy.start()
    for copy in first + rest:
        copy.wait()


def pack_qkv(weights):
    block, width = weights[0].shape
    return pl.pallas_call(
        pack_qkv_kernel,
        out_shape=(shape((block, 3 * width)), shape((block // 2, 3 * width))),
        in_specs=[HBM] * 3,
        out_specs=[VM] * 2,
        scratch_shapes=[pltpu.SemaphoreType.DMA((6,))],
        cost_estimate=cost(2_000_000, 400_000),
        compiler_params=params(),
        name="pack_qkv",
    )(*in_hbm(*weights))


def norm_kernel(x_hbm, gain_hbm, wc_hbm, send_ref, own_ref, pair_ref, wc_ref, x_ref, gain_ref, normed, sems):
    side, low = lax.axis_index("sp") // 2, lax.axis_index("sp") % 2
    core = lax.axis_index("tp") % 2
    block = own_ref.shape[1]
    half = 2 * block
    half_rows = send_ref.shape[0]
    columns = wc_ref.shape[1]
    mine = pl.ds(pl.multiple_of(lax.axis_index("grp") * columns, columns), columns)
    copies = [
        pltpu.make_async_copy(x_hbm, x_ref, sems.at[0]),
        pltpu.make_async_copy(gain_hbm, gain_ref, sems.at[1]),
        pltpu.make_async_copy(wc_hbm.at[:, mine], wc_ref, sems.at[2]),
    ]
    for copy in copies:
        copy.start()
    for copy in copies[:2]:
        copy.wait()
    x = x_ref[...].astype(F32)
    squares = jnp.mean(x * x, axis=1, keepdims=True)
    normed[...] = (x * lax.rsqrt(squares + norm_eps) * gain_ref[...]).astype(BF16)
    first = pl.multiple_of(core * half_rows, half_rows)
    away = pl.multiple_of((1 - side) * half, half)
    send_ref[...] = normed[pl.ds(first, half_rows), pl.ds(away, half)]
    own_ref[...] = normed[:, pl.ds(pl.multiple_of(side * half + low * block, block), block)]
    pair_ref[...] = normed[:, pl.ds(pl.multiple_of(side * half + (1 - low) * block, block), block)]
    copies[2].wait()


def norm_parts(tokens, gain, block, wc):
    rows, features = tokens.shape
    return pl.pallas_call(
        norm_kernel,
        out_shape=(
            shape((rows // 2, 2 * block)),
            shape((rows, block)),
            shape((rows, block)),
            shape((wc.shape[0], wc.shape[1] // 2)),
        ),
        in_specs=[HBM] * 3,
        out_specs=[VM] * 4,
        scratch_shapes=[
            pltpu.VMEM((rows, features), BF16),
            pltpu.VMEM((1, features), F32),
            pltpu.VMEM((rows, features), BF16),
            pltpu.SemaphoreType.DMA((3,)),
        ],
        cost_estimate=cost(2_000_000, 1_000_000),
        compiler_params=params(),
        name="norm_parts",
    )(*in_hbm(tokens, gain.reshape(1, features), wc))


def pack_kernel(
    gv_hbm, gg_hbm, wa_hbm, off_hbm, head_hbm, gain_hbm, bias_hbm, *refs
):
    gv_ref, gv_send, gg_ref, out_ref, off_ref, head_ref, gain_ref, bias_ref, sems = refs
    cw, aw = gv_hbm.shape[1], wa_hbm.shape[0]
    part = gv_send.shape[0]
    mine = pl.ds(pl.multiple_of(lax.axis_index("grp") * part, part), part)
    pairs = (
        (gain_hbm, gain_ref),
        (bias_hbm, bias_ref),
        (gv_hbm.at[mine, :], gv_send),
        (gg_hbm, gg_ref),
        (wa_hbm, out_ref.at[:aw, :]),
        (off_hbm, off_ref),
        (head_hbm, head_ref),
        (gv_hbm, gv_ref),
    )
    copies = [pltpu.make_async_copy(a, b, sems.at[n]) for n, (a, b) in enumerate(pairs)]
    for copy in copies:
        copy.start()
    for copy in copies[:2]:
        copy.wait()
    extra = out_ref.shape[0] - aw
    for n, ref in enumerate((gain_ref, bias_ref)):
        rest = ref[...]
        for piece in range(3):
            part = rest.astype(BF16)
            rest = rest - part.astype(F32)
            first = (3 * n + piece) * cw
            out_ref[aw:, first : first + cw] = jnp.broadcast_to(part, (extra, cw))
    for copy in copies[2:]:
        copy.wait()


def pack(gv, gg, wa, off, head_gain, gain, bias):
    block, cw = gv.shape
    aw, width = wa.shape
    return pl.pallas_call(
        pack_kernel,
        out_shape=(
            shape((block, cw)),
            shape((block // 2, cw)),
            shape((block, cw)),
            shape((aw + 16, width)),
            shape(off.shape),
            shape(head_gain.shape, F32),
        ),
        in_specs=[HBM] * 7,
        out_specs=[VM] * 6,
        scratch_shapes=[
            pltpu.VMEM((1, cw), F32),
            pltpu.VMEM((1, cw), F32),
            pltpu.SemaphoreType.DMA((8,)),
        ],
        cost_estimate=cost(2_000_000, 2_000_000),
        compiler_params=params(),
        name="pack",
    )(*in_hbm(gv, gg, wa, off, head_gain, gain.reshape(1, cw), bias.reshape(1, cw)))


def assemble_kernel(own_ref, pair_ref, got_ref, other_ref, own_out, pair_out):
    low = lax.axis_index("sp") % 2
    core = lax.axis_index("tp") % 2
    rows, block = own_ref.shape
    half = got_ref.shape[0]
    own_out[:rows, :] = own_ref[...]
    pair_out[:rows, :] = pair_ref[...]
    own_at = pl.multiple_of(low * block, block)
    pair_at = pl.multiple_of((1 - low) * block, block)
    for part, at in ((got_ref, core), (other_ref, 1 - core)):
        first = pl.multiple_of(rows + at * half, half)
        own_out[pl.ds(first, half), :] = part[:, pl.ds(own_at, block)]
        pair_out[pl.ds(first, half), :] = part[:, pl.ds(pair_at, block)]


def assemble(own, pair, got, other):
    rows, block = own.shape
    return pl.pallas_call(
        assemble_kernel,
        out_shape=(shape((2 * rows, block)),) * 2,
        in_specs=[VM] * 4,
        out_specs=[VM] * 2,
        cost_estimate=cost(2_000_000, 1_000_000),
        compiler_params=params(),
        name="assemble",
    )(own, pair, got, other)


def far_dot(x_pair, same, other):
    part = same.shape[0]
    group = lax.axis_index("grp")
    near = x_pair[:, pl.ds(pl.multiple_of(group * part, part), part)]
    rest = x_pair[:, pl.ds(pl.multiple_of((1 - group) * part, part), part)]
    return dot_f32(near, same[...]) + dot_f32(rest, other[...])


def qkv_kernel(x_own, x_pair, own, same, other, off_ref, keep_ref, send_ref):
    rows = x_own.shape[0] // 2
    width = send_ref.shape[1]
    total = dot_f32(x_own[...], own[...]) + far_dot(x_pair, same, other)
    keep_ref[...] = total
    for n in range(3):
        part = total[:, n * width : (n + 1) * width].astype(BF16)
        first = 4 * rows if n == 0 else 2 * (n - 1) * rows
        send_ref[first : first + rows, :] = part[rows:]
        if n > 0:
            send_ref[first + rows : first + 2 * rows, :] = part[:rows]
    send_ref[5 * rows :, :] = jnp.zeros((send_ref.shape[0] - 5 * rows, width), BF16)
    send_ref[5 * rows : 5 * rows + off_ref.shape[0], :] = off_ref[...]


def project_qkv(x_own, x_pair, own, same, other, off):
    rows, width = x_own.shape[0], own.shape[1] // 3
    return pl.pallas_call(
        qkv_kernel,
        out_shape=(shape((rows, 3 * width), F32), shape((5 * rows // 2 + 16, width))),
        in_specs=[VM] * 6,
        out_specs=[VM] * 2,
        cost_estimate=cost(200_000_000, 1_000_000),
        compiler_params=params(),
        name="project_qkv",
    )(x_own, x_pair, own, same, other, off)


def sum_kernel(keep_ref, got_ref, sent_ref, after, q_ref, out_ref):
    rows, width = q_ref.shape

    def got(n):
        return got_ref[n * rows : (n + 1) * rows, :].astype(F32)

    q_ref[...] = (keep_ref[:rows, :width] + got(4)).astype(BF16)
    for n in range(4):
        at = slice((1 + n // 2) * width, (2 + n // 2) * width)
        part = keep_ref[(n % 2) * rows : (n % 2 + 1) * rows, at]
        out_ref[n * rows : (n + 1) * rows, :] = (part + got(n)).astype(BF16)
    first = 5 * rows
    out_ref[4 * rows :, :] = jnp.concatenate([sent_ref[first : first + 8, :], got_ref[first : first + 8, :]])


def sum_qkv(keep, got, sent, after):
    rows, width = keep.shape[0] // 2, got.shape[1]
    return pl.pallas_call(
        sum_kernel,
        out_shape=(shape((rows, width)), shape((4 * rows + 16, width))),
        in_specs=[VM] * 3 + [ANY],
        out_specs=[VM] * 2,
        cost_estimate=cost(1_000_000, 1_000_000),
        compiler_params=params(),
        name="sum_qkv",
    )(keep, got, sent, after)


def glu_kernel(x_own, x_pair, gv, gg, gv_same, gv_other, gg_pair, after, keep_ref, send_ref, own_tail, far_tail):
    rows = x_own.shape[0] // 2
    tail, cw = own_tail.shape[0], gv.shape[1]
    for n in range(2):
        own = (gv, gg)[n]
        far = far_dot(x_pair, gv_same, gv_other) if n == 0 else dot_f32(x_pair[...], gg_pair[...])
        total = dot_f32(x_own[...], own[...]) + far
        at = slice(n * cw, (n + 1) * cw)
        keep_ref[:, at] = total[:rows]
        send_ref[:, at] = total[rows:].astype(BF16)
        own_tail[:, at] = total[rows - tail : rows].astype(BF16)
        far_tail[:, at] = total[2 * rows - tail :].astype(BF16)


def project_glu(x_own, x_pair, own, pair, tail, after):
    rows, width = x_own.shape[0] // 2, 2 * own[0].shape[1]
    return pl.pallas_call(
        glu_kernel,
        out_shape=(
            shape((rows, width), F32),
            shape((rows, width)),
            shape((tail, width)),
            shape((tail, width)),
        ),
        in_specs=[VM] * 7 + [ANY],
        out_specs=[VM] * 4,
        cost_estimate=cost(270_000_000, 1_000_000),
        compiler_params=params(),
        name="project_glu",
    )(x_own, x_pair, *own, *pair, after)


def conv_kernel(keep_ref, got_ref, near_ref, far_ref, taps_ref, att_ref, act_ref, padded):
    rows, aw = att_ref.shape
    tail, cw = near_ref.shape[0], taps_ref.shape[1]
    taps = taps_ref.shape[0]

    def gated(glu):
        value = glu[:, :cw].astype(BF16).astype(F32)
        gate = glu[:, cw:].astype(BF16).astype(F32)
        return (value * jax.nn.sigmoid(gate)).astype(BF16).astype(F32)

    padded[:tail, :] = gated(near_ref[...].astype(F32) + far_ref[...].astype(F32))
    padded[tail:, :] = gated(keep_ref[...] + got_ref[...].astype(F32))
    total = None
    for tap in range(taps):
        first = tail - (taps - 1) + tap
        part = taps_ref[tap : tap + 1, :] * padded[first : first + rows, :]
        total = part if total is None else total + part
    act_ref[:, :aw] = att_ref[...]
    act_ref[:, aw:] = total.astype(BF16)


def conv(keep, got, near, far, taps, attended):
    rows, cw = keep.shape[0], taps.shape[1]
    return pl.pallas_call(
        conv_kernel,
        out_shape=shape((rows, attended.shape[1] + cw)),
        in_specs=[VM] * 6,
        out_specs=VM,
        scratch_shapes=[pltpu.VMEM((rows + near.shape[0], cw), F32)],
        cost_estimate=cost(20_000_000, 500_000),
        compiler_params=params(),
        name="conv",
    )(keep, got, near, far, taps, attended)


def suffix_matrix(keys):
    before = lax.broadcasted_iota(jnp.int32, (2 * keys, 2 * keys), 0) % keys
    column = lax.broadcasted_iota(jnp.int32, (2 * keys, 2 * keys), 1)
    return jnp.where((column >= keys) | (before > column), 1.0, 0.0).astype(BF16)


def stick_block(q, k, v, off, hd, suffix, carry, diagonal):
    rows, width = q.shape
    keys = k.shape[0]
    lane = lax.broadcasted_iota(jnp.int32, (rows, width), 1) // hd
    offsets = off.astype(F32)
    weights, totals, values = [], [], []
    for h in range(width // hd):
        qh = jnp.where(lane == h, q, jnp.zeros_like(q))
        s = dot_f32(qh, k, ((1,), (1,))) * hd ** (-0.5) + offsets[h : h + 1, :]
        soft = jnp.maximum(s, 0.0) + jnp.log(1.0 + jnp.exp(-jnp.abs(s)))
        log_not = -soft
        if diagonal:
            allowed = lax.broadcasted_iota(jnp.int32, (rows, keys), 1) <= lax.broadcasted_iota(
                jnp.int32, (rows, keys), 0
            )
            log_not = jnp.where(allowed, log_not, 0.0)
        high = log_not.astype(BF16)
        low = (log_not - high.astype(F32)).astype(BF16)
        sums = dot_f32(jnp.concatenate([high, low], axis=1), suffix)
        later = sums[:, :keys]
        if carry is not None:
            later = later + carry[h]
        w = jnp.exp(s - soft + later)
        if diagonal:
            w = jnp.where(allowed, w, 0.0)
        weights.append(w)
        totals.append(sums[:, keys:])
        values.append(jnp.where(lane == h, v, jnp.zeros_like(v)))
    mix = dot_f32(
        jnp.concatenate([w.astype(BF16) for w in weights], axis=1), jnp.concatenate(values, axis=0)
    )
    return mix, weights, totals


def near_kernel(q_ref, mine_ref, gain_ref, after, mix_ref, mass_ref, carry_ref):
    rows = q_ref.shape[0]
    heads, hd = gain_ref.shape
    suffix = suffix_matrix(rows)
    for n in range(2):
        k = mine_ref[n * rows : (n + 1) * rows, :]
        v = mine_ref[(2 + n) * rows : (3 + n) * rows, :]
        off = mine_ref[4 * rows + 8 * n : 4 * rows + 8 * n + 8, :]
        mix, weights, totals = stick_block(q_ref[...], k, v, off, hd, suffix, None, n == 0)
        mix_ref[n] = mix
        for h in range(heads):
            mass_ref[n * heads + h] = weights[h]
            carry_ref[n * heads + h] = totals[h]


def near_attention(q, mine, head_gain, after):
    rows, width = q.shape
    heads = head_gain.shape[0]
    return pl.pallas_call(
        near_kernel,
        out_shape=(
            shape((2, rows, width), F32),
            shape((2 * heads, rows, rows), F32),
            shape((2 * heads, rows, rows), F32),
        ),
        in_specs=[VM] * 3 + [ANY],
        out_specs=[VM] * 3,
        cost_estimate=cost(200_000_000, 1_000_000),
        compiler_params=params(),
        name="near_attention",
    )(q, mine, head_gain, after)


def attention_kernel(q_ref, pair_ref, gain_ref, mix_ref, mass_ref, carry_ref, after, out_ref, log_ref, acc, mass, carry):
    me = lax.axis_index("sp")
    rows, width = q_ref.shape
    heads, hd = gain_ref.shape
    lane = lax.broadcasted_iota(jnp.int32, (rows, width), 1) // hd
    suffix = suffix_matrix(rows)
    acc[...] = mix_ref[0]
    for h in range(heads):
        mass[h] = mass_ref[h]
        carry[h] = carry_ref[h]

    def earlier(t, _):
        slot = jnp.bitwise_xor(me - t, me)

        @pl.when(slot == 2)
        def _():
            scale = jnp.zeros_like(acc)
            for h in range(heads):
                left = jnp.exp(carry[h])
                mass[h] = mass[h] + left * mass_ref[heads + h]
                scale = jnp.where(lane == h, left, scale)
                carry[h] = carry[h] + carry_ref[heads + h]
            acc[...] = acc[...] + scale * mix_ref[1]

        @pl.when(slot != 2)
        def _():
            n = slot // 2
            k = pair_ref[pl.ds(pl.multiple_of(n * rows, rows), rows), :]
            v = pair_ref[pl.ds(pl.multiple_of((2 + n) * rows, rows), rows), :]
            off = jnp.where(
                n == 0,
                pair_ref[4 * rows : 4 * rows + 8, :].astype(F32),
                pair_ref[4 * rows + 8 : 4 * rows + 16, :].astype(F32),
            )
            so_far = [carry[h] for h in range(heads)]
            mix, weights, totals = stick_block(q_ref[...], k, v, off, hd, suffix, so_far, False)
            acc[...] = acc[...] + mix
            for h in range(heads):
                mass[h] = mass[h] + weights[h]
                carry[h] = so_far[h] + totals[h]

        return 0

    lax.fori_loop(1, me + 1, earlier, 0)
    mixed = acc[...]
    squares = mixed * mixed
    inverse = jnp.zeros_like(mixed)
    for h in range(heads):
        mean = jnp.sum(jnp.where(lane == h, squares, 0.0), axis=1, keepdims=True) / hd
        inverse = jnp.where(lane == h, lax.rsqrt(mean + norm_eps), inverse)
    gain = jnp.concatenate([gain_ref[h : h + 1, :] for h in range(heads)], axis=1)
    out_ref[...] = (mixed * inverse * gain).astype(BF16)
    for h in range(heads):
        log_ref[h : h + 1, :] = jnp.log(jnp.sum(jnp.transpose(mass[h]), axis=0, keepdims=True))


def attention(q, pair, head_gain, near, after):
    rows, width = q.shape
    heads = head_gain.shape[0]
    return pl.pallas_call(
        attention_kernel,
        out_shape=(shape((rows, width)), shape((heads, rows), F32)),
        in_specs=[VM] * 6 + [ANY],
        out_specs=[VM] * 2,
        scratch_shapes=[
            pltpu.VMEM((rows, width), F32),
            pltpu.VMEM((heads, rows, rows), F32),
            pltpu.VMEM((heads, rows, rows), F32),
        ],
        cost_estimate=cost(400_000_000, 1_000_000),
        compiler_params=params(),
        name="stick_attention",
    )(q, pair, head_gain, *near, after)


def heads_part(act, wa, aw, at):
    w = jnp.concatenate([ref[:aw, at] for ref in wa], axis=0)
    return dot_f32(jnp.concatenate([ref[:, :aw] for ref in act], axis=1), w)


def begin_kernel(act0, act1, wa0, wa1, out_ref):
    aw = wa0.shape[0] - 16
    for first in range(0, out_ref.shape[1], CHUNK):
        at = slice(first, first + CHUNK)
        out_ref[:, at] = heads_part((act0, act1), (wa0, wa1), aw, at)


def begin(act0, act1, wa0, wa1):
    rows, width = act0.shape[0], wa0.shape[1]
    return pl.pallas_call(
        begin_kernel,
        out_shape=shape((rows, width), F32),
        in_specs=[VM] * 4,
        out_specs=VM,
        cost_estimate=cost(130_000_000, 2_000_000),
        compiler_params=params(),
        name="begin_rows",
    )(act0, act1, wa0, wa1)


def final_kernel(*refs):
    act, wa, wc, begun, gain_ref, out_ref, mix = refs[:4], refs[4:8], refs[8:14], *refs[14:]
    cw = wc[0].shape[0]
    aw = act[0].shape[1] - cw
    convs = [c[:, aw:].astype(F32) for c in act]
    mean = sum(jnp.sum(v, axis=1, keepdims=True) for v in convs) / (4 * cw)
    centered = [v - mean for v in convs]
    spread = sum(jnp.sum(v * v, axis=1, keepdims=True) for v in centered) / (4 * cw)
    inverse = lax.rsqrt(spread + norm_eps)
    ys = []
    for slot in range(4):
        pieces = [wa[slot][aw : aw + 1, n * cw : (n + 1) * cw].astype(F32) for n in range(6)]
        gain = pieces[0] + pieces[1] + pieces[2]
        bias = pieces[3] + pieces[4] + pieces[5]
        y = centered[slot] * inverse * gain + bias
        ys.append((y * jax.nn.sigmoid(y)).astype(BF16))
    group = lax.axis_index("grp")
    rows, width = mix.shape
    half = width // 2
    squares = jnp.zeros((rows, 1), F32)
    for n in range(2):
        base = (group if n == 0 else 1 - group) * half
        for first in range(0, half, CHUNK):
            at = pl.ds(pl.multiple_of(base + first, CHUNK), CHUNK)
            inner = slice(first, first + CHUNK)
            part = begun[:, at]
            for slot in range(4):
                w = wc[slot][:, at] if slot < 2 else wc[2 * slot - 2 + n][:, inner]
                part = part + dot_f32(ys[slot], w)
            part = part + heads_part(act[2:], wa[2:], aw, at)
            mix[:, at] = part
            squares = squares + jnp.sum(part * part, axis=1, keepdims=True)
    out_ref[...] = (mix[...] * lax.rsqrt(squares / width + norm_eps) * gain_ref[...]).astype(BF16)


CHUNK = 256


def finish(act, wa, wc, begun, out_gain):
    rows, width = act[0].shape[0], wa[0].shape[1]
    return pl.pallas_call(
        final_kernel,
        out_shape=shape((rows, width)),
        in_specs=[VM] * 16,
        out_specs=VM,
        scratch_shapes=[pltpu.VMEM((rows, width), F32)],
        cost_estimate=cost(800_000_000, 7_000_000),
        compiler_params=params(32),
        name="finish_rows",
    )(*act, *wa, *wc, begun, out_gain.reshape(1, width))


def paired(
    tokens,
    norm_gain,
    w_query,
    w_key,
    w_value,
    w_glu_value,
    w_glu_gate,
    key_offset,
    head_gain,
    conv_taps,
    channel_gain,
    channel_bias,
    w_out_attn,
    w_out_conv,
    out_gain,
):
    own_qkv, half_qkv = pack_qkv((w_query, w_key, w_value))
    qkv_same = exchange(half_qkv, "sp", 1)
    x_send, mine_own, mine_pair, wc_half = norm_parts(tokens, norm_gain, w_query.shape[0], w_out_conv)
    wc_x = exchange(wc_half, "tp", 2)
    wc_y = exchange(wc_x, "grp", 1)
    wc_yc = exchange(wc_y, "tp", 1)
    x_got = exchange(x_send, "sp", 2)
    own_gv, half_gv, own_gg, wa_mine, off, head_rows = pack(
        w_glu_value, w_glu_gate, w_out_attn, key_offset.T, head_gain, channel_gain, channel_bias
    )
    qkv_same, half_gv = lax.optimization_barrier((qkv_same, half_gv))
    gv_same = exchange(half_gv, "sp", 1)
    gg_pair = exchange(own_gg, "sp", 1)
    gv_other = exchange(gv_same, "grp", 1)
    qkv_other = exchange(qkv_same, "grp", 1)
    x_other = exchange(x_got, "tp", 1)
    wa_x = exchange(wa_mine, "tp", 2)
    wc_core = exchange(w_out_conv, "tp", 1)
    wa_core = exchange(wa_mine, "tp", 1)
    wc_xc = exchange(wc_x, "tp", 1)
    wa_xc = exchange(wa_x, "tp", 1)
    x_own, x_pair = assemble(mine_own, mine_pair, x_got, x_other)

    keep, sent = project_qkv(x_own, x_pair, own_qkv, qkv_same, qkv_other, off)
    got = exchange(sent, "sp", 2)
    tail_rows = -(-conv_taps.shape[0] // 16) * 16
    glu_keep, glu_sent, own_tail, cross_tail = project_glu(
        x_own, x_pair, (own_gv, own_gg), (gv_same, gv_other, gg_pair), tail_rows, sent
    )
    glu_got = exchange(glu_sent, "sp", 2)
    tail_near = from_behind(own_tail, "sp", 1)
    tail_far = from_cross_behind(cross_tail, "sp")
    q, mine_two = sum_qkv(keep, got, sent, glu_sent)
    pair_two = exchange(mine_two, "sp", 1)
    near = near_attention(q, mine_two, head_rows, mine_two)
    attended, log_mass = attention(q, pair_two, head_rows, near, mine_two)
    act_mine = conv(glu_keep, glu_got, tail_near, tail_far, conv_taps, attended)
    act_x = exchange(act_mine, "tp", 2)
    act_core = exchange(act_mine, "tp", 1)
    act = (act_mine, act_core, act_x, exchange(act_x, "tp", 1))
    wa = (wa_mine, wa_core, wa_x, wa_xc)
    wc = (w_out_conv, wc_core, wc_x, wc_y, wc_xc, wc_yc)
    begun = begin(act_mine, act_core, wa_mine, wa_core)
    mixed = finish(act, wa, wc, begun, out_gain)
    return (mixed, log_mass)


def gathered(
    tokens,
    norm_gain,
    w_query,
    w_key,
    w_value,
    w_glu_value,
    w_glu_gate,
    key_offset,
    head_gain,
    conv_taps,
    channel_gain,
    channel_bias,
    w_out_attn,
    w_out_conv,
    out_gain,
):
    row_count = tokens.shape[0]
    hd = head_gain.shape[1]
    channels = conv_taps.shape[1] * lax.axis_size("tp")
    normed = row_norm(tokens.astype(jnp.float32), norm_gain).astype(jnp.bfloat16)
    weights_in = (w_query, w_key, w_value, w_glu_value, w_glu_gate)
    pieces = (
        lax.all_gather(weights_in[0], "sp", axis=0, tiled=True),
        lax.all_gather(weights_in[1], "sp", axis=0, tiled=True),
        lax.all_gather(weights_in[2], "sp", axis=0, tiled=True),
        lax.all_gather(weights_in[3], "sp", axis=0, tiled=True),
        lax.all_gather(weights_in[4], "sp", axis=0, tiled=True),
    )
    projected = tuple(
        (jnp.dot(normed, shard_piece, preferred_element_type=jnp.float32) for shard_piece in pieces)
    )
    query, key_rows, value_rows, glu_value, glu_gate = [
        summed.astype(jnp.bfloat16) for summed in projected
    ]
    kv_local = key_rows.shape[1] // hd
    group_size = query.shape[1] // key_rows.shape[1]
    heads_local = kv_local * group_size
    all_keys, all_values, all_offsets = (
        lax.all_gather(key_rows, "sp", axis=0, tiled=True),
        lax.all_gather(value_rows, "sp", axis=0, tiled=True),
        lax.all_gather(key_offset, "sp", axis=0, tiled=True),
    )
    sequence_length_total = all_keys.shape[0]
    shard_count = lax.axis_size("sp")
    per_block = 1
    while (
        per_block * 2 <= shard_count
        and shard_count % (per_block * 2) == 0
        and (per_block * 2 * row_count <= 1024)
    ):
        per_block = per_block * 2
    span_len = per_block * row_count
    query_heads = query.reshape(row_count, kv_local, group_size, hd)
    key_heads = all_keys.reshape(sequence_length_total, kv_local, hd)
    value_heads = all_values.reshape(sequence_length_total, kv_local, hd)
    my_index = lax.axis_index("sp")
    query_pos = my_index * row_count + jnp.arange(row_count, dtype=jnp.int32)
    last_block = my_index // per_block
    zeros_mix = jnp.zeros((kv_local, group_size, row_count, hd), jnp.float32)
    zeros_row = jnp.zeros((kv_local, group_size, row_count), jnp.float32)

    def sweep(turn_index, carry):
        head_mix, mass_sum, carried = carry
        first_key = (last_block - turn_index) * span_len
        key_block = lax.dynamic_slice_in_dim(key_heads, first_key, span_len, 0)
        value_block = lax.dynamic_slice_in_dim(value_heads, first_key, span_len, 0)
        offset_block = lax.dynamic_slice_in_dim(all_offsets, first_key, span_len, 0).astype(
            jnp.float32
        )
        offset_block = offset_block.T.reshape(kv_local, group_size, 1, span_len)
        scores = (
            jnp.einsum("qhgd,khd->hgqk", query_heads, key_block, preferred_element_type=jnp.float32)
            * hd ** (-0.5)
            + offset_block
        )
        key_pos = first_key + jnp.arange(span_len, dtype=jnp.int32)
        allowed = key_pos[None, :] <= query_pos[:, None]
        log_not = jnp.where(allowed, jax.nn.log_sigmoid(-scores), 0.0)
        later = lax.cumsum(log_not, axis=3, reverse=True) - log_not + carried[..., None]
        weights = jnp.where(allowed, jnp.exp(jax.nn.log_sigmoid(scores) + later), 0.0)
        head_mix = head_mix + jnp.einsum(
            "hgqk,khd->hgqd",
            weights.astype(jnp.bfloat16),
            value_block,
            preferred_element_type=jnp.float32,
        )
        return (head_mix, mass_sum + jnp.sum(weights, axis=3), carried + jnp.sum(log_not, axis=3))

    head_mix, mass_sum, _ = lax.fori_loop(
        0, last_block + 1, sweep, (zeros_mix, zeros_row, zeros_row)
    )
    log_mass = jnp.log(mass_sum).reshape(heads_local, row_count)
    head_rows = head_mix.transpose(2, 0, 1, 3).reshape(row_count, heads_local, hd)
    attended = (
        row_norm(head_rows, head_gain).astype(jnp.bfloat16).reshape(row_count, heads_local * hd)
    )
    gated = (glu_value.astype(jnp.float32) * jax.nn.sigmoid(glu_gate.astype(jnp.float32))).astype(
        jnp.bfloat16
    )
    reach_len = conv_taps.shape[0] - 1
    before = from_behind(gated[row_count - reach_len :], "sp", 1)
    padded = jnp.concatenate([before, gated], axis=0).astype(jnp.float32)
    conv_out = jnp.zeros(gated.shape, jnp.float32)
    for tap_index in range(conv_taps.shape[0]):
        conv_out = conv_out + conv_taps[tap_index] * padded[tap_index : tap_index + row_count]
    total_sum, total_squares = lax.psum(
        (jnp.sum(conv_out, axis=1), jnp.sum(conv_out * conv_out, axis=1)), "tp"
    )
    chan_mean = (total_sum / channels)[:, None]
    spread = (total_squares / channels)[:, None] - chan_mean * chan_mean
    centered = conv_out - chan_mean
    channel_out = jax.nn.silu(
        centered * lax.rsqrt(spread + norm_eps) * channel_gain + channel_bias
    ).astype(jnp.bfloat16)
    share = lax.psum_scatter(
        jnp.dot(attended, w_out_attn, preferred_element_type=jnp.float32)
        + jnp.dot(channel_out, w_out_conv, preferred_element_type=jnp.float32),
        "tp",
        scatter_dimension=0,
        tiled=True,
    )
    mixed = lax.all_gather(row_norm(share, out_gain).astype(jnp.bfloat16), "tp", axis=0, tiled=True)
    return (mixed, log_mass)


def solution(mesh):
    in_specs = (
        P(("grp", "sp"), None),
        P(),
        P("sp", "tp"),
        P("sp", "tp"),
        P("sp", "tp"),
        P("sp", "tp"),
        P("sp", "tp"),
        P(("grp", "sp"), "tp"),
        P("tp", None),
        P(None, "tp"),
        P("tp"),
        P("tp"),
        P("tp", None),
        P("tp", None),
        P(),
    )
    out_specs = (P(("grp", "sp"), None), P("tp", ("grp", "sp")))
    small = mesh.shape["sp"] == 4 and mesh.shape["tp"] == 4 and mesh.shape["grp"] == 2
    local = paired if small else gathered
    return jax.shard_map(local, mesh=mesh, in_specs=in_specs, out_specs=out_specs, check_vma=False)
```

```python
import jax
import jax.numpy as jnp
from jax import lax
from jax.experimental import pallas as pl
from jax.experimental.pallas import tpu as pltpu
from jax.sharding import PartitionSpec as P

norm_eps = 1e-06
BF16 = jnp.bfloat16
F32 = jnp.float32


def exchange(value, axis, bit):
    count = lax.axis_size(axis)
    return lax.ppermute(value, axis, [(s, s ^ bit) for s in range(count)])


def from_cross_behind(value, axis):
    count = lax.axis_size(axis)
    pairs = [(source, (source ^ 2) + 1) for source in range(count)]
    return lax.ppermute(value, axis, [(a, b) for a, b in pairs if b < count])


def from_behind(value, axis, steps):
    count = lax.axis_size(axis)
    initial, last = (max(0, -steps), min(count, count - steps))
    return lax.ppermute(value, axis, [(source, source + steps) for source in range(initial, last)])


def row_norm(values_in, gain_vec):
    squares = jnp.mean(values_in * values_in, axis=-1, keepdims=True)
    return values_in * lax.rsqrt(squares + norm_eps) * gain_vec


def dot_f32(a, b, dims=((1,), (0,))):
    return lax.dot_general(a, b, (dims, ((), ())), preferred_element_type=F32)


def params(limit=16):
    return pltpu.CompilerParams(vmem_limit_bytes=limit * 1024 * 1024)


VM = pl.BlockSpec(memory_space=pltpu.VMEM)
ANY = pl.BlockSpec(memory_space=pl.ANY)
HBM = pl.BlockSpec(memory_space=pltpu.HBM)


def shape(dims, dtype=BF16):
    return jax.ShapeDtypeStruct(dims, dtype)


def cost(flops, moved):
    return pl.CostEstimate(flops=flops, bytes_accessed=moved, transcendentals=0)


def in_hbm(*values):
    return [pltpu.with_memory_space_constraint(v, pltpu.HBM) for v in values]


def pack_qkv_kernel(wq, wk, wv, all_ref, send_ref, sems):
    part, width = send_ref.shape[0], wq.shape[1]
    mine = pl.ds(pl.multiple_of(lax.axis_index("grp") * part, part), part)
    first, rest = [], []
    for n, w in enumerate((wq, wk, wv)):
        at = slice(n * width, (n + 1) * width)
        first.append(pltpu.make_async_copy(w.at[mine, :], send_ref.at[:, at], sems.at[n]))
        rest.append(pltpu.make_async_copy(w, all_ref.at[:, at], sems.at[3 + n]))
    for copy in first + rest:
        copy.start()
    for copy in first + rest:
        copy.wait()


def pack_qkv(weights):
    block, width = weights[0].shape
    return pl.pallas_call(
        pack_qkv_kernel,
        out_shape=(shape((block, 3 * width)), shape((block // 2, 3 * width))),
        in_specs=[HBM] * 3,
        out_specs=[VM] * 2,
        scratch_shapes=[pltpu.SemaphoreType.DMA((6,))],
        cost_estimate=cost(2_000_000, 400_000),
        compiler_params=params(),
        name="pack_qkv",
    )(*in_hbm(*weights))


def norm_kernel(x_hbm, gain_hbm, wc_hbm, send_ref, own_ref, pair_ref, wc_ref, x_ref, gain_ref, normed, sems):
    side, low = lax.axis_index("sp") // 2, lax.axis_index("sp") % 2
    core = lax.axis_index("tp") % 2
    block = own_ref.shape[1]
    half = 2 * block
    half_rows = send_ref.shape[0]
    columns = wc_ref.shape[1]
    mine = pl.ds(pl.multiple_of(lax.axis_index("grp") * columns, columns), columns)
    copies = [
        pltpu.make_async_copy(x_hbm, x_ref, sems.at[0]),
        pltpu.make_async_copy(gain_hbm, gain_ref, sems.at[1]),
        pltpu.make_async_copy(wc_hbm.at[:, mine], wc_ref, sems.at[2]),
    ]
    for copy in copies:
        copy.start()
    for copy in copies[:2]:
        copy.wait()
    x = x_ref[...].astype(F32)
    squares = jnp.mean(x * x, axis=1, keepdims=True)
    normed[...] = (x * lax.rsqrt(squares + norm_eps) * gain_ref[...]).astype(BF16)
    first = pl.multiple_of(core * half_rows, half_rows)
    away = pl.multiple_of((1 - side) * half, half)
    send_ref[...] = normed[pl.ds(first, half_rows), pl.ds(away, half)]
    own_ref[...] = normed[:, pl.ds(pl.multiple_of(side * half + low * block, block), block)]
    pair_ref[...] = normed[:, pl.ds(pl.multiple_of(side * half + (1 - low) * block, block), block)]
    copies[2].wait()


def norm_parts(tokens, gain, block, wc):
    rows, features = tokens.shape
    return pl.pallas_call(
        norm_kernel,
        out_shape=(
            shape((rows // 2, 2 * block)),
            shape((rows, block)),
            shape((rows, block)),
            shape((wc.shape[0], wc.shape[1] // 2)),
        ),
        in_specs=[HBM] * 3,
        out_specs=[VM] * 4,
        scratch_shapes=[
            pltpu.VMEM((rows, features), BF16),
            pltpu.VMEM((1, features), F32),
            pltpu.VMEM((rows, features), BF16),
            pltpu.SemaphoreType.DMA((3,)),
        ],
        cost_estimate=cost(2_000_000, 1_000_000),
        compiler_params=params(),
        name="norm_parts",
    )(*in_hbm(tokens, gain.reshape(1, features), wc))


def pack_kernel(
    gv_hbm, gg_hbm, wa_hbm, off_hbm, head_hbm, gain_hbm, bias_hbm, *refs
):
    gv_ref, gv_send, gg_ref, out_ref, off_ref, head_ref, gain_ref, bias_ref, sems = refs
    cw, aw = gv_hbm.shape[1], wa_hbm.shape[0]
    part = gv_send.shape[0]
    mine = pl.ds(pl.multiple_of(lax.axis_index("grp") * part, part), part)
    pairs = (
        (gain_hbm, gain_ref),
        (bias_hbm, bias_ref),
        (gv_hbm.at[mine, :], gv_send),
        (gg_hbm, gg_ref),
        (wa_hbm, out_ref.at[:aw, :]),
        (off_hbm, off_ref),
        (head_hbm, head_ref),
        (gv_hbm, gv_ref),
    )
    copies = [pltpu.make_async_copy(a, b, sems.at[n]) for n, (a, b) in enumerate(pairs)]
    for copy in copies:
        copy.start()
    for copy in copies[:2]:
        copy.wait()
    extra = out_ref.shape[0] - aw
    for n, ref in enumerate((gain_ref, bias_ref)):
        rest = ref[...]
        for piece in range(3):
            part = rest.astype(BF16)
            rest = rest - part.astype(F32)
            first = (3 * n + piece) * cw
            out_ref[aw:, first : first + cw] = jnp.broadcast_to(part, (extra, cw))
    for copy in copies[2:]:
        copy.wait()


def pack(gv, gg, wa, off, head_gain, gain, bias):
    block, cw = gv.shape
    aw, width = wa.shape
    return pl.pallas_call(
        pack_kernel,
        out_shape=(
            shape((block, cw)),
            shape((block // 2, cw)),
            shape((block, cw)),
            shape((aw + 16, width)),
            shape(off.shape),
            shape(head_gain.shape, F32),
        ),
        in_specs=[HBM] * 7,
        out_specs=[VM] * 6,
        scratch_shapes=[
            pltpu.VMEM((1, cw), F32),
            pltpu.VMEM((1, cw), F32),
            pltpu.SemaphoreType.DMA((8,)),
        ],
        cost_estimate=cost(2_000_000, 2_000_000),
        compiler_params=params(),
        name="pack",
    )(*in_hbm(gv, gg, wa, off, head_gain, gain.reshape(1, cw), bias.reshape(1, cw)))


def assemble_kernel(own_ref, pair_ref, got_ref, other_ref, own_out, pair_out):
    low = lax.axis_index("sp") % 2
    core = lax.axis_index("tp") % 2
    rows, block = own_ref.shape
    half = got_ref.shape[0]
    own_out[:rows, :] = own_ref[...]
    pair_out[:rows, :] = pair_ref[...]
    own_at = pl.multiple_of(low * block, block)
    pair_at = pl.multiple_of((1 - low) * block, block)
    for part, at in ((got_ref, core), (other_ref, 1 - core)):
        first = pl.multiple_of(rows + at * half, half)
        own_out[pl.ds(first, half), :] = part[:, pl.ds(own_at, block)]
        pair_out[pl.ds(first, half), :] = part[:, pl.ds(pair_at, block)]


def assemble(own, pair, got, other):
    rows, block = own.shape
    return pl.pallas_call(
        assemble_kernel,
        out_shape=(shape((2 * rows, block)),) * 2,
        in_specs=[VM] * 4,
        out_specs=[VM] * 2,
        cost_estimate=cost(2_000_000, 1_000_000),
        compiler_params=params(),
        name="assemble",
    )(own, pair, got, other)


def far_dot(x_pair, same, other):
    part = same.shape[0]
    group = lax.axis_index("grp")
    near = x_pair[:, pl.ds(pl.multiple_of(group * part, part), part)]
    rest = x_pair[:, pl.ds(pl.multiple_of((1 - group) * part, part), part)]
    return dot_f32(near, same[...]) + dot_f32(rest, other[...])


def qkv_kernel(x_own, x_pair, own, same, other, off_ref, keep_ref, send_ref):
    rows = x_own.shape[0] // 2
    width = send_ref.shape[1]
    total = dot_f32(x_own[...], own[...]) + far_dot(x_pair, same, other)
    keep_ref[...] = total
    for n in range(3):
        part = total[:, n * width : (n + 1) * width].astype(BF16)
        first = 4 * rows if n == 0 else 2 * (n - 1) * rows
        send_ref[first : first + rows, :] = part[rows:]
        if n > 0:
            send_ref[first + rows : first + 2 * rows, :] = part[:rows]
    send_ref[5 * rows :, :] = jnp.zeros((send_ref.shape[0] - 5 * rows, width), BF16)
    send_ref[5 * rows : 5 * rows + off_ref.shape[0], :] = off_ref[...]


def project_qkv(x_own, x_pair, own, same, other, off):
    rows, width = x_own.shape[0], own.shape[1] // 3
    return pl.pallas_call(
        qkv_kernel,
        out_shape=(shape((rows, 3 * width), F32), shape((5 * rows // 2 + 16, width))),
        in_specs=[VM] * 6,
        out_specs=[VM] * 2,
        cost_estimate=cost(200_000_000, 1_000_000),
        compiler_params=params(),
        name="project_qkv",
    )(x_own, x_pair, own, same, other, off)


def sum_kernel(keep_ref, got_ref, sent_ref, after, q_ref, out_ref):
    rows, width = q_ref.shape

    def got(n):
        return got_ref[n * rows : (n + 1) * rows, :].astype(F32)

    q_ref[...] = (keep_ref[:rows, :width] + got(4)).astype(BF16)
    for n in range(4):
        at = slice((1 + n // 2) * width, (2 + n // 2) * width)
        part = keep_ref[(n % 2) * rows : (n % 2 + 1) * rows, at]
        out_ref[n * rows : (n + 1) * rows, :] = (part + got(n)).astype(BF16)
    first = 5 * rows
    out_ref[4 * rows :, :] = jnp.concatenate([sent_ref[first : first + 8, :], got_ref[first : first + 8, :]])


def sum_qkv(keep, got, sent, after):
    rows, width = keep.shape[0] // 2, got.shape[1]
    return pl.pallas_call(
        sum_kernel,
        out_shape=(shape((rows, width)), shape((4 * rows + 16, width))),
        in_specs=[VM] * 3 + [ANY],
        out_specs=[VM] * 2,
        cost_estimate=cost(1_000_000, 1_000_000),
        compiler_params=params(),
        name="sum_qkv",
    )(keep, got, sent, after)


def glu_kernel(x_own, x_pair, gv, gg, gv_same, gv_other, gg_pair, after, keep_ref, send_ref, own_tail, far_tail):
    rows = x_own.shape[0] // 2
    tail, cw = own_tail.shape[0], gv.shape[1]
    for n in range(2):
        own = (gv, gg)[n]
        far = far_dot(x_pair, gv_same, gv_other) if n == 0 else dot_f32(x_pair[...], gg_pair[...])
        total = dot_f32(x_own[...], own[...]) + far
        at = slice(n * cw, (n + 1) * cw)
        keep_ref[:, at] = total[:rows]
        send_ref[:, at] = total[rows:].astype(BF16)
        own_tail[:, at] = total[rows - tail : rows].astype(BF16)
        far_tail[:, at] = total[2 * rows - tail :].astype(BF16)


def project_glu(x_own, x_pair, own, pair, tail, after):
    rows, width = x_own.shape[0] // 2, 2 * own[0].shape[1]
    return pl.pallas_call(
        glu_kernel,
        out_shape=(
            shape((rows, width), F32),
            shape((rows, width)),
            shape((tail, width)),
            shape((tail, width)),
        ),
        in_specs=[VM] * 7 + [ANY],
        out_specs=[VM] * 4,
        cost_estimate=cost(270_000_000, 1_000_000),
        compiler_params=params(),
        name="project_glu",
    )(x_own, x_pair, *own, *pair, after)


def conv_kernel(keep_ref, got_ref, near_ref, far_ref, taps_ref, att_ref, act_ref, padded):
    rows, aw = att_ref.shape
    tail, cw = near_ref.shape[0], taps_ref.shape[1]
    taps = taps_ref.shape[0]

    def gated(glu):
        value = glu[:, :cw].astype(BF16).astype(F32)
        gate = glu[:, cw:].astype(BF16).astype(F32)
        return (value * jax.nn.sigmoid(gate)).astype(BF16).astype(F32)

    padded[:tail, :] = gated(near_ref[...].astype(F32) + far_ref[...].astype(F32))
    padded[tail:, :] = gated(keep_ref[...] + got_ref[...].astype(F32))
    total = None
    for tap in range(taps):
        first = tail - (taps - 1) + tap
        part = taps_ref[tap : tap + 1, :] * padded[first : first + rows, :]
        total = part if total is None else total + part
    act_ref[:, :aw] = att_ref[...]
    act_ref[:, aw:] = total.astype(BF16)


def conv(keep, got, near, far, taps, attended):
    rows, cw = keep.shape[0], taps.shape[1]
    return pl.pallas_call(
        conv_kernel,
        out_shape=shape((rows, attended.shape[1] + cw)),
        in_specs=[VM] * 6,
        out_specs=VM,
        scratch_shapes=[pltpu.VMEM((rows + near.shape[0], cw), F32)],
        cost_estimate=cost(20_000_000, 500_000),
        compiler_params=params(),
        name="conv",
    )(keep, got, near, far, taps, attended)


def suffix_matrix(keys):
    before = lax.broadcasted_iota(jnp.int32, (2 * keys, 2 * keys), 0) % keys
    column = lax.broadcasted_iota(jnp.int32, (2 * keys, 2 * keys), 1)
    return jnp.where((column >= keys) | (before > column), 1.0, 0.0).astype(BF16)


def stick_block(q, k, v, off, hd, suffix, carry, diagonal):
    rows, width = q.shape
    keys = k.shape[0]
    lane = lax.broadcasted_iota(jnp.int32, (rows, width), 1) // hd
    offsets = off.astype(F32)
    weights, totals, values = [], [], []
    for h in range(width // hd):
        qh = jnp.where(lane == h, q, jnp.zeros_like(q))
        s = dot_f32(qh, k, ((1,), (1,))) * hd ** (-0.5) + offsets[h : h + 1, :]
        soft = jnp.maximum(s, 0.0) + jnp.log(1.0 + jnp.exp(-jnp.abs(s)))
        log_not = -soft
        if diagonal:
            allowed = lax.broadcasted_iota(jnp.int32, (rows, keys), 1) <= lax.broadcasted_iota(
                jnp.int32, (rows, keys), 0
            )
            log_not = jnp.where(allowed, log_not, 0.0)
        high = log_not.astype(BF16)
        low = (log_not - high.astype(F32)).astype(BF16)
        sums = dot_f32(jnp.concatenate([high, low], axis=1), suffix)
        later = sums[:, :keys]
        if carry is not None:
            later = later + carry[h]
        w = jnp.exp(s - soft + later)
        if diagonal:
            w = jnp.where(allowed, w, 0.0)
        weights.append(w)
        totals.append(sums[:, keys:])
        values.append(jnp.where(lane == h, v, jnp.zeros_like(v)))
    mix = dot_f32(
        jnp.concatenate([w.astype(BF16) for w in weights], axis=1), jnp.concatenate(values, axis=0)
    )
    return mix, weights, totals


def near_kernel(q_ref, mine_ref, gain_ref, after, mix_ref, mass_ref, carry_ref):
    rows = q_ref.shape[0]
    heads, hd = gain_ref.shape
    suffix = suffix_matrix(rows)
    for n in range(2):
        k = mine_ref[n * rows : (n + 1) * rows, :]
        v = mine_ref[(2 + n) * rows : (3 + n) * rows, :]
        off = mine_ref[4 * rows + 8 * n : 4 * rows + 8 * n + 8, :]
        mix, weights, totals = stick_block(q_ref[...], k, v, off, hd, suffix, None, n == 0)
        mix_ref[n] = mix
        for h in range(heads):
            mass_ref[n * heads + h] = weights[h]
            carry_ref[n * heads + h] = totals[h]


def near_attention(q, mine, head_gain, after):
    rows, width = q.shape
    heads = head_gain.shape[0]
    return pl.pallas_call(
        near_kernel,
        out_shape=(
            shape((2, rows, width), F32),
            shape((2 * heads, rows, rows), F32),
            shape((2 * heads, rows, rows), F32),
        ),
        in_specs=[VM] * 3 + [ANY],
        out_specs=[VM] * 3,
        cost_estimate=cost(200_000_000, 1_000_000),
        compiler_params=params(),
        name="near_attention",
    )(q, mine, head_gain, after)


def attention_kernel(q_ref, pair_ref, gain_ref, mix_ref, mass_ref, carry_ref, after, out_ref, log_ref, acc, mass, carry):
    me = lax.axis_index("sp")
    rows, width = q_ref.shape
    heads, hd = gain_ref.shape
    lane = lax.broadcasted_iota(jnp.int32, (rows, width), 1) // hd
    suffix = suffix_matrix(rows)
    acc[...] = mix_ref[0]
    for h in range(heads):
        mass[h] = mass_ref[h]
        carry[h] = carry_ref[h]

    def earlier(t, _):
        slot = jnp.bitwise_xor(me - t, me)

        @pl.when(slot == 2)
        def _():
            scale = jnp.zeros_like(acc)
            for h in range(heads):
                left = jnp.exp(carry[h])
                mass[h] = mass[h] + left * mass_ref[heads + h]
                scale = jnp.where(lane == h, left, scale)
                carry[h] = carry[h] + carry_ref[heads + h]
            acc[...] = acc[...] + scale * mix_ref[1]

        @pl.when(slot != 2)
        def _():
            n = slot // 2
            k = pair_ref[pl.ds(pl.multiple_of(n * rows, rows), rows), :]
            v = pair_ref[pl.ds(pl.multiple_of((2 + n) * rows, rows), rows), :]
            off = jnp.where(
                n == 0,
                pair_ref[4 * rows : 4 * rows + 8, :].astype(F32),
                pair_ref[4 * rows + 8 : 4 * rows + 16, :].astype(F32),
            )
            so_far = [carry[h] for h in range(heads)]
            mix, weights, totals = stick_block(q_ref[...], k, v, off, hd, suffix, so_far, False)
            acc[...] = acc[...] + mix
            for h in range(heads):
                mass[h] = mass[h] + weights[h]
                carry[h] = so_far[h] + totals[h]

        return 0

    lax.fori_loop(1, me + 1, earlier, 0)
    mixed = acc[...]
    squares = mixed * mixed
    inverse = jnp.zeros_like(mixed)
    for h in range(heads):
        mean = jnp.sum(jnp.where(lane == h, squares, 0.0), axis=1, keepdims=True) / hd
        inverse = jnp.where(lane == h, lax.rsqrt(mean + norm_eps), inverse)
    gain = jnp.concatenate([gain_ref[h : h + 1, :] for h in range(heads)], axis=1)
    out_ref[...] = (mixed * inverse * gain).astype(BF16)
    for h in range(heads):
        log_ref[h : h + 1, :] = jnp.log(jnp.sum(jnp.transpose(mass[h]), axis=0, keepdims=True))


def attention(q, pair, head_gain, near, after):
    rows, width = q.shape
    heads = head_gain.shape[0]
    return pl.pallas_call(
        attention_kernel,
        out_shape=(shape((rows, width)), shape((heads, rows), F32)),
        in_specs=[VM] * 6 + [ANY],
        out_specs=[VM] * 2,
        scratch_shapes=[
            pltpu.VMEM((rows, width), F32),
            pltpu.VMEM((heads, rows, rows), F32),
            pltpu.VMEM((heads, rows, rows), F32),
        ],
        cost_estimate=cost(400_000_000, 1_000_000),
        compiler_params=params(),
        name="stick_attention",
    )(q, pair, head_gain, *near, after)


def heads_part(act, wa, aw, at):
    w = jnp.concatenate([ref[:aw, at] for ref in wa], axis=0)
    return dot_f32(jnp.concatenate([ref[:, :aw] for ref in act], axis=1), w)


def begin_kernel(act0, act1, wa0, wa1, out_ref):
    aw = wa0.shape[0] - 16
    for first in range(0, out_ref.shape[1], CHUNK):
        at = slice(first, first + CHUNK)
        out_ref[:, at] = heads_part((act0, act1), (wa0, wa1), aw, at)


def begin(act0, act1, wa0, wa1):
    rows, width = act0.shape[0], wa0.shape[1]
    return pl.pallas_call(
        begin_kernel,
        out_shape=shape((rows, width), F32),
        in_specs=[VM] * 4,
        out_specs=VM,
        cost_estimate=cost(130_000_000, 2_000_000),
        compiler_params=params(),
        name="begin_rows",
    )(act0, act1, wa0, wa1)


def final_kernel(*refs):
    act, wa, wc, begun, gain_ref, out_ref, mix, done, sems = refs[:4], refs[4:8], refs[8:14], *refs[14:]
    cw = wc[0].shape[0]
    aw = act[0].shape[1] - cw
    convs = [c[:, aw:].astype(F32) for c in act]
    mean = sum(jnp.sum(v, axis=1, keepdims=True) for v in convs) / (4 * cw)
    centered = [v - mean for v in convs]
    spread = sum(jnp.sum(v * v, axis=1, keepdims=True) for v in centered) / (4 * cw)
    inverse = lax.rsqrt(spread + norm_eps)
    ys = []
    for slot in range(4):
        pieces = [wa[slot][aw : aw + 1, n * cw : (n + 1) * cw].astype(F32) for n in range(6)]
        gain = pieces[0] + pieces[1] + pieces[2]
        bias = pieces[3] + pieces[4] + pieces[5]
        y = centered[slot] * inverse * gain + bias
        ys.append((y * jax.nn.sigmoid(y)).astype(BF16))
    group = lax.axis_index("grp")
    rows, width = mix.shape
    half = width // 2
    squares = jnp.zeros((rows, 1), F32)
    for n in range(2):
        base = (group if n == 0 else 1 - group) * half
        for first in range(0, half, CHUNK):
            at = pl.ds(pl.multiple_of(base + first, CHUNK), CHUNK)
            inner = slice(first, first + CHUNK)
            part = begun[:, at]
            for slot in range(4):
                w = wc[slot][:, at] if slot < 2 else wc[2 * slot - 2 + n][:, inner]
                part = part + dot_f32(ys[slot], w)
            part = part + heads_part(act[2:], wa[2:], aw, at)
            mix[:, at] = part
            squares = squares + jnp.sum(part * part, axis=1, keepdims=True)
    inverse = lax.rsqrt(squares / width + norm_eps)
    step = rows // 4
    copies = []
    for n in range(4):
        at = slice(n * step, (n + 1) * step)
        done[at, :] = (mix[at, :] * inverse[at] * gain_ref[...]).astype(BF16)
        copies.append(pltpu.make_async_copy(done.at[at, :], out_ref.at[at, :], sems.at[n]))
        copies[-1].start()
    for copy in copies:
        copy.wait()


CHUNK = 256


def finish(act, wa, wc, begun, out_gain):
    rows, width = act[0].shape[0], wa[0].shape[1]
    return pl.pallas_call(
        final_kernel,
        out_shape=shape((rows, width)),
        in_specs=[VM] * 16,
        out_specs=HBM,
        scratch_shapes=[
            pltpu.VMEM((rows, width), F32),
            pltpu.VMEM((rows, width), BF16),
            pltpu.SemaphoreType.DMA((4,)),
        ],
        cost_estimate=cost(800_000_000, 7_000_000),
        compiler_params=params(32),
        name="finish_rows",
    )(*act, *wa, *wc, begun, out_gain.reshape(1, width))


def paired(
    tokens,
    norm_gain,
    w_query,
    w_key,
    w_value,
    w_glu_value,
    w_glu_gate,
    key_offset,
    head_gain,
    conv_taps,
    channel_gain,
    channel_bias,
    w_out_attn,
    w_out_conv,
    out_gain,
):
    own_qkv, half_qkv = pack_qkv((w_query, w_key, w_value))
    qkv_same = exchange(half_qkv, "sp", 1)
    x_send, mine_own, mine_pair, wc_half = norm_parts(tokens, norm_gain, w_query.shape[0], w_out_conv)
    wc_x = exchange(wc_half, "tp", 2)
    wc_y = exchange(wc_x, "grp", 1)
    wc_yc = exchange(wc_y, "tp", 1)
    x_got = exchange(x_send, "sp", 2)
    own_gv, half_gv, own_gg, wa_mine, off, head_rows = pack(
        w_glu_value, w_glu_gate, w_out_attn, key_offset.T, head_gain, channel_gain, channel_bias
    )
    qkv_same, half_gv = lax.optimization_barrier((qkv_same, half_gv))
    gv_same = exchange(half_gv, "sp", 1)
    gg_pair = exchange(own_gg, "sp", 1)
    gv_other = exchange(gv_same, "grp", 1)
    qkv_other = exchange(qkv_same, "grp", 1)
    x_other = exchange(x_got, "tp", 1)
    wa_x = exchange(wa_mine, "tp", 2)
    wc_core = exchange(w_out_conv, "tp", 1)
    wa_core = exchange(wa_mine, "tp", 1)
    wc_xc = exchange(wc_x, "tp", 1)
    wa_xc = exchange(wa_x, "tp", 1)
    x_own, x_pair = assemble(mine_own, mine_pair, x_got, x_other)

    keep, sent = project_qkv(x_own, x_pair, own_qkv, qkv_same, qkv_other, off)
    got = exchange(sent, "sp", 2)
    tail_rows = -(-conv_taps.shape[0] // 16) * 16
    glu_keep, glu_sent, own_tail, cross_tail = project_glu(
        x_own, x_pair, (own_gv, own_gg), (gv_same, gv_other, gg_pair), tail_rows, sent
    )
    glu_got = exchange(glu_sent, "sp", 2)
    tail_near = from_behind(own_tail, "sp", 1)
    tail_far = from_cross_behind(cross_tail, "sp")
    q, mine_two = sum_qkv(keep, got, sent, glu_sent)
    pair_two = exchange(mine_two, "sp", 1)
    near = near_attention(q, mine_two, head_rows, mine_two)
    attended, log_mass = attention(q, pair_two, head_rows, near, mine_two)
    act_mine = conv(glu_keep, glu_got, tail_near, tail_far, conv_taps, attended)
    act_x = exchange(act_mine, "tp", 2)
    act_core = exchange(act_mine, "tp", 1)
    act = (act_mine, act_core, act_x, exchange(act_x, "tp", 1))
    wa = (wa_mine, wa_core, wa_x, wa_xc)
    wc = (w_out_conv, wc_core, wc_x, wc_y, wc_xc, wc_yc)
    begun = begin(act_mine, act_core, wa_mine, wa_core)
    mixed = finish(act, wa, wc, begun, out_gain)
    return (mixed, log_mass)


def gathered(
    tokens,
    norm_gain,
    w_query,
    w_key,
    w_value,
    w_glu_value,
    w_glu_gate,
    key_offset,
    head_gain,
    conv_taps,
    channel_gain,
    channel_bias,
    w_out_attn,
    w_out_conv,
    out_gain,
):
    row_count = tokens.shape[0]
    hd = head_gain.shape[1]
    channels = conv_taps.shape[1] * lax.axis_size("tp")
    normed = row_norm(tokens.astype(jnp.float32), norm_gain).astype(jnp.bfloat16)
    weights_in = (w_query, w_key, w_value, w_glu_value, w_glu_gate)
    pieces = (
        lax.all_gather(weights_in[0], "sp", axis=0, tiled=True),
        lax.all_gather(weights_in[1], "sp", axis=0, tiled=True),
        lax.all_gather(weights_in[2], "sp", axis=0, tiled=True),
        lax.all_gather(weights_in[3], "sp", axis=0, tiled=True),
        lax.all_gather(weights_in[4], "sp", axis=0, tiled=True),
    )
    projected = tuple(
        (jnp.dot(normed, shard_piece, preferred_element_type=jnp.float32) for shard_piece in pieces)
    )
    query, key_rows, value_rows, glu_value, glu_gate = [
        summed.astype(jnp.bfloat16) for summed in projected
    ]
    kv_local = key_rows.shape[1] // hd
    group_size = query.shape[1] // key_rows.shape[1]
    heads_local = kv_local * group_size
    all_keys, all_values, all_offsets = (
        lax.all_gather(key_rows, "sp", axis=0, tiled=True),
        lax.all_gather(value_rows, "sp", axis=0, tiled=True),
        lax.all_gather(key_offset, "sp", axis=0, tiled=True),
    )
    sequence_length_total = all_keys.shape[0]
    shard_count = lax.axis_size("sp")
    per_block = 1
    while (
        per_block * 2 <= shard_count
        and shard_count % (per_block * 2) == 0
        and (per_block * 2 * row_count <= 1024)
    ):
        per_block = per_block * 2
    span_len = per_block * row_count
    query_heads = query.reshape(row_count, kv_local, group_size, hd)
    key_heads = all_keys.reshape(sequence_length_total, kv_local, hd)
    value_heads = all_values.reshape(sequence_length_total, kv_local, hd)
    my_index = lax.axis_index("sp")
    query_pos = my_index * row_count + jnp.arange(row_count, dtype=jnp.int32)
    last_block = my_index // per_block
    zeros_mix = jnp.zeros((kv_local, group_size, row_count, hd), jnp.float32)
    zeros_row = jnp.zeros((kv_local, group_size, row_count), jnp.float32)

    def sweep(turn_index, carry):
        head_mix, mass_sum, carried = carry
        first_key = (last_block - turn_index) * span_len
        key_block = lax.dynamic_slice_in_dim(key_heads, first_key, span_len, 0)
        value_block = lax.dynamic_slice_in_dim(value_heads, first_key, span_len, 0)
        offset_block = lax.dynamic_slice_in_dim(all_offsets, first_key, span_len, 0).astype(
            jnp.float32
        )
        offset_block = offset_block.T.reshape(kv_local, group_size, 1, span_len)
        scores = (
            jnp.einsum("qhgd,khd->hgqk", query_heads, key_block, preferred_element_type=jnp.float32)
            * hd ** (-0.5)
            + offset_block
        )
        key_pos = first_key + jnp.arange(span_len, dtype=jnp.int32)
        allowed = key_pos[None, :] <= query_pos[:, None]
        log_not = jnp.where(allowed, jax.nn.log_sigmoid(-scores), 0.0)
        later = lax.cumsum(log_not, axis=3, reverse=True) - log_not + carried[..., None]
        weights = jnp.where(allowed, jnp.exp(jax.nn.log_sigmoid(scores) + later), 0.0)
        head_mix = head_mix + jnp.einsum(
            "hgqk,khd->hgqd",
            weights.astype(jnp.bfloat16),
            value_block,
            preferred_element_type=jnp.float32,
        )
        return (head_mix, mass_sum + jnp.sum(weights, axis=3), carried + jnp.sum(log_not, axis=3))

    head_mix, mass_sum, _ = lax.fori_loop(
        0, last_block + 1, sweep, (zeros_mix, zeros_row, zeros_row)
    )
    log_mass = jnp.log(mass_sum).reshape(heads_local, row_count)
    head_rows = head_mix.transpose(2, 0, 1, 3).reshape(row_count, heads_local, hd)
    attended = (
        row_norm(head_rows, head_gain).astype(jnp.bfloat16).reshape(row_count, heads_local * hd)
    )
    gated = (glu_value.astype(jnp.float32) * jax.nn.sigmoid(glu_gate.astype(jnp.float32))).astype(
        jnp.bfloat16
    )
    reach_len = conv_taps.shape[0] - 1
    before = from_behind(gated[row_count - reach_len :], "sp", 1)
    padded = jnp.concatenate([before, gated], axis=0).astype(jnp.float32)
    conv_out = jnp.zeros(gated.shape, jnp.float32)
    for tap_index in range(conv_taps.shape[0]):
        conv_out = conv_out + conv_taps[tap_index] * padded[tap_index : tap_index + row_count]
    total_sum, total_squares = lax.psum(
        (jnp.sum(conv_out, axis=1), jnp.sum(conv_out * conv_out, axis=1)), "tp"
    )
    chan_mean = (total_sum / channels)[:, None]
    spread = (total_squares / channels)[:, None] - chan_mean * chan_mean
    centered = conv_out - chan_mean
    channel_out = jax.nn.silu(
        centered * lax.rsqrt(spread + norm_eps) * channel_gain + channel_bias
    ).astype(jnp.bfloat16)
    share = lax.psum_scatter(
        jnp.dot(attended, w_out_attn, preferred_element_type=jnp.float32)
        + jnp.dot(channel_out, w_out_conv, preferred_element_type=jnp.float32),
        "tp",
        scatter_dimension=0,
        tiled=True,
    )
    mixed = lax.all_gather(row_norm(share, out_gain).astype(jnp.bfloat16), "tp", axis=0, tiled=True)
    return (mixed, log_mass)


def solution(mesh):
    in_specs = (
        P(("grp", "sp"), None),
        P(),
        P("sp", "tp"),
        P("sp", "tp"),
        P("sp", "tp"),
        P("sp", "tp"),
        P("sp", "tp"),
        P(("grp", "sp"), "tp"),
        P("tp", None),
        P(None, "tp"),
        P("tp"),
        P("tp"),
        P("tp", None),
        P("tp", None),
        P(),
    )
    out_specs = (P(("grp", "sp"), None), P("tp", ("grp", "sp")))
    small = mesh.shape["sp"] == 4 and mesh.shape["tp"] == 4 and mesh.shape["grp"] == 2
    local = paired if small else gathered
    return jax.shard_map(local, mesh=mesh, in_specs=in_specs, out_specs=out_specs, check_vma=False)
```
